256 devices in a mesh: sp: 64 (over z, x, core), tp: 4 (over y).
Axes of the slice: x: 4, y: 4, z: 8, core: 2. Of those that a mesh axis runs over, the one named last changes fastest.
Arguments:
- tokens: bfloat16 [8192, 2048], P('sp'), may hold values from -6 to 6
- norm_gain: float32 [2048], replicated, may hold values from 0.1 to 1.9
- cotangent: bfloat16 [8192, 2048], P('sp'), may hold values from -16 to 16
- routes: int32 [8192, 2], P('sp'), may hold values from 0 to 31, all different within a row; in each aligned block of 128 rows (0 to 127, 128 to 255, ...) at most 16 rows name the same one
- route_weight: float32 [8192, 2], P('sp'), may hold values from 0.2 to 1
- gate_weight: bfloat16 [64, 2048, 1792], P('sp', None, 'tp'), may hold values from -0.125 to 0.125
- up_weight: bfloat16 [64, 2048, 1792], P('sp', None, 'tp'), may hold values from -0.125 to 0.125
- down_weight: bfloat16 [64, 1792, 2048], P('sp', 'tp'), may hold values from -0.09375 to 0.09375
- scan_input: bfloat16 [8192, 1024], P('sp', 'tp'), may hold values from -6 to 6
- out_gate: bfloat16 [8192, 1024], P('sp', 'tp'), may hold values from -6 to 6
- step_size: float32 [16, 8192], P('tp', 'sp'), may hold values from 0.24 to 4.1
- decay_rate: float32 [16], P('tp'), may hold values from 1.2084961e-06 to 0.031
- write_keys: bfloat16 [8192, 256], P('sp', 'tp'), may hold values from -0.75 to 0.75
- read_keys: bfloat16 [8192, 256], P('sp', 'tp'), may hold values from -0.75 to 0.75
- start_state: float32 [64, 16, 64, 64], P('sp', 'tp'), may hold values from -12 to 12
- out_proj: bfloat16 [2048, 1024], P(None, 'tp'), may hold values from -0.1875 to 0.1875
Outputs:
- residual_grad: bfloat16 [8192, 2048], P('sp', 'tp')
- gate_weight_grad: bfloat16 [64, 2048, 1792], P('sp', None, 'tp')
- up_weight_grad: bfloat16 [64, 2048, 1792], P('sp', None, 'tp')
- down_weight_grad: bfloat16 [64, 1792, 2048], P('sp', 'tp')
- out_proj_grad: float32 [2048, 1024], P('sp', 'tp')
- scan_input_grad: bfloat16 [8192, 1024], P('sp', 'tp')
- out_gate_grad: bfloat16 [8192, 1024], P('sp', 'tp')
- write_keys_grad: bfloat16 [8192, 256], P('sp', 'tp')
- read_keys_grad: bfloat16 [8192, 256], P('sp', 'tp')
The draws below stay inside these ranges and needn't reach their ends.
Inputs may be any that keep to these rules, and one draw needn't show every extreme that they name: Each token names two different experts. Among the tokens of one block of 128 positions at most 16 routes name one expert, and in every draw some expert gets exactly 16 routes from some block.
All inputs are finite; a program needn't handle non-finite values.
Results may differ from the reference program's by a relative error of at most 0.0078.
Values may be sent and summed in bfloat16 or wider, within the bound.
A program may use at most 128 MiB of HBM per device.

```python
import math
import jax
import jax.numpy as jnp
import numpy as np
from jax import lax

D = 2048
FF = 3584
FF_HALF = 1792
HEADS = 16
HEAD_DIM = 64
STATE = 64
GROUPS = 4
MIX = 1024
TOK_DEV = 128
BLOCKS = 64
TOKENS = 8192
EXPERTS = 32
CAP = 16
N_SP = 64


def draw_step_size(key, part):
    token_key, block_key = jax.random.split(jax.random.fold_in(key, 11))
    block_count = TOKENS // TOK_DEV
    local = jax.random.uniform(token_key, (HEADS, TOKENS), jnp.float32, -0.7, 0.7)
    slow = jax.random.uniform(block_key, (HEADS, block_count, 1), jnp.float32, -0.7, 0.7)
    slow = jnp.broadcast_to(slow, (HEADS, block_count, TOK_DEV)).reshape(HEADS, TOKENS)
    return jnp.exp(local + slow)


def draw_decay_rate(key, part):
    lowest = math.log(0.01 / TOKENS)
    highest = math.log(0.03)
    drawn = jax.random.uniform(jax.random.fold_in(key, 23), (HEADS,), jnp.float32, lowest, highest)
    return jnp.exp(drawn)


def spiked(array, key, source, target, shards_of, factor):
    owner, partner = [(jnp.arange(array.shape[dim]) // (array.shape[dim] // shards_of)).reshape([-1 if axis == dim else 1 for axis in range(array.ndim)]) for dim in (source, target)]
    chosen = jax.random.permutation(key, shards_of)[partner]
    strong = (owner == chosen) | (owner == (partner + shards_of // 2) % shards_of)
    return jnp.where(strong, factor * array, array)


def block_scale(own_key, shape, cuts, smallest, top_value):
    factor_of, own = 1.0, jax.random.fold_in(own_key, 6)
    for axis_at, blocks in cuts:
        heights = jnp.exp(jax.random.uniform(jax.random.fold_in(own, axis_at), (blocks,), jnp.float32, smallest / len(cuts), top_value / len(cuts)))
        factor_of = factor_of * jnp.repeat(heights, shape[axis_at] // blocks).reshape([-1 if axis == axis_at else 1 for axis in range(len(shape))])
    return factor_of


def deal_out(key, own, number, rows, number_of, top, reach, slope):
    order = jax.random.permutation(key, number_of)
    heavy_load, usual = load_shares(number_of, rows * top, reach, slope, True), load_shares(number_of, rows * top, reach, slope, False)
    places = jnp.arange(number_of)

    def named(sizes, turn):
        used = int((sizes > 0).sum())
        fixed = max(1, used // 4)
        shifted = fixed + (places - fixed + turn * (used - fixed)) % max(1, number_of - fixed)
        return jnp.zeros((number_of,), jnp.int32).at[order[jnp.where(places < fixed, places, shifted)]].set(jnp.asarray(sizes, jnp.int32))

    sizes = jnp.where(number % 4 == 0, named(heavy_load, number // 4), named(usual, number - number // 4 - 1))
    mixed = jax.random.permutation(jax.random.fold_in(own, 3), number_of)
    donor, sink = mixed[0:number_of // 2 * 2:2], mixed[1:number_of // 2 * 2:2]
    margin = jnp.minimum(sizes[donor] - 1, reach - sizes[sink]) // 2
    margin = jnp.where((donor == order[0]) | (sink == order[0]) | (sizes[sink] == 0), 0, jnp.maximum(margin, 0))
    shifted = jax.random.randint(jax.random.fold_in(own, 4), (number_of // 2,), 0, 1 << 20) % (margin + 1)
    sizes = sizes.at[donor].add(-shifted).at[sink].add(shifted)
    members = jnp.searchsorted(jnp.cumsum(sizes), jnp.arange(rows * top), side="right").astype(jnp.int32)
    listing = members.reshape(top, rows).T
    listing = listing[jax.random.permutation(jax.random.fold_in(own, 1), rows)]
    turn = jax.random.randint(jax.random.fold_in(own, 2), (rows, 1), 0, top)
    return jnp.take_along_axis(listing, (jnp.arange(top)[None, :] + turn) % top, axis=1)


def load_shares(count, total, reach, slope, full):
    loads = [(1 << 20) // math.isqrt(rank ** slope) + 1 for rank in range(1, count + 1)]
    largest = reach if full else min(reach, max(-(-total // count), total * loads[0] // sum(loads)))
    least = 1 if total - largest >= count - 1 else 0
    counts, surplus = [largest] + [least] * (count - 1), total - largest - least * (count - 1)
    while surplus > 0:
        free = [i for i in range(1, count) if counts[i] < largest] or [i for i in range(1, count) if counts[i] < reach]
        whole, budget = sum([loads[i] for i in free]), surplus
        for i in free:
            more = min(reach - counts[i], max(1, budget * loads[i] // whole), surplus)
            counts[i] = counts[i] + more
            surplus = surplus - more
    return np.array(counts)


def centred(stream_key, extent, scale, bound, cuts=(), kind=jnp.bfloat16):
    result = scale * jax.random.normal(stream_key, extent, jnp.float32)
    if cuts:
        result = result * block_scale(stream_key, extent, cuts, -0.22, 0.18)
    return jnp.clip(result, -bound, bound).astype(kind)


def noise_with(stream_key, shape, scale, reach, shards, heavy, dtype=jnp.bfloat16):
    values = scale * jax.random.normal(stream_key, shape, jnp.float32)
    if shards:
        values = values * block_scale(stream_key, shape, shards, -0.22, 0.18)
    return jnp.clip(spiked(values, jax.random.fold_in(stream_key, 3), *heavy), -reach, reach).astype(dtype)


def setup_inputs(seed: int = 0) -> dict:
    streams_of = jax.random.split(jax.random.key(seed), 17)
    tokens = centred(streams_of[0], (TOKENS, D), 1.0, 6.0, ((0, 64),))
    norm_gain = jnp.clip(1.0 + 0.18 * jax.random.normal(streams_of[1], (D,), jnp.float32), 0.1, 1.9)
    cotangent = noise_with(streams_of[2], (TOKENS, D), 1.0, 16.0, ((0, 64),), (0, 1, 64, 4.0))
    routes_keys = jax.random.split(jax.random.fold_in(streams_of[3], 1), TOKENS // TOK_DEV)
    routes_turns = jax.random.permutation(jax.random.fold_in(streams_of[3], 3), TOKENS // TOK_DEV)
    routes = jax.vmap(lambda own, number: deal_out(jax.random.fold_in(streams_of[3], 2), own, number, TOK_DEV, EXPERTS, 2, CAP, 1))(routes_keys, routes_turns).reshape((TOKENS, 2))
    route_weight = jnp.clip(0.2 + 0.8 * jax.random.uniform(streams_of[4], (TOKENS, 2), jnp.float32) ** block_scale(streams_of[4], (TOKENS, 2), ((0, 64),), -0.2, 0.2), 0.2, 1.0)
    gate_weight = centred(streams_of[5], (N_SP, D, FF_HALF), D ** -0.5, 0.125, ((0, 64), (2, 4)))
    up_weight = centred(streams_of[6], (N_SP, D, FF_HALF), D ** -0.5, 0.125, ((0, 64), (2, 4)))
    down_weight = centred(streams_of[7], (N_SP, FF_HALF, D), FF ** -0.5, 0.09375, ((0, 64), (1, 4)))
    scan_input = centred(streams_of[8], (TOKENS, MIX), 1.0, 6.0, ((0, 64), (1, 4)))
    out_gate = centred(streams_of[9], (TOKENS, MIX), 1.0, 6.0, ((0, 64), (1, 4)))
    step_size = draw_step_size(jax.random.fold_in(streams_of[16], 71), 0)
    decay_rate = draw_decay_rate(jax.random.fold_in(streams_of[16], 71), 0)
    write_keys = centred(streams_of[12], (TOKENS, GROUPS * STATE), 0.125, 0.75, ((0, 64), (1, 4)))
    read_keys = centred(streams_of[13], (TOKENS, GROUPS * STATE), 0.125, 0.75, ((0, 64), (1, 4)))
    start_state = centred(streams_of[14], (BLOCKS, HEADS, HEAD_DIM, STATE), 2.0, 12.0, ((0, 64), (1, 4)), jnp.float32)
    out_proj = centred(streams_of[15], (D, MIX), MIX ** -0.5, 0.1875, ((1, 4),))
    return dict(tokens=tokens, norm_gain=norm_gain, cotangent=cotangent, routes=routes, route_weight=route_weight, gate_weight=gate_weight, up_weight=up_weight, down_weight=down_weight, scan_input=scan_input, out_gate=out_gate, step_size=step_size, decay_rate=decay_rate, write_keys=write_keys, read_keys=read_keys, start_state=start_state, out_proj=out_proj)


EPS = 1e-06
HIGHEST = lax.Precision.HIGHEST

def prepare(scan_rows, step_rows, write_rows, read_rows, decay_rates, per_group):
    length = scan_rows.shape[0]
    head_count = step_rows.shape[0]
    logdec = jnp.cumsum(-decay_rates[:, None] * step_rows, axis=1)
    causal = jnp.arange(length)[:, None] >= jnp.arange(length)[None, :]
    spread = jnp.where(causal[None, :, :], logdec[:, :, None] - logdec[:, None, :], -jnp.inf)
    weights = jnp.exp(spread)
    inputs = scan_rows.astype(jnp.float32).reshape(length, head_count, -1) * jnp.transpose(step_rows)[:, :, None]
    write_head = jnp.repeat(write_rows.astype(jnp.float32).reshape(length, -1, STATE), per_group, axis=1)
    read_head = jnp.repeat(read_rows.astype(jnp.float32).reshape(length, -1, STATE), per_group, axis=1)
    scores = jnp.einsum('thn,shn->hts', read_head, write_head, precision=HIGHEST) * weights
    return (logdec, weights, inputs, write_head, read_head, scores)

def block_forward(scan_rows, gate_rows, step_rows, write_rows, read_rows, decay_rates, entry_state, mix_grad, per_group):
    logdec, weights, inputs, write_head, read_head, scores = prepare(scan_rows, step_rows, write_rows, read_rows, decay_rates, per_group)
    length, head_count = (inputs.shape[0], inputs.shape[1])
    growth = jnp.transpose(jnp.exp(logdec))
    output = jnp.einsum('hts,shp->thp', scores, inputs, precision=HIGHEST)
    output = output + growth[:, :, None] * jnp.einsum('thn,hpn->thp', read_head, entry_state, precision=HIGHEST)
    gate_val = gate_rows.astype(jnp.float32).reshape(length, head_count, -1)
    sigmoid_val = jax.nn.sigmoid(gate_val)
    gated = (output * gate_val * sigmoid_val).reshape(length, -1).astype(jnp.bfloat16)
    out_grad = mix_grad.reshape(length, head_count, -1)
    state_grad = out_grad * gate_val * sigmoid_val
    gate_grad = (out_grad * output * sigmoid_val * (1.0 + gate_val * (1.0 - sigmoid_val))).reshape(length, -1).astype(jnp.bfloat16)
    carried = jnp.einsum('th,thp,thn->hpn', growth, state_grad, read_head, precision=HIGHEST)
    return (gated, gate_grad, jnp.exp(logdec[:, -1]), carried, state_grad)

def block_back(scan_rows, step_rows, write_rows, read_rows, decay_rates, entry_state, state_grad, later_state, per_group):
    logdec, weights, inputs, write_head, read_head, scores = prepare(scan_rows, step_rows, write_rows, read_rows, decay_rates, per_group)
    length, head_count = (inputs.shape[0], inputs.shape[1])
    growth = jnp.transpose(jnp.exp(logdec))
    shrink = jnp.transpose(jnp.exp(logdec[:, -1:] - logdec))
    in_grad = jnp.einsum('hts,thp->shp', scores, state_grad, precision=HIGHEST)
    in_grad = in_grad + shrink[:, :, None] * jnp.einsum('shn,hpn->shp', write_head, later_state, precision=HIGHEST)
    scan_grad = (in_grad * jnp.transpose(step_rows)[:, :, None]).reshape(length, -1).astype(jnp.bfloat16)
    pair_terms = jnp.einsum('thp,shp->hts', state_grad, inputs, precision=HIGHEST) * weights
    read_grad = jnp.einsum('hts,shn->thn', pair_terms, write_head, precision=HIGHEST)
    read_grad = read_grad + growth[:, :, None] * jnp.einsum('thp,hpn->thn', state_grad, entry_state, precision=HIGHEST)
    write_grad = jnp.einsum('hts,thn->shn', pair_terms, read_head, precision=HIGHEST)
    write_grad = write_grad + shrink[:, :, None] * jnp.einsum('shp,hpn->shn', inputs, later_state, precision=HIGHEST)
    group_count = head_count // per_group
    read_total = lax.optimization_barrier(jnp.sum(read_grad.reshape(length, group_count, per_group, -1), axis=2)).reshape(length, -1).astype(jnp.bfloat16)
    write_total = lax.optimization_barrier(jnp.sum(write_grad.reshape(length, group_count, per_group, -1), axis=2)).reshape(length, -1).astype(jnp.bfloat16)
    return (scan_grad, write_total, read_total)

def expert_grads(rows_in, rows_cot, gate_mat, up_mat, down_mat):
    contract_rows = (((0,), (0,)), ((), ()))
    contract_cols = (((1,), (1,)), ((), ()))
    gate_pre = jnp.dot(rows_in, gate_mat, preferred_element_type=jnp.float32)
    up_pre = jnp.dot(rows_in, up_mat, preferred_element_type=jnp.float32)
    sigmoid_val = jax.nn.sigmoid(gate_pre)
    active = (gate_pre * sigmoid_val * up_pre).astype(jnp.bfloat16)
    down_grad = lax.dot_general(active, rows_cot, contract_rows, preferred_element_type=jnp.float32)
    act_grad = lax.dot_general(rows_cot, down_mat, contract_cols, preferred_element_type=jnp.float32)
    gate_pre_grad = (act_grad * up_pre * sigmoid_val * (1.0 + gate_pre * (1.0 - sigmoid_val))).astype(jnp.bfloat16)
    up_pre_grad = (act_grad * gate_pre * sigmoid_val).astype(jnp.bfloat16)
    gate_grad = lax.dot_general(rows_in, gate_pre_grad, contract_rows, preferred_element_type=jnp.float32)
    up_grad = lax.dot_general(rows_in, up_pre_grad, contract_rows, preferred_element_type=jnp.float32)
    input_grad = lax.dot_general(gate_pre_grad, gate_mat, contract_cols, preferred_element_type=jnp.float32)
    input_grad = input_grad + lax.dot_general(up_pre_grad, up_mat, contract_cols, preferred_element_type=jnp.float32)
    return (gate_grad, up_grad, down_grad, input_grad)

def reference(tokens, norm_gain, cotangent, routes, route_weight, gate_weight, up_weight, down_weight, scan_input, out_gate, step_size, decay_rate, write_keys, read_keys, start_state, out_proj):
    hidden = tokens.astype(jnp.float32)
    inverse = lax.rsqrt(lax.optimization_barrier(jnp.mean(hidden * hidden, axis=1)) + EPS)
    normed = (hidden * inverse[:, None] * norm_gain[None, :]).astype(jnp.bfloat16)
    most_rows = N_SP * CAP
    gate_whole = jnp.transpose(gate_weight.reshape(EXPERTS, 2, D, FF_HALF), (0, 2, 1, 3)).reshape(EXPERTS, D, FF)
    up_whole = jnp.transpose(up_weight.reshape(EXPERTS, 2, D, FF_HALF), (0, 2, 1, 3)).reshape(EXPERTS, D, FF)
    down_whole = down_weight.reshape(EXPERTS, FF, D)

    def expert_step(running, operands):
        expert_index, gate_mat, up_mat, down_mat = operands
        chosen = routes == expert_index
        scaling = lax.optimization_barrier(jnp.sum(jnp.where(chosen, route_weight, 0.0), axis=1))
        picked = jnp.any(chosen, axis=1)
        row_ids = jnp.nonzero(picked, size=most_rows, fill_value=0)[0]
        filled = jnp.arange(most_rows) < jnp.sum(picked.astype(jnp.int32))
        rows_in = normed[row_ids]
        scaled = (scaling[row_ids][:, None] * cotangent[row_ids].astype(jnp.float32)).astype(jnp.bfloat16)
        rows_cot = jnp.where(filled[:, None], scaled, jnp.zeros((), jnp.bfloat16))
        gate_grad, up_grad, down_grad, input_grad = expert_grads(rows_in, rows_cot, gate_mat, up_mat, down_mat)
        running = running.at[row_ids].add(jnp.where(filled[:, None], input_grad, 0.0))
        return (running, (gate_grad.astype(jnp.bfloat16), up_grad.astype(jnp.bfloat16), down_grad.astype(jnp.bfloat16)))
    normed_grad, (gate_all, up_all, down_all) = lax.scan(expert_step, jnp.zeros((TOKENS, D), jnp.float32), (jnp.arange(EXPERTS).astype(jnp.int32), gate_whole, up_whole, down_whole))
    gate_weight_grad = jnp.transpose(gate_all.reshape(EXPERTS, D, 2, FF_HALF), (0, 2, 1, 3)).reshape(N_SP, D, FF_HALF)
    up_weight_grad = jnp.transpose(up_all.reshape(EXPERTS, D, 2, FF_HALF), (0, 2, 1, 3)).reshape(N_SP, D, FF_HALF)
    down_weight_grad = down_all.reshape(N_SP, FF_HALF, D)
    gained = norm_gain[None, :] * normed_grad
    dotted = lax.optimization_barrier(jnp.sum(hidden * gained, axis=1))
    residual = cotangent.astype(jnp.float32) + inverse[:, None] * gained - hidden * (inverse ** 3 * dotted / D)[:, None]
    residual_grad = residual.astype(jnp.bfloat16)
    mix_grad = jnp.dot(residual_grad, out_proj, preferred_element_type=jnp.float32)
    per_group = HEADS // GROUPS
    scan_blocks = scan_input.reshape(BLOCKS, TOK_DEV, MIX)
    gate_blocks = out_gate.reshape(BLOCKS, TOK_DEV, MIX)
    step_blocks = jnp.transpose(step_size.reshape(HEADS, BLOCKS, TOK_DEV), (1, 0, 2))
    write_blocks = write_keys.reshape(BLOCKS, TOK_DEV, GROUPS * STATE)
    read_blocks = read_keys.reshape(BLOCKS, TOK_DEV, GROUPS * STATE)
    mix_blocks = mix_grad.reshape(BLOCKS, TOK_DEV, MIX)

    def forward_one(operands):
        scan_rows, gate_rows, step_rows, write_rows, read_rows, entry_state, mix_rows = operands
        return block_forward(scan_rows, gate_rows, step_rows, write_rows, read_rows, decay_rate, entry_state, mix_rows, per_group)
    gated, gate_grads, decays, carries, state_grads = lax.map(forward_one, (scan_blocks, gate_blocks, step_blocks, write_blocks, read_blocks, start_state, mix_blocks))

    def back_step(later_state, operands):
        decay_now, carry_now = operands
        return (carry_now + decay_now[:, None, None] * later_state, later_state)
    _, later_all = lax.scan(back_step, jnp.zeros((HEADS, HEAD_DIM, STATE), jnp.float32), (decays, carries), reverse=True)

    def back_one(operands):
        scan_rows, step_rows, write_rows, read_rows, entry_state, state_grad, later_state = operands
        return block_back(scan_rows, step_rows, write_rows, read_rows, decay_rate, entry_state, state_grad, later_state, per_group)
    scan_grads, write_grads, read_grads = lax.map(back_one, (scan_blocks, step_blocks, write_blocks, read_blocks, start_state, state_grads, later_all))
    gated_all = gated.reshape(TOKENS, MIX)
    out_proj_grad = jnp.dot(jnp.transpose(residual_grad), gated_all, preferred_element_type=jnp.float32)
    return (residual_grad, gate_weight_grad, up_weight_grad, down_weight_grad, out_proj_grad, scan_grads.reshape(TOKENS, MIX), gate_grads.reshape(TOKENS, MIX), write_grads.reshape(TOKENS, GROUPS * STATE), read_grads.reshape(TOKENS, GROUPS * STATE))
```

```python
import jax
import jax.numpy as jnp
from jax import lax
from jax.experimental import pallas as pl
from jax.experimental.pallas import tpu as pltpu
from jax.sharding import Mesh
from jax.sharding import PartitionSpec as P

D = 2048
HEADS = 16
STATE = 64
GROUPS = 4
SP = ("sp_0", "sp_1", "sp_2")


EPS = 1e-06
HIGHEST = lax.Precision.HIGHEST


MESH = pl.DeviceIdType.MESH
NZ, NX, NC, NY = 8, 4, 2, 4
CHIPS = NZ * NX
CAP = 16
HALF = CHIPS * CAP
QUARTER = 512


def position():
    return tuple(lax.axis_index(a) for a in ("sp_0", "sp_1", "sp_2", "tp"))


def at(z, x, c, y):
    return {"sp_0": z, "sp_1": x, "sp_2": c, "tp": y}


def remote(src, dst, send, recv, device):
    return pltpu.make_async_remote_copy(
        src_ref=src,
        dst_ref=dst,
        send_sem=send,
        recv_sem=recv,
        device_id=device,
        device_id_type=MESH,
    )


def signal(sem, device):
    pl.semaphore_signal(sem, inc=1, device_id=device, device_id_type=MESH)


def plane_peer(z, x, d):
    return lax.rem(z + d // NX, NZ), lax.rem(x + d % NX, NX)


def greet(z, x, c, y):
    barrier = pltpu.get_barrier_semaphore()

    def hello(d, carry):
        pz, px = plane_peer(z, x, d)
        signal(barrier, at(pz, px, c, y))
        return carry

    lax.fori_loop(1, CHIPS, hello, 0)
    signal(barrier, at(z, x, 1 - c, y))
    signal(barrier, at(z, x, c, lax.rem(y + 1, NY)))
    signal(barrier, at(z, x, c, lax.rem(y + 3, NY)))
    pl.semaphore_wait(barrier, CHIPS + 2)


CHUNKS = ((0, 0), (0, 1), (1, 0), (1, 1))
WIDE = QUARTER // 2


def dispatch_kernel(
    in_ref, cot_ref, gated_ref, rin_ref, rcot_ref, gz_ref, s1, r1, own_sem, sy, ry, sm, rm, sg, rg
):
    z, x, c, y = position()
    chip = z * NX + x
    up, down, far = lax.rem(y + 1, NY), lax.rem(y + 3, NY), lax.rem(y + 2, NY)
    greet(z, x, c, y)
    sources, targets = (in_ref, cot_ref), (rin_ref, rcot_ref)

    def cols(q, part):
        return pl.ds(pl.multiple_of(q * QUARTER + part * WIDE, WIDE), WIDE)

    def block(k, row, rows, q):
        array, part = CHUNKS[k]
        return targets[array].at[pl.ds(pl.multiple_of(row, CAP), rows), cols(q, part)]

    for k, (array, part) in enumerate(CHUNKS):
        local = pltpu.make_async_copy(
            sources[array].at[
                pl.ds(pl.multiple_of(chip * CAP, CAP), CAP), pl.ds(part * WIDE, WIDE)
            ],
            block(k, c * HALF + chip * CAP, CAP, y),
            own_sem.at[k],
        )
        local.start()

        def spread(d, carry):
            pz, px = plane_peer(z, x, d)
            peer = pz * NX + px
            remote(
                sources[array].at[
                    pl.ds(pl.multiple_of(peer * CAP, CAP), CAP), pl.ds(part * WIDE, WIDE)
                ],
                block(k, c * HALF + chip * CAP, CAP, y),
                s1.at[k],
                r1.at[k],
                at(pz, px, c, y),
            ).start()
            return carry

        lax.fori_loop(1, CHIPS, spread, 0)

    tokens_rows = gated_ref.shape[0]

    def gated_block(owner):
        return gz_ref.at[pl.ds(pl.multiple_of(owner * tokens_rows, 16), tokens_rows), :]

    gated_own = pltpu.make_async_copy(gated_ref, gated_block(z), own_sem.at[len(CHUNKS)])
    gated_own.start()

    def spread_gated(d, carry):
        remote(gated_ref, gated_block(z), sg, rg, at(lax.rem(z + d, NZ), x, c, y)).start()
        return carry

    lax.fori_loop(1, NZ, spread_gated, 0)

    mine, other = c * HALF, (1 - c) * HALF
    short = HALF - CAP
    part_rows = HALF // 2
    last = len(CHUNKS) - 1

    def relay(k, row, rows, q, slot):
        return remote(
            block(k, row, rows, q),
            block(k, row, rows, q),
            sm.at[k, slot],
            rm.at[k, slot],
            at(z, x, 1 - c, y),
        )

    def along(k, row, rows, q, slot, target):
        return remote(
            block(k, row, rows, q),
            block(k, row, rows, q),
            sy.at[k, slot],
            ry.at[k, slot],
            at(z, x, c, target),
        )

    def first(k):
        remote(
            block(k, 0, short, y), block(k, 0, short, y), s1.at[k], r1.at[k], at(z, x, c, up)
        ).wait_recv()
        pltpu.make_async_copy(
            block(k, 0, CAP, y), block(k, 0, CAP, y), own_sem.at[k]
        ).wait()
        along(k, mine, HALF, y, 0, up).start()
        along(k, mine, HALF, y, 1, down).start()
        relay(k, mine, HALF, y, 0).start()

    def second(k):
        along(k, mine, HALF, down, 0, up).wait_recv()
        along(k, mine, part_rows, down, 2, up).start()
        relay(k, mine, HALF, down, 1).start()
        along(k, mine, HALF, up, 1, down).wait_recv()
        along(k, mine + part_rows, part_rows, up, 3, down).start()
        relay(k, mine, HALF, up, 2).start()

    def third(k):
        along(k, mine, part_rows, far, 2, up).wait_recv()
        along(k, mine + part_rows, part_rows, far, 3, down).wait_recv()
        relay(k, mine, HALF, far, 3).start()

    for k in range(last + 1):
        first(k)
        if k >= 1:
            second(k - 1)
        if k >= 2:
            third(k - 2)
    second(last)
    third(last - 1)
    third(last)
    for k in range(last + 1):
        remote(
            block(k, 0, short, y), block(k, 0, short, y), s1.at[k], r1.at[k], at(z, x, c, up)
        ).wait_send()
        along(k, mine, HALF, y, 0, up).wait_send()
        along(k, mine, HALF, y, 1, down).wait_send()
        along(k, mine, part_rows, down, 2, up).wait_send()
        along(k, mine + part_rows, part_rows, up, 3, down).wait_send()
        for slot, q in enumerate((y, down, up, far)):
            relay(k, mine, HALF, q, slot).wait_send()
            relay(k, other, HALF, q, slot).wait_recv()
    gated_own.wait()
    seven = gz_ref.at[pl.ds(0, (NZ - 1) * tokens_rows), :]
    remote(seven, seven, sg, rg, at(z, x, c, up)).wait()


def dispatch(rows_in, rows_cot, gated):
    dma = pltpu.SemaphoreType.DMA
    n = len(CHUNKS)
    vmem, hbm = pl.BlockSpec(memory_space=pltpu.VMEM), pl.BlockSpec(memory_space=pl.ANY)
    return pl.pallas_call(
        dispatch_kernel,
        out_shape=(
            jax.ShapeDtypeStruct((2 * HALF, D), jnp.bfloat16),
            jax.ShapeDtypeStruct((2 * HALF, D), jnp.bfloat16),
            jax.ShapeDtypeStruct((NZ * gated.shape[0], gated.shape[1]), jnp.bfloat16),
        ),
        in_specs=[vmem] * 3,
        out_specs=(hbm, hbm, hbm),
        scratch_shapes=[
            dma((n,)),
            dma((n,)),
            dma((n + 1,)),
            dma((n, 4)),
            dma((n, 4)),
            dma((n, 4)),
            dma((n, 4)),
            dma,
            dma,
        ],
        compiler_params=pltpu.CompilerParams(collective_id=0, has_side_effects=True),
        name="dispatch",
    )(rows_in, rows_cot, gated)


def add_rows(target, t0, t1, pieces, step=64):
    rows = pieces[0][1]

    def body(i, carry):
        total = None
        for ref, _, r0, c0, width in pieces:
            value = ref[pl.ds(pl.multiple_of(r0 + i * step, 16), step), pl.ds(c0, width)].astype(
                jnp.float32
            )
            total = value if total is None else total + value
        target[
            pl.ds(pl.multiple_of(t0 + i * step, 16), step), pl.ds(t1, pieces[0][4])
        ] = total.astype(target.dtype)
        return carry

    lax.fori_loop(0, rows // step, body, 0)


def combine_kernel(
    part_ref, place_ref, out_ref, mate, acc, fwd, got, done, back, rows_out, sm, rm, sy, ry, sb, rb,
    sg, rg,
):
    z, x, c, y = position()
    chip = z * NX + x
    up, down, far = lax.rem(y + 1, NY), lax.rem(y + 3, NY), lax.rem(y + 2, NY)
    greet(z, x, c, y)
    mine, other = c * HALF, (1 - c) * HALF
    half = HALF // 2

    def cols(q):
        return pl.ds(pl.multiple_of(q * QUARTER, QUARTER), QUARTER)

    def rows(r0, n):
        return pl.ds(pl.multiple_of(r0, CAP), n)

    order = (far, up, down, y)
    for slot, q in enumerate(order):
        remote(
            part_ref.at[rows(other, HALF), cols(q)],
            mate.at[slot],
            sm.at[slot],
            rm.at[slot],
            at(z, x, 1 - c, y),
        ).start()

    def fold(slot):
        q = order[slot]
        remote(
            part_ref.at[rows(other, HALF), cols(q)],
            mate.at[slot],
            sm.at[slot],
            rm.at[slot],
            at(z, x, 1 - c, y),
        ).wait_recv()
        base = pl.multiple_of(q * QUARTER, QUARTER)

        def body(i, carry):
            at_rows = pl.ds(pl.multiple_of(i * 64, 64), 64)
            own = part_ref[
                pl.ds(pl.multiple_of(mine + i * 64, 64), 64), pl.ds(base, QUARTER)
            ].astype(jnp.float32)
            acc[slot, at_rows, :] = (own + mate[slot, at_rows, :].astype(jnp.float32)).astype(
                jnp.bfloat16
            )
            return carry

        lax.fori_loop(0, HALF // 64, body, 0)

    def along(src, dst, slot, target):
        return remote(src, dst, sy.at[slot], ry.at[slot], at(z, x, c, target))

    lo, hi = pl.ds(0, half), pl.ds(half, half)
    fold(0)
    f_up = along(acc.at[0, lo], fwd.at[0], 0, up)
    f_down = along(acc.at[0, hi], fwd.at[1], 1, down)
    f_up.start()
    f_down.start()
    fold(1)
    d_up = along(acc.at[1, hi], got.at[0, hi], 2, up)
    d_up.start()
    fold(2)
    d_down = along(acc.at[2, lo], got.at[1, lo], 3, down)
    d_down.start()

    def pass_on(slot, start, index):
        def body(i, carry):
            at_rows = pl.ds(pl.multiple_of(start + i * 64, 64), 64)
            from_rows = pl.ds(pl.multiple_of(i * 64, 64), 64)
            acc[slot, at_rows, :] = (
                acc[slot, at_rows, :].astype(jnp.float32)
                + fwd[index, from_rows, :].astype(jnp.float32)
            ).astype(jnp.bfloat16)
            return carry

        lax.fori_loop(0, half // 64, body, 0)

    f_up.wait_recv()
    pass_on(1, 0, 0)
    a_up = along(acc.at[1, lo], got.at[0, lo], 4, up)
    a_up.start()
    f_down.wait_recv()
    pass_on(2, half, 1)
    a_down = along(acc.at[2, hi], got.at[1, hi], 5, down)
    a_down.start()
    fold(3)
    d_up.wait_recv()
    d_down.wait_recv()

    def finish(start):
        def body(i, carry):
            at_rows = pl.ds(pl.multiple_of(start + i * 64, 64), 64)
            done[at_rows, :] = (
                acc[3, at_rows, :].astype(jnp.float32)
                + got[0, at_rows, :].astype(jnp.float32)
                + got[1, at_rows, :].astype(jnp.float32)
            ).astype(jnp.bfloat16)
            return carry

        lax.fori_loop(0, half // 64, body, 0)

    a_up.wait_recv()
    finish(0)
    a_down.wait_recv()
    finish(half)

    own_rows = pl.ds(pl.multiple_of(chip * CAP, CAP), CAP)

    def give_back(d, carry):
        pz, px = plane_peer(z, x, d)
        remote(
            done.at[rows((pz * NX + px) * CAP, CAP), :],
            back.at[own_rows, :],
            sb,
            rb,
            at(pz, px, c, y),
        ).start()
        return carry

    lax.fori_loop(1, CHIPS, give_back, 0)
    back[own_rows, :] = done[own_rows, :]
    short = pl.ds(0, HALF - CAP)
    all_back = remote(done.at[short, :], back.at[short, :], sb, rb, at(z, x, c, up))
    all_back.wait_recv()
    rows_out[y] = jnp.dot(
        place_ref[...], back[...], preferred_element_type=jnp.float32
    ).astype(jnp.bfloat16)
    n = rows_out.shape[1]
    first, second = pl.ds(0, n // 2), pl.ds(n // 2, n // 2)

    def share(q, piece, slot, target):
        return remote(
            rows_out.at[q, piece], rows_out.at[q, piece], sg.at[slot], rg.at[slot], at(z, x, c, target)
        )

    everything = pl.ds(0, n)
    share(y, everything, 0, up).start()
    share(y, everything, 1, down).start()
    share(down, everything, 0, up).wait_recv()
    share(down, first, 2, up).start()
    share(up, everything, 1, down).wait_recv()
    share(up, second, 3, down).start()
    out_ref[:, cols(y)] = rows_out[y]
    out_ref[:, cols(down)] = rows_out[down]
    out_ref[:, cols(up)] = rows_out[up]
    share(far, first, 2, up).wait_recv()
    share(far, second, 3, down).wait_recv()
    out_ref[:, cols(far)] = rows_out[far]
    for slot, q in enumerate(order):
        remote(
            part_ref.at[rows(other, HALF), cols(q)],
            mate.at[slot],
            sm.at[slot],
            rm.at[slot],
            at(z, x, 1 - c, y),
        ).wait_send()
    for copy in (f_up, f_down, d_up, d_down, a_up, a_down, all_back):
        copy.wait_send()
    share(y, everything, 0, up).wait_send()
    share(y, everything, 1, down).wait_send()
    share(down, first, 2, up).wait_send()
    share(up, second, 3, down).wait_send()


def combine(parts, place):
    dma = pltpu.SemaphoreType.DMA
    vmem = pl.BlockSpec(memory_space=pltpu.VMEM)
    tok_rows = place.shape[0]
    bf16 = jnp.bfloat16
    return pl.pallas_call(
        combine_kernel,
        out_shape=jax.ShapeDtypeStruct((tok_rows, D), bf16),
        in_specs=[vmem] * 2,
        out_specs=vmem,
        scratch_shapes=[
            pltpu.VMEM((NY, HALF, QUARTER), bf16),
            pltpu.VMEM((NY, HALF, QUARTER), bf16),
            pltpu.VMEM((2, HALF // 2, QUARTER), bf16),
            pltpu.VMEM((2, HALF, QUARTER), bf16),
            pltpu.VMEM((HALF, QUARTER), bf16),
            pltpu.VMEM((HALF, QUARTER), bf16),
            pltpu.VMEM((NY, tok_rows, QUARTER), bf16),
            dma((NY,)),
            dma((NY,)),
            dma((6,)),
            dma((6,)),
            dma,
            dma,
            dma((4,)),
            dma((4,)),
        ],
        compiler_params=pltpu.CompilerParams(collective_id=1, has_side_effects=True),
        name="combine",
    )(parts, place)


ROWS8 = 16
MESSAGE = 24


def carry_kernel(
    msg_ref, res_ref, gated_ref, later_ref, opg_ref, box_a, plane, box_b, fan, res_box, prod,
    opg_box, sa, ra, sb, rb, sc, rc, sr, rr, so, ro,
):
    z, x, c, y = position()
    w = x * NC + c
    barrier = pltpu.get_barrier_semaphore()

    def in_plane(d):
        p = lax.rem(w + d, NX * NC)
        return p, at(z, p // NC, p % NC, y)

    def in_line(d):
        p = lax.rem(z + d, NZ)
        return p, at(p, x, c, y)

    for d in range(1, 8):
        signal(barrier, in_plane(d)[1])
        signal(barrier, in_line(d)[1])
    pl.semaphore_wait(barrier, 14)

    for d in range(1, 8):
        p, device = in_plane(d)
        remote(msg_ref.at[p], box_a.at[w], sa.at[d], ra.at[d], device).start()
    box_a[w] = msg_ref[w]
    for d in range(1, 8):
        p, device = in_plane(d)
        source = lax.rem(w + 8 - d, 8)
        remote(msg_ref.at[p], box_a.at[source], sa.at[d], ra.at[d], device).wait_recv()

    data, scale = pl.ds(0, ROWS8), pl.ds(ROWS8, 8)

    def pair(ref, i):
        s = ref[i, scale, :]
        return ref[i, data, :], jnp.concatenate([s, s], axis=0)

    total = jnp.zeros((ROWS8, 128), jnp.float32)
    decay = jnp.ones((ROWS8, 128), jnp.float32)
    inside, inside_decay = [], []
    for k in reversed(range(8)):
        inside.append(total)
        inside_decay.append(decay)
        value, factor = pair(box_a, k)
        total = value + factor * total
        decay = factor * decay
    inside, inside_decay = inside[::-1], inside_decay[::-1]
    plane[data, :] = total
    plane[scale, :] = decay[0:8, :]
    box_b[z, data, :] = total
    box_b[z, scale, :] = decay[0:8, :]
    for d in range(1, 8):
        p, device = in_line(d)
        remote(plane, box_b.at[z], sb.at[d], rb.at[d], device).start()

    def feature_cols(p):
        return pl.ds(pl.multiple_of(p * 256, 256), 256)

    for d in range(1, 8):
        p, device = in_line(d)
        remote(res_ref.at[:, feature_cols(p)], res_box.at[z], sr.at[d], rr.at[d], device).start()
    for d in range(1, 8):
        p, device = in_line(d)
        source = lax.rem(z + 8 - d, 8)
        remote(plane, box_b.at[source], sb.at[d], rb.at[d], device).wait_recv()
    beyond = jnp.zeros((ROWS8, 128), jnp.float32)
    for k in reversed(range(1, 8)):
        value, factor = pair(box_b, k)
        beyond = jnp.where(k > z, value + factor * beyond, beyond)
    for k in range(8):
        fan[k] = inside[k] + inside_decay[k] * beyond

    def own_rows(p):
        return pl.ds(pl.multiple_of(p * ROWS8, ROWS8), ROWS8)

    for d in range(1, 8):
        p, device = in_plane(d)
        remote(fan.at[p], later_ref.at[own_rows(w), :], sc.at[d], rc.at[d], device).start()
    later_ref[own_rows(w), :] = fan[w]

    res_box[z] = res_ref[:, feature_cols(z)]
    for d in range(1, 8):
        p, device = in_line(d)
        source = lax.rem(z + 8 - d, 8)
        remote(
            res_ref.at[:, feature_cols(p)], res_box.at[source], sr.at[d], rr.at[d], device
        ).wait_recv()
    n = res_ref.shape[0]
    value = None
    for k in range(8):
        term = lax.dot_general(
            res_box[k],
            gated_ref[pl.ds(k * n, n), :],
            (((0,), (0,)), ((), ())),
            preferred_element_type=jnp.float32,
        )
        value = term if value is None else value + term
    prod[...] = value.reshape(prod.shape)
    for d in range(1, 8):
        p, device = in_plane(d)
        remote(prod.at[p], opg_box.at[w], so.at[d], ro.at[d], device).start()
    opg_box[w] = prod[w]
    for d in range(1, 8):
        p, device = in_plane(d)
        source = lax.rem(w + 8 - d, 8)
        remote(prod.at[p], opg_box.at[source], so.at[d], ro.at[d], device).wait_recv()
    opg = opg_box[0]
    for k in range(1, 8):
        opg = opg + opg_box[k]
    opg_ref[...] = opg
    for d in range(1, 8):
        p, device = in_plane(d)
        source = lax.rem(w + 8 - d, 8)
        remote(fan.at[p], later_ref.at[own_rows(source), :], sc.at[d], rc.at[d], device).wait_recv()
        remote(msg_ref.at[p], box_a.at[w], sa.at[d], ra.at[d], device).wait_send()
        remote(fan.at[p], later_ref.at[own_rows(w), :], sc.at[d], rc.at[d], device).wait_send()
        remote(prod.at[p], opg_box.at[w], so.at[d], ro.at[d], device).wait_send()
        p, device = in_line(d)
        remote(plane, box_b.at[z], sb.at[d], rb.at[d], device).wait_send()
        remote(
            res_ref.at[:, feature_cols(p)], res_box.at[z], sr.at[d], rr.at[d], device
        ).wait_send()


def exchange_carry(messages, residual_grad, gated_line):
    dma = pltpu.SemaphoreType.DMA
    vmem = pl.BlockSpec(memory_space=pltpu.VMEM)
    f32 = jnp.float32
    n, channels = residual_grad.shape[0], gated_line.shape[1]
    return pl.pallas_call(
        carry_kernel,
        out_shape=(
            jax.ShapeDtypeStruct((128, 128), f32),
            jax.ShapeDtypeStruct((32, channels), f32),
        ),
        in_specs=[vmem] * 3,
        out_specs=(vmem, vmem),
        scratch_shapes=[
            pltpu.VMEM((8, MESSAGE, 128), f32),
            pltpu.VMEM((MESSAGE, 128), f32),
            pltpu.VMEM((8, MESSAGE, 128), f32),
            pltpu.VMEM((8, ROWS8, 128), f32),
            pltpu.VMEM((8, n, 256), jnp.bfloat16),
            pltpu.VMEM((8, 32, channels), f32),
            pltpu.VMEM((8, 32, channels), f32),
        ]
        + [dma((8,))] * 10,
        compiler_params=pltpu.CompilerParams(collective_id=2, has_side_effects=True),
        name="carry",
    )(messages, residual_grad, gated_line)


def prepare(scan_rows, step_rows, write_rows, read_rows, decay_rates, per_group):
    length = scan_rows.shape[0]
    head_count = step_rows.shape[0]
    logdec = jnp.cumsum(-decay_rates[:, None] * step_rows, axis=1)
    causal = jnp.arange(length)[:, None] >= jnp.arange(length)[None, :]
    spread = jnp.where(causal[None, :, :], logdec[:, :, None] - logdec[:, None, :], -jnp.inf)
    weights = jnp.exp(spread)
    inputs = (
        scan_rows.astype(jnp.float32).reshape(length, head_count, -1)
        * jnp.transpose(step_rows)[:, :, None]
    )
    write_head = jnp.repeat(
        write_rows.astype(jnp.float32).reshape(length, -1, STATE), per_group, axis=1
    )
    read_head = jnp.repeat(
        read_rows.astype(jnp.float32).reshape(length, -1, STATE), per_group, axis=1
    )
    scores = jnp.einsum("thn,shn->hts", read_head, write_head, precision=HIGHEST) * weights
    return (logdec, weights, inputs, write_head, read_head, scores)


def block_back(
    step_rows,
    logdec,
    weights,
    inputs,
    write_head,
    read_head,
    scores,
    entry_state,
    state_grad,
    later_state,
    per_group,
):
    length, head_count = (inputs.shape[0], inputs.shape[1])
    growth = jnp.transpose(jnp.exp(logdec))
    shrink = jnp.transpose(jnp.exp(logdec[:, -1:] - logdec))
    in_grad = jnp.einsum("hts,thp->shp", scores, state_grad, precision=HIGHEST)
    in_grad = in_grad + shrink[:, :, None] * jnp.einsum(
        "shn,hpn->shp", write_head, later_state, precision=HIGHEST
    )
    scan_grad = (
        (in_grad * jnp.transpose(step_rows)[:, :, None]).reshape(length, -1).astype(jnp.bfloat16)
    )
    pair_terms = jnp.einsum("thp,shp->hts", state_grad, inputs, precision=HIGHEST) * weights
    read_grad = jnp.einsum("hts,shn->thn", pair_terms, write_head, precision=HIGHEST)
    read_grad = read_grad + growth[:, :, None] * jnp.einsum(
        "thp,hpn->thn", state_grad, entry_state, precision=HIGHEST
    )
    write_grad = jnp.einsum("hts,thn->shn", pair_terms, read_head, precision=HIGHEST)
    write_grad = write_grad + shrink[:, :, None] * jnp.einsum(
        "shp,hpn->shn", inputs, later_state, precision=HIGHEST
    )
    group_count = head_count // per_group
    read_total = (
        jnp.sum(read_grad.reshape(length, group_count, per_group, -1), axis=2)
        .reshape(length, -1)
        .astype(jnp.bfloat16)
    )
    write_total = (
        jnp.sum(write_grad.reshape(length, group_count, per_group, -1), axis=2)
        .reshape(length, -1)
        .astype(jnp.bfloat16)
    )
    return (scan_grad, write_total, read_total)


def expert_grads(rows_in, rows_cot, gate_mat, up_mat, down_mat):
    contract_rows = (((0,), (0,)), ((), ()))
    contract_cols = (((1,), (1,)), ((), ()))
    gate_pre = jnp.dot(rows_in, gate_mat, preferred_element_type=jnp.float32)
    up_pre = jnp.dot(rows_in, up_mat, preferred_element_type=jnp.float32)
    sigmoid_val = jax.nn.sigmoid(gate_pre)
    active = (gate_pre * sigmoid_val * up_pre).astype(jnp.bfloat16)
    down_grad = lax.dot_general(active, rows_cot, contract_rows, preferred_element_type=jnp.float32)
    act_grad = lax.dot_general(
        rows_cot, down_mat, contract_cols, preferred_element_type=jnp.float32
    )
    gate_pre_grad = (
        act_grad * up_pre * sigmoid_val * (1.0 + gate_pre * (1.0 - sigmoid_val))
    ).astype(jnp.bfloat16)
    up_pre_grad = (act_grad * gate_pre * sigmoid_val).astype(jnp.bfloat16)
    gate_grad = lax.dot_general(
        rows_in, gate_pre_grad, contract_rows, preferred_element_type=jnp.float32
    )
    up_grad = lax.dot_general(
        rows_in, up_pre_grad, contract_rows, preferred_element_type=jnp.float32
    )
    input_grad = lax.dot_general(
        gate_pre_grad, gate_mat, contract_cols, preferred_element_type=jnp.float32
    )
    input_grad = input_grad + lax.dot_general(
        up_pre_grad, up_mat, contract_cols, preferred_element_type=jnp.float32
    )
    return (gate_grad, up_grad, down_grad, input_grad)


def shards(
    tokens,
    norm_gain,
    cotangent,
    routes,
    route_weight,
    gate_weight,
    up_weight,
    down_weight,
    scan_input,
    out_gate,
    step_size,
    decay_rate,
    write_keys,
    read_keys,
    start_state,
    out_proj,
):
    tok_rows = tokens.shape[0]
    experts_count = CHIPS
    y = lax.axis_index("tp")
    hidden = tokens.astype(jnp.float32)
    inverse = lax.rsqrt(jnp.mean(hidden * hidden, axis=1) + EPS)

    def quarter_of(a):
        return lax.dynamic_slice_in_dim(a, y * QUARTER, QUARTER, a.ndim - 1)

    normed_q = (
        quarter_of(tokens).astype(jnp.float32) * inverse[:, None] * quarter_of(norm_gain)[None, :]
    ).astype(jnp.bfloat16)
    cot_q = quarter_of(cotangent)
    route_flat = routes.reshape(-1)
    member = (route_flat[:, None] == jnp.arange(experts_count, dtype=jnp.int32)[None, :]).astype(
        jnp.int32
    )
    earlier_count = jnp.sum((jnp.cumsum(member, axis=0) - member) * member, axis=1)
    places = (route_flat * CAP + earlier_count).reshape(tok_rows, 2)
    slot_ids = jnp.arange(experts_count * CAP, dtype=jnp.int32)[:, None]
    first_hit = slot_ids == places[None, :, 0]
    second_hit = slot_ids == places[None, :, 1]
    placing = jnp.logical_or(first_hit, second_hit)
    place_matrix = placing.astype(jnp.bfloat16)
    slot_weight = jnp.sum(
        jnp.where(first_hit, route_weight[None, :, 0], 0.0)
        + jnp.where(second_hit, route_weight[None, :, 1], 0.0),
        axis=1,
    )
    send_in = jnp.dot(place_matrix, normed_q, preferred_element_type=jnp.float32).astype(
        jnp.bfloat16
    )
    send_cot = (
        slot_weight[:, None] * jnp.dot(place_matrix, cot_q, preferred_element_type=jnp.float32)
    ).astype(jnp.bfloat16)
    per_group = HEADS // GROUPS
    entry_state = start_state[0]
    logdec, weights, inputs, write_head, read_head, scores = prepare(
        scan_input, step_size, write_keys, read_keys, decay_rate, per_group
    )
    head_count = inputs.shape[1]
    growth = jnp.transpose(jnp.exp(logdec))
    scan_out = jnp.einsum("hts,shp->thp", scores, inputs, precision=HIGHEST)
    scan_out = scan_out + growth[:, :, None] * jnp.einsum(
        "thn,hpn->thp", read_head, entry_state, precision=HIGHEST
    )
    gate_val = out_gate.astype(jnp.float32).reshape(tok_rows, head_count, -1)
    sigmoid_val = jax.nn.sigmoid(gate_val)
    gated = (scan_out * gate_val * sigmoid_val).reshape(tok_rows, -1).astype(jnp.bfloat16)
    rows_in, rows_cot, gated_line = dispatch(send_in, send_cot, gated)
    gate_grad, up_grad, down_grad, input_part = expert_grads(
        rows_in, rows_cot, gate_weight[0], up_weight[0], down_weight[0]
    )
    normed_grad = combine(
        input_part.astype(jnp.bfloat16), jnp.transpose(place_matrix)
    ).astype(jnp.float32)
    gained = norm_gain[None, :] * normed_grad
    dotted = jnp.sum(hidden * gained, axis=1)
    residual = (
        cotangent.astype(jnp.float32)
        + inverse[:, None] * gained
        - hidden * (inverse**3 * dotted / D)[:, None]
    )
    residual_grad = residual.astype(jnp.bfloat16)
    mix_grad = jnp.dot(residual_grad, out_proj, preferred_element_type=jnp.float32)
    out_grad = mix_grad.reshape(tok_rows, head_count, -1)
    state_grad = out_grad * gate_val * sigmoid_val
    gate_out_grad = (
        (out_grad * scan_out * sigmoid_val * (1.0 + gate_val * (1.0 - sigmoid_val)))
        .reshape(tok_rows, -1)
        .astype(jnp.bfloat16)
    )
    carried = jnp.einsum("th,thp,thn->hpn", growth, state_grad, read_head, precision=HIGHEST)
    decay_now = jnp.exp(logdec[:, -1])
    messages = jnp.concatenate(
        [
            carried.reshape(8, ROWS8, 128),
            jnp.broadcast_to(jnp.repeat(decay_now, 2)[:, None, None], (8, 8, 128)),
        ],
        axis=1,
    )
    later, out_proj_grad = exchange_carry(messages, residual_grad, gated_line)
    later_state = later.reshape(head_count, 64, 64)
    scan_grad, write_grad, read_grad = block_back(
        step_size,
        logdec,
        weights,
        inputs,
        write_head,
        read_head,
        scores,
        entry_state,
        state_grad,
        later_state,
        per_group,
    )
    residual_part = quarter_of(residual_grad)
    return (
        residual_part,
        gate_grad.astype(jnp.bfloat16)[None],
        up_grad.astype(jnp.bfloat16)[None],
        down_grad.astype(jnp.bfloat16)[None],
        out_proj_grad,
        scan_grad,
        gate_out_grad,
        write_grad,
        read_grad,
    )


def solution(mesh):
    finer = Mesh(mesh.devices.reshape(8, 4, 2, mesh.shape["tp"]), ("sp_0", "sp_1", "sp_2", "tp"))
    in_specs = (
        P(SP, None),
        P(),
        P(SP, None),
        P(SP, None),
        P(SP, None),
        P(SP, None, "tp"),
        P(SP, None, "tp"),
        P(SP, "tp", None),
        P(SP, "tp"),
        P(SP, "tp"),
        P("tp", SP),
        P("tp"),
        P(SP, "tp"),
        P(SP, "tp"),
        P(SP, "tp", None, None),
        P(None, "tp"),
    )
    out_specs = (
        P(SP, "tp"),
        P(SP, None, "tp"),
        P(SP, None, "tp"),
        P(SP, "tp", None),
        P(SP, "tp"),
        P(SP, "tp"),
        P(SP, "tp"),
        P(SP, "tp"),
        P(SP, "tp"),
    )
    return jax.shard_map(
        shards, mesh=finer, in_specs=in_specs, out_specs=out_specs, check_vma=False
    )
```

```python
import jax
import jax.numpy as jnp
from jax import lax
from jax.experimental import pallas as pl
from jax.experimental.pallas import tpu as pltpu
from jax.sharding import Mesh
from jax.sharding import PartitionSpec as P

D = 2048
HEADS = 16
STATE = 64
GROUPS = 4
SP = ("sp_0", "sp_1", "sp_2")


EPS = 1e-06
HIGHEST = lax.Precision.HIGHEST


MESH = pl.DeviceIdType.MESH
NZ, NX, NC, NY = 8, 4, 2, 4
NW = NX * NC
CHIPS = NZ * NX
CAP = 16
HALF = CHIPS * CAP
ROWS = 2 * HALF
QUARTER = 512
HID = 448
TOK = 128
CH = 256
HD = 64
LOCAL_HEADS = 4
BF16, F32 = jnp.bfloat16, jnp.float32
CHUNKS = ((0, 0), (0, 1), (1, 0), (1, 1))
WIDE = QUARTER // 2
PIECE = 32
NT = (((1,), (1,)), ((), ()))
TN = (((0,), (0,)), ((), ()))
NN = (((1,), (0,)), ((), ()))


def position():
    return tuple(lax.axis_index(a) for a in ("sp_0", "sp_1", "sp_2", "tp"))


def at(z, x, c, y):
    return {"sp_0": z, "sp_1": x, "sp_2": c, "tp": y}


def remote(src, dst, send, recv, device):
    return pltpu.make_async_remote_copy(
        src_ref=src,
        dst_ref=dst,
        send_sem=send,
        recv_sem=recv,
        device_id=device,
        device_id_type=MESH,
    )


def signal(sem, device):
    pl.semaphore_signal(sem, inc=1, device_id=device, device_id_type=MESH)


def plane_peer(z, x, d):
    return lax.rem(z + d // NX, NZ), lax.rem(x + d % NX, NX)


def greet(z, x, c, y):
    barrier = pltpu.get_barrier_semaphore()

    def hello(d, carry):
        pz, px = plane_peer(z, x, d)
        signal(barrier, at(pz, px, c, y))
        return carry

    lax.fori_loop(1, CHIPS, hello, 0)
    for d in range(NX):
        signal(barrier, at(z, lax.rem(x + d, NX), 1 - c, y))
    signal(barrier, at(z, x, c, lax.rem(y + 1, NY)))
    signal(barrier, at(z, x, c, lax.rem(y + 3, NY)))
    pl.semaphore_wait(barrier, CHIPS - 1 + NX + 2)


def times(n, body):
    def step(i, carry):
        body(i)
        return carry

    lax.fori_loop(0, n, step, 0)


def mult(i, n):
    return pl.multiple_of(i * n, n)


def dot(a, b, dims, precision=None):
    return lax.dot_general(a, b, dims, preferred_element_type=F32, precision=precision)


def layer_kernel(
    in_ref, cot_ref, gated_ref, place_ref, tok_ref, cotan_ref, gain_ref, inv_ref, og_ref, scan_ref,
    growth_ref, read_ref, gw_hbm, uw_hbm, dw_hbm, ow_hbm,
    gg_hbm, ug_hbm, dg_hbm, res_out, opg_out, sg_out, gog_out, later_out,
    rin, rcot, gz, wts, ow, accg, accu, acca, act_t, gp_t, up_t, gp, up_g, wg, po, pm, mate, acc,
    fwd, got, done, back, share_buf, ng, res, msg, box_a, plane, box_b, fan, res_box, prod, opg_box,
    lw, s1, r1, sy, ry, sm, rm, sgz, rgz, spm, rpm, sf, rf, sb, rb, ss, rs, sa, ra, sbb, rbb, sc,
    rc, sr, rr, so, ro,
):
    z, x, c, y = position()
    chip = z * NX + x
    w = x * NC + c
    up, down, far = lax.rem(y + 1, NY), lax.rem(y + 3, NY), lax.rem(y + 2, NY)
    mine, other = c * HALF, (1 - c) * HALF
    part_rows = HALF // 2
    loads = [
        pltpu.make_async_copy(gw_hbm, wts.at[0], lw.at[0]),
        pltpu.make_async_copy(uw_hbm, wts.at[1], lw.at[1]),
        pltpu.make_async_copy(dw_hbm, wts.at[2], lw.at[2]),
        pltpu.make_async_copy(ow_hbm, ow, lw.at[3]),
    ]
    for load in loads:
        load.start()
    sources, targets = (in_ref, cot_ref), (rin, rcot)
    own_rows = pl.ds(pl.multiple_of(chip * CAP, CAP), CAP)
    kept_rows = pl.ds(pl.multiple_of(mine + chip * CAP, CAP), CAP)
    own_cols = pl.ds(mult(y, QUARTER), QUARTER)
    rin[kept_rows, own_cols] = in_ref[own_rows, :]
    rcot[kept_rows, own_cols] = cot_ref[own_rows, :]
    own_tokens = pl.ds(mult(z, TOK), TOK)
    gz[own_tokens, :] = gated_ref[...]
    greet(z, x, c, y)

    def block(k, row, rows, q):
        array, part = CHUNKS[k]
        return targets[array].at[
            pl.ds(pl.multiple_of(row, CAP), rows),
            pl.ds(pl.multiple_of(q * QUARTER + part * WIDE, WIDE), WIDE),
        ]

    short = HALF - CAP

    def issue(k):
        array, part = CHUNKS[k]

        def spread(d, carry):
            pz, px = plane_peer(z, x, d)
            remote(
                sources[array].at[
                    pl.ds(pl.multiple_of((pz * NX + px) * CAP, CAP), CAP), pl.ds(part * WIDE, WIDE)
                ],
                block(k, mine + chip * CAP, CAP, y),
                s1.at[k],
                r1.at[k],
                at(pz, px, c, y),
            ).start()
            return carry

        lax.fori_loop(1, CHIPS, spread, 0)

    def whole(k):
        array, part = CHUNKS[k]
        return remote(
            sources[array].at[pl.ds(0, short), pl.ds(part * WIDE, WIDE)],
            block(k, 0, short, y),
            s1.at[k],
            r1.at[k],
            at(z, x, c, up),
        )

    def relay(k, row, q, slot):
        return remote(
            block(k, row, HALF, q), block(k, row, HALF, q), sm.at[k, slot], rm.at[k, slot],
            at(z, x, 1 - c, y),
        )

    def along(k, row, rows, q, slot, target):
        return remote(
            block(k, row, rows, q), block(k, row, rows, q), sy.at[k, slot], ry.at[k, slot],
            at(z, x, c, target),
        )

    def first(k):
        whole(k).wait_recv()
        along(k, mine, HALF, y, 0, up).start()
        along(k, mine, HALF, y, 1, down).start()
        relay(k, mine, y, 0).start()

    def second(k):
        along(k, mine, HALF, down, 0, up).wait_recv()
        along(k, mine, part_rows, down, 2, up).start()
        relay(k, mine, down, 1).start()
        along(k, mine, HALF, up, 1, down).wait_recv()
        along(k, mine + part_rows, part_rows, up, 3, down).start()
        relay(k, mine, up, 2).start()

    def third(k):
        along(k, mine, part_rows, far, 2, up).wait_recv()
        along(k, mine + part_rows, part_rows, far, 3, down).wait_recv()
        relay(k, mine, far, 3).start()

    def gather(k):
        for slot, q in enumerate((y, down, up, far)):
            relay(k, other, q, slot).wait_recv()

    def forward(k):
        array, part = CHUNKS[k]
        pairs = ((0, accg), (1, accu)) if array == 0 else ((2, acca),)
        rows_ref = targets[array]
        fresh = part == 0

        def body(n):
            nrows = pl.ds(mult(n, 256), 256)
            for index, total in pairs:
                value = None
                for q in range(NY):
                    cols = pl.ds(q * QUARTER + part * WIDE, WIDE)
                    term = dot(wts[index, :, cols], rows_ref[nrows, cols], NT)
                    value = term if value is None else value + term
                if fresh:
                    total[:, nrows] = value
                else:
                    total[:, nrows] += value

        times(ROWS // 256, body)

    def activate():
        def body(i):
            r = pl.ds(mult(i, 16), 16)
            g, u = accg[r, :], accu[r, :]
            s = jax.nn.sigmoid(g)
            silu = g * s
            act_t[r, :] = (silu * u).astype(BF16)
            accu[r, :] = u * s * (1.0 + g * (1.0 - s))
            accg[r, :] = silu

        times(HID // 16, body)

    def grads():
        def body(i):
            r = pl.ds(mult(i, 16), 16)
            a = acca[r, :]
            g = a * accu[r, :]
            u = a * accg[r, :]
            accu[r, :] = g
            accg[r, :] = u
            gp_t[r, :] = g.astype(BF16)
            up_t[r, :] = u.astype(BF16)

        times(HID // 16, body)

        def turn(j):
            cols = pl.ds(mult(j, 128), 128)
            gp[cols, :] = jnp.transpose(accu[:, cols]).astype(BF16)
            up_g[cols, :] = jnp.transpose(accg[:, cols]).astype(BF16)

        times(ROWS // 128, turn)

    issue(0)
    whole(0).wait_send()
    issue(1)
    first(0)
    whole(1).wait_send()
    issue(2)
    first(1)
    second(0)
    whole(2).wait_send()
    issue(3)
    first(2)
    second(1)
    third(0)
    loads[0].wait()
    loads[1].wait()
    gather(0)
    forward(0)
    first(3)
    whole(3).wait_send()

    def line_peer(d):
        p = lax.rem(z + d, NZ)
        return p, at(p, x, c, y)

    def plane_mate(d):
        p = lax.rem(w + d, NW)
        return p, at(z, p // NC, p % NC, y)

    for d in range(1, NZ):
        remote(gated_ref, gz.at[own_tokens, :], sgz, rgz, line_peer(d)[1]).start()
    second(2)
    third(1)
    gather(1)
    forward(1)
    activate()
    second(3)
    third(2)
    loads[2].wait()
    gather(2)
    forward(2)
    third(3)
    gather(3)
    forward(3)
    grads()

    order = (far, up, down, y)

    def product(slot, row, target):
        cols = pl.ds(mult(order[slot], QUARTER), QUARTER)

        def body(i):
            r = pl.ds(pl.multiple_of(row + i * 128, 128), 128)
            value = dot(gp[r, :], wts[0, :, cols], NN) + dot(up_g[r, :], wts[1, :, cols], NN)
            target[slot, pl.ds(mult(i, 128), 128), :] = value.astype(target.dtype)

        times(HALF // 128, body)

    def to_mate(slot):
        return remote(po.at[slot], mate.at[slot], spm.at[slot], rpm.at[slot], at(z, x, 1 - c, y))

    def fold(slot):
        to_mate(slot).wait_recv()

        def body(i):
            r = pl.ds(mult(i, 32), 32)
            acc[slot, r, :] = (pm[slot, r, :] + mate[slot, r, :].astype(F32)).astype(BF16)

        times(HALF // 32, body)

    lo, hi = pl.ds(0, part_rows), pl.ds(part_rows, part_rows)

    def part(ch):
        return pl.ds(ch * WIDE, WIDE)

    def ring(src, dst, slot, ch, target):
        return remote(src, dst, sf.at[slot, ch], rf.at[slot, ch], at(z, x, c, target))

    def f_up(ch):
        return ring(acc.at[0, lo, part(ch)], fwd.at[0, :, part(ch)], 0, ch, up)

    def f_down(ch):
        return ring(acc.at[0, hi, part(ch)], fwd.at[1, :, part(ch)], 1, ch, down)

    def d_up(ch):
        return ring(acc.at[1, hi, part(ch)], got.at[0, hi, part(ch)], 2, ch, up)

    def d_down(ch):
        return ring(acc.at[2, lo, part(ch)], got.at[1, lo, part(ch)], 3, ch, down)

    def a_up(ch):
        return ring(acc.at[1, lo, part(ch)], got.at[0, lo, part(ch)], 4, ch, up)

    def a_down(ch):
        return ring(acc.at[2, hi, part(ch)], got.at[1, hi, part(ch)], 5, ch, down)

    def pass_on(slot, start, index, ch):
        def body(i):
            r = pl.ds(pl.multiple_of(start + i * 32, 32), 32)
            f = pl.ds(mult(i, 32), 32)
            acc[slot, r, part(ch)] = (
                acc[slot, r, part(ch)].astype(F32) + fwd[index, f, part(ch)].astype(F32)
            ).astype(BF16)

        times(part_rows // 32, body)

    def finish(ch):
        def body(i):
            r = pl.ds(mult(i, 32), 32)
            done[r, part(ch)] = (
                acc[3, r, part(ch)].astype(F32)
                + got[0, r, part(ch)].astype(F32)
                + got[1, r, part(ch)].astype(F32)
            ).astype(BF16)

        times(HALF // 32, body)

    def give_back(ch):
        def spread(d, carry):
            pz, px = plane_peer(z, x, d)
            remote(
                done.at[pl.ds(pl.multiple_of((pz * NX + px) * CAP, CAP), CAP), part(ch)],
                back.at[own_rows, part(ch)],
                sb.at[ch],
                rb.at[ch],
                at(pz, px, c, y),
            ).start()
            return carry

        lax.fori_loop(1, CHIPS, spread, 0)
        back[own_rows, part(ch)] = done[own_rows, part(ch)]

    def all_back(ch):
        piece = (pl.ds(0, short), part(ch))
        return remote(done.at[piece], back.at[piece], sb.at[ch], rb.at[ch], at(z, x, c, up))

    def weight_grads(start, stop):
        def step(i, carry):
            cols = pl.ds(mult(i, 256), 256)
            wg[0, :, cols] = dot(gp_t[...], rin[:, cols], NN).astype(BF16)
            wg[1, :, cols] = dot(up_t[...], rin[:, cols], NN).astype(BF16)
            wg[2, :, cols] = dot(act_t[...], rcot[:, cols], NN).astype(BF16)
            return carry

        lax.fori_loop(start, stop, step, 0)

    product(0, other, po)
    to_mate(0).start()
    product(0, mine, pm)
    product(1, other, po)
    to_mate(1).start()
    fold(0)
    f_up(0).start()
    f_down(0).start()
    product(1, mine, pm)
    product(2, other, po)
    to_mate(2).start()
    fold(1)
    d_up(0).start()
    product(2, mine, pm)
    product(3, other, po)
    to_mate(3).start()
    fold(2)
    d_down(0).start()
    f_up(1).start()
    f_down(1).start()
    product(3, mine, pm)
    fold(3)
    f_up(0).wait_recv()
    pass_on(1, 0, 0, 0)
    a_up(0).start()
    f_down(0).wait_recv()
    pass_on(2, part_rows, 1, 0)
    a_down(0).start()
    d_up(1).start()
    d_down(1).start()
    weight_grads(0, 3)
    f_up(1).wait_recv()
    pass_on(1, 0, 0, 1)
    a_up(1).start()
    f_down(1).wait_recv()
    pass_on(2, part_rows, 1, 1)
    a_down(1).start()
    d_up(0).wait_recv()
    d_down(0).wait_recv()
    a_up(0).wait_recv()
    a_down(0).wait_recv()
    finish(0)
    give_back(0)
    weight_grads(3, 6)
    d_up(1).wait_recv()
    d_down(1).wait_recv()
    a_up(1).wait_recv()
    a_down(1).wait_recv()
    finish(1)
    give_back(1)

    first_rows, second_rows = pl.ds(0, TOK // 2), pl.ds(TOK // 2, TOK // 2)
    everything = pl.ds(0, TOK)

    def share(q, piece, slot, target, ch):
        ref = share_buf.at[q, piece, part(ch)]
        return remote(ref, ref, ss.at[slot, ch], rs.at[slot, ch], at(z, x, c, target))

    def place(ch):
        all_back(ch).wait_recv()
        share_buf[y, :, part(ch)] = dot(place_ref[...], back[:, part(ch)], NN).astype(BF16)
        share(y, everything, 0, up, ch).start()
        share(y, everything, 1, down, ch).start()

    def pass_shares(ch):
        share(down, everything, 0, up, ch).wait_recv()
        share(down, first_rows, 2, up, ch).start()
        share(up, everything, 1, down, ch).wait_recv()
        share(up, second_rows, 3, down, ch).start()

    place(0)
    weight_grads(6, 8)
    outs = [
        pltpu.make_async_copy(wg.at[i], hbm, lw.at[4 + i])
        for i, hbm in enumerate((gg_hbm, ug_hbm, dg_hbm))
    ]
    for out in outs:
        out.start()
    pass_shares(0)
    place(1)
    pass_shares(1)
    for ch in range(2):
        share(far, first_rows, 2, up, ch).wait_recv()
        share(far, second_rows, 3, down, ch).wait_recv()

    inv = inv_ref[...]
    dotted = jnp.zeros((TOK, 1), F32)
    for q in range(NY):
        cols = pl.ds(q * QUARTER, QUARTER)
        gained = gain_ref[:, cols] * share_buf[q].astype(F32)
        dotted += jnp.sum(tok_ref[:, cols].astype(F32) * gained, axis=1, keepdims=True)
    coef = inv * inv * inv * dotted / D
    mix = None
    loads[3].wait()
    for q in range(NY):
        cols = pl.ds(q * QUARTER, QUARTER)
        gained = gain_ref[:, cols] * share_buf[q].astype(F32)
        value = (
            cotan_ref[:, cols].astype(F32) + inv * gained - tok_ref[:, cols].astype(F32) * coef
        ).astype(BF16)
        res[:, cols] = value
        term = dot(value, ow[cols, :], NN)
        mix = term if mix is None else mix + term
    res_out[...] = res[:, own_cols]
    res_box[z] = res[:, pl.ds(mult(z, CH), CH)]

    def send_res(d):
        p, device = line_peer(d)
        return remote(
            res.at[:, pl.ds(mult(p, CH), CH)], res_box.at[z], sr.at[d], rr.at[d], device
        )

    def recv_res(d):
        source = lax.rem(z + NZ - d, NZ)
        p, device = line_peer(d)
        return remote(
            res.at[:, pl.ds(mult(p, CH), CH)], res_box.at[source], sr.at[d], rr.at[d], device
        )

    og = og_ref[...].astype(F32)
    sig = jax.nn.sigmoid(og)
    state = mix * og * sig
    sg_out[...] = state
    gog_out[...] = (mix * scan_ref[...] * sig * (1.0 + og * (1.0 - sig))).astype(BF16)
    read = read_ref[...].astype(F32)
    for h in range(LOCAL_HEADS):
        grown = growth_ref[:, h : h + 1] * state[:, h * HD : (h + 1) * HD]
        carried = dot(grown, read, TN, HIGHEST)
        last = growth_ref[TOK - 1 : TOK, h : h + 1]
        for i in range(2):
            msg[2 * h + i, 0:PIECE, :] = carried[i * PIECE : (i + 1) * PIECE, :]
            msg[2 * h + i, PIECE : PIECE + 8, :] = jnp.broadcast_to(last, (8, HD))
    for d in range(1, NW):
        p, device = plane_mate(d)
        remote(msg.at[p], box_a.at[w], sa.at[d], ra.at[d], device).start()
    for d in (1, 7, 2, 6):
        send_res(d).start()
    box_a[w] = msg[w]

    def source_of(d):
        return lax.rem(w + NW - d, NW)

    for d in range(1, NW):
        p, device = plane_mate(d)
        remote(msg.at[p], box_a.at[source_of(d)], sa.at[d], ra.at[d], device).wait_recv()
    data, scale = pl.ds(0, PIECE), pl.ds(PIECE, 8)

    def pair(ref, i):
        s = ref[i, scale, :]
        return ref[i, data, :], jnp.concatenate([s] * (PIECE // 8), axis=0)

    total = jnp.zeros((PIECE, HD), F32)
    decay = jnp.ones((PIECE, HD), F32)
    inside, inside_decay = [], []
    for k in reversed(range(NW)):
        inside.append(total)
        inside_decay.append(decay)
        value, factor = pair(box_a, k)
        total = value + factor * total
        decay = factor * decay
    inside, inside_decay = inside[::-1], inside_decay[::-1]
    plane[data, :] = total
    plane[scale, :] = decay[0:8, :]
    box_b[z, data, :] = total
    box_b[z, scale, :] = decay[0:8, :]
    for d in range(1, NZ):
        remote(plane, box_b.at[z], sbb.at[d], rbb.at[d], line_peer(d)[1]).start()
    for d in (3, 5, 4):
        send_res(d).start()
    for d in range(1, NZ):
        source = lax.rem(z + NZ - d, NZ)
        remote(plane, box_b.at[source], sbb.at[d], rbb.at[d], line_peer(d)[1]).wait_recv()
    beyond = jnp.zeros((PIECE, HD), F32)
    for k in reversed(range(1, NZ)):
        value, factor = pair(box_b, k)
        beyond = jnp.where(k > z, value + factor * beyond, beyond)
    for k in range(NW):
        fan[k] = inside[k] + inside_decay[k] * beyond

    def slot_of(p):
        return later_out.at[p // 2, pl.ds(mult(p % 2, PIECE), PIECE), :]

    for d in range(1, NW):
        p, device = plane_mate(d)
        remote(fan.at[p], slot_of(w), sc.at[d], rc.at[d], device).start()
    later_out[w // 2, pl.ds(mult(w % 2, PIECE), PIECE), :] = fan[w]
    seven = gz.at[pl.ds(0, (NZ - 1) * TOK), :]
    remote(seven, seven, sgz, rgz, at(z, x, c, up)).wait()
    for d in range(1, NZ):
        recv_res(d).wait_recv()
    value = None
    for k in range(NZ):
        term = dot(res_box[k], gz[pl.ds(k * TOK, TOK), :], TN)
        value = term if value is None else value + term
    prod[...] = value.reshape(prod.shape)
    for d in range(1, NW):
        p, device = plane_mate(d)
        remote(prod.at[p], opg_box.at[w], so.at[d], ro.at[d], device).start()
    opg_box[w] = prod[w]
    for d in range(1, NW):
        p, device = plane_mate(d)
        remote(prod.at[p], opg_box.at[source_of(d)], so.at[d], ro.at[d], device).wait_recv()
    opg = opg_box[0]
    for k in range(1, NW):
        opg = opg + opg_box[k]
    opg_out[...] = opg

    for d in range(1, NW):
        p, device = plane_mate(d)
        remote(fan.at[p], slot_of(source_of(d)), sc.at[d], rc.at[d], device).wait_recv()
        remote(msg.at[p], box_a.at[w], sa.at[d], ra.at[d], device).wait_send()
        remote(fan.at[p], slot_of(w), sc.at[d], rc.at[d], device).wait_send()
        remote(prod.at[p], opg_box.at[w], so.at[d], ro.at[d], device).wait_send()
        remote(plane, box_b.at[z], sbb.at[d], rbb.at[d], line_peer(d)[1]).wait_send()
        send_res(d).wait_send()
    for k in range(len(CHUNKS)):
        along(k, mine, HALF, y, 0, up).wait_send()
        along(k, mine, HALF, y, 1, down).wait_send()
        along(k, mine, part_rows, down, 2, up).wait_send()
        along(k, mine + part_rows, part_rows, up, 3, down).wait_send()
        for slot, q in enumerate((y, down, up, far)):
            relay(k, mine, q, slot).wait_send()
    for slot in range(NY):
        to_mate(slot).wait_send()
    for ch in range(2):
        for copy in (f_up, f_down, d_up, d_down, a_up, a_down, all_back):
            copy(ch).wait_send()
        share(y, everything, 0, up, ch).wait_send()
        share(y, everything, 1, down, ch).wait_send()
        share(down, first_rows, 2, up, ch).wait_send()
        share(up, second_rows, 3, down, ch).wait_send()
    for out in outs:
        out.wait()


def layer(*operands):
    dma = pltpu.SemaphoreType.DMA
    vmem, hbm = pl.BlockSpec(memory_space=pltpu.VMEM), pl.BlockSpec(memory_space=pl.ANY)
    n = len(CHUNKS)
    shape = jax.ShapeDtypeStruct
    wide = shape((HID, D), BF16)
    return pl.pallas_call(
        layer_kernel,
        out_shape=(
            wide,
            wide,
            wide,
            shape((TOK, QUARTER), BF16),
            shape((32, CH), F32),
            shape((TOK, CH), F32),
            shape((TOK, CH), BF16),
            shape((LOCAL_HEADS, HD, HD), F32),
        ),
        in_specs=[vmem] * 12 + [hbm] * 4,
        out_specs=(hbm,) * 3 + (vmem,) * 5,
        scratch_shapes=[
            pltpu.VMEM((ROWS, D), BF16),
            pltpu.VMEM((ROWS, D), BF16),
            pltpu.VMEM((NZ * TOK, CH), BF16),
            pltpu.VMEM((3, HID, D), BF16),
            pltpu.VMEM((D, CH), BF16),
            pltpu.VMEM((HID, ROWS), F32),
            pltpu.VMEM((HID, ROWS), F32),
            pltpu.VMEM((HID, ROWS), F32),
            pltpu.VMEM((HID, ROWS), BF16),
            pltpu.VMEM((HID, ROWS), BF16),
            pltpu.VMEM((HID, ROWS), BF16),
            pltpu.VMEM((ROWS, HID), BF16),
            pltpu.VMEM((ROWS, HID), BF16),
            pltpu.VMEM((3, HID, D), BF16),
            pltpu.VMEM((NY, HALF, QUARTER), BF16),
            pltpu.VMEM((NY, HALF, QUARTER), F32),
            pltpu.VMEM((NY, HALF, QUARTER), BF16),
            pltpu.VMEM((NY, HALF, QUARTER), BF16),
            pltpu.VMEM((2, HALF // 2, QUARTER), BF16),
            pltpu.VMEM((2, HALF, QUARTER), BF16),
            pltpu.VMEM((HALF, QUARTER), BF16),
            pltpu.VMEM((HALF, QUARTER), BF16),
            pltpu.VMEM((NY, TOK, QUARTER), BF16),
            pltpu.VMEM((8, 128), F32),
            pltpu.VMEM((TOK, D), BF16),
            pltpu.VMEM((NW, PIECE + 8, HD), F32),
            pltpu.VMEM((NW, PIECE + 8, HD), F32),
            pltpu.VMEM((PIECE + 8, HD), F32),
            pltpu.VMEM((NZ, PIECE + 8, HD), F32),
            pltpu.VMEM((NW, PIECE, HD), F32),
            pltpu.VMEM((NZ, TOK, CH), BF16),
            pltpu.VMEM((NW, 32, CH), F32),
            pltpu.VMEM((NW, 32, CH), F32),
            dma((7,)),
            dma((n,)),
            dma((n,)),
            dma((n, 4)),
            dma((n, 4)),
            dma((n, 4)),
            dma((n, 4)),
            dma,
            dma,
            dma((NY,)),
            dma((NY,)),
            dma((6, 2)),
            dma((6, 2)),
            dma((2,)),
            dma((2,)),
            dma((4, 2)),
            dma((4, 2)),
        ]
        + [dma((8,))] * 10,
        compiler_params=pltpu.CompilerParams(
            collective_id=0, has_side_effects=True, vmem_limit_bytes=62 * 1024 * 1024
        ),
        name="layer",
    )(*operands)


def prepare(scan_rows, step_rows, write_rows, read_rows, decay_rates, per_group):
    length = scan_rows.shape[0]
    head_count = step_rows.shape[0]
    logdec = jnp.cumsum(-decay_rates[:, None] * step_rows, axis=1)
    causal = jnp.arange(length)[:, None] >= jnp.arange(length)[None, :]
    spread = jnp.where(causal[None, :, :], logdec[:, :, None] - logdec[:, None, :], -jnp.inf)
    weights = jnp.exp(spread)
    inputs = (
        scan_rows.astype(jnp.float32).reshape(length, head_count, -1)
        * jnp.transpose(step_rows)[:, :, None]
    )
    write_head = jnp.repeat(
        write_rows.astype(jnp.float32).reshape(length, -1, STATE), per_group, axis=1
    )
    read_head = jnp.repeat(
        read_rows.astype(jnp.float32).reshape(length, -1, STATE), per_group, axis=1
    )
    scores = jnp.einsum("thn,shn->hts", read_head, write_head, precision=HIGHEST) * weights
    return (logdec, weights, inputs, write_head, read_head, scores)


def block_back(
    step_rows,
    logdec,
    weights,
    inputs,
    write_head,
    read_head,
    scores,
    entry_state,
    state_grad,
    later_state,
    per_group,
):
    length, head_count = (inputs.shape[0], inputs.shape[1])
    growth = jnp.transpose(jnp.exp(logdec))
    shrink = jnp.transpose(jnp.exp(logdec[:, -1:] - logdec))
    in_grad = jnp.einsum("hts,thp->shp", scores, state_grad, precision=HIGHEST)
    in_grad = in_grad + shrink[:, :, None] * jnp.einsum(
        "shn,hpn->shp", write_head, later_state, precision=HIGHEST
    )
    scan_grad = (
        (in_grad * jnp.transpose(step_rows)[:, :, None]).reshape(length, -1).astype(jnp.bfloat16)
    )
    pair_terms = jnp.einsum("thp,shp->hts", state_grad, inputs, precision=HIGHEST) * weights
    read_grad = jnp.einsum("hts,shn->thn", pair_terms, write_head, precision=HIGHEST)
    read_grad = read_grad + growth[:, :, None] * jnp.einsum(
        "thp,hpn->thn", state_grad, entry_state, precision=HIGHEST
    )
    write_grad = jnp.einsum("hts,thn->shn", pair_terms, read_head, precision=HIGHEST)
    write_grad = write_grad + shrink[:, :, None] * jnp.einsum(
        "shp,hpn->shn", inputs, later_state, precision=HIGHEST
    )
    group_count = head_count // per_group
    read_total = (
        jnp.sum(read_grad.reshape(length, group_count, per_group, -1), axis=2)
        .reshape(length, -1)
        .astype(jnp.bfloat16)
    )
    write_total = (
        jnp.sum(write_grad.reshape(length, group_count, per_group, -1), axis=2)
        .reshape(length, -1)
        .astype(jnp.bfloat16)
    )
    return (scan_grad, write_total, read_total)


def shards(
    tokens,
    norm_gain,
    cotangent,
    routes,
    route_weight,
    gate_weight,
    up_weight,
    down_weight,
    scan_input,
    out_gate,
    step_size,
    decay_rate,
    write_keys,
    read_keys,
    start_state,
    out_proj,
):
    tok_rows = tokens.shape[0]
    experts_count = CHIPS
    y = lax.axis_index("tp")
    hidden = tokens.astype(jnp.float32)
    inverse = lax.rsqrt(jnp.mean(hidden * hidden, axis=1) + EPS)

    def quarter_of(a):
        return lax.dynamic_slice_in_dim(a, y * QUARTER, QUARTER, a.ndim - 1)

    normed_q = (
        quarter_of(tokens).astype(jnp.float32) * inverse[:, None] * quarter_of(norm_gain)[None, :]
    ).astype(jnp.bfloat16)
    cot_q = quarter_of(cotangent)
    route_flat = routes.reshape(-1)
    member = (route_flat[:, None] == jnp.arange(experts_count, dtype=jnp.int32)[None, :]).astype(
        jnp.int32
    )
    earlier_count = jnp.sum((jnp.cumsum(member, axis=0) - member) * member, axis=1)
    places = (route_flat * CAP + earlier_count).reshape(tok_rows, 2)
    slot_ids = jnp.arange(experts_count * CAP, dtype=jnp.int32)[:, None]
    first_hit = slot_ids == places[None, :, 0]
    second_hit = slot_ids == places[None, :, 1]
    placing = jnp.logical_or(first_hit, second_hit)
    place_matrix = placing.astype(jnp.bfloat16)
    slot_weight = jnp.sum(
        jnp.where(first_hit, route_weight[None, :, 0], 0.0)
        + jnp.where(second_hit, route_weight[None, :, 1], 0.0),
        axis=1,
    )
    send_in = jnp.dot(place_matrix, normed_q, preferred_element_type=jnp.float32).astype(
        jnp.bfloat16
    )
    send_cot = (
        slot_weight[:, None] * jnp.dot(place_matrix, cot_q, preferred_element_type=jnp.float32)
    ).astype(jnp.bfloat16)
    per_group = HEADS // GROUPS
    entry_state = start_state[0]
    logdec, weights, inputs, write_head, read_head, scores = prepare(
        scan_input, step_size, write_keys, read_keys, decay_rate, per_group
    )
    head_count = inputs.shape[1]
    growth = jnp.transpose(jnp.exp(logdec))
    scan_out = jnp.einsum("hts,shp->thp", scores, inputs, precision=HIGHEST)
    scan_out = scan_out + growth[:, :, None] * jnp.einsum(
        "thn,hpn->thp", read_head, entry_state, precision=HIGHEST
    )
    gate_val = out_gate.astype(jnp.float32).reshape(tok_rows, head_count, -1)
    sigmoid_val = jax.nn.sigmoid(gate_val)
    gated = (scan_out * gate_val * sigmoid_val).reshape(tok_rows, -1).astype(jnp.bfloat16)
    (
        gate_grad,
        up_grad,
        down_grad,
        residual_part,
        out_proj_grad,
        state_grad,
        gate_out_grad,
        later_state,
    ) = layer(
        send_in,
        send_cot,
        gated,
        jnp.transpose(place_matrix),
        tokens,
        cotangent,
        norm_gain[None, :],
        inverse[:, None],
        out_gate,
        scan_out.reshape(tok_rows, -1),
        growth,
        read_keys,
        jnp.transpose(gate_weight[0]),
        jnp.transpose(up_weight[0]),
        down_weight[0],
        out_proj,
    )
    state_grad = state_grad.reshape(tok_rows, head_count, -1)
    scan_grad, write_grad, read_grad = block_back(
        step_size,
        logdec,
        weights,
        inputs,
        write_head,
        read_head,
        scores,
        entry_state,
        state_grad,
        later_state,
        per_group,
    )
    return (
        residual_part,
        jnp.transpose(gate_grad)[None],
        jnp.transpose(up_grad)[None],
        down_grad[None],
        out_proj_grad,
        scan_grad,
        gate_out_grad,
        write_grad,
        read_grad,
    )


def solution(mesh):
    finer = Mesh(mesh.devices.reshape(8, 4, 2, mesh.shape["tp"]), ("sp_0", "sp_1", "sp_2", "tp"))
    in_specs = (
        P(SP, None),
        P(),
        P(SP, None),
        P(SP, None),
        P(SP, None),
        P(SP, None, "tp"),
        P(SP, None, "tp"),
        P(SP, "tp", None),
        P(SP, "tp"),
        P(SP, "tp"),
        P("tp", SP),
        P("tp"),
        P(SP, "tp"),
        P(SP, "tp"),
        P(SP, "tp", None, None),
        P(None, "tp"),
    )
    out_specs = (
        P(SP, "tp"),
        P(SP, None, "tp"),
        P(SP, None, "tp"),
        P(SP, "tp", None),
        P(SP, "tp"),
        P(SP, "tp"),
        P(SP, "tp"),
        P(SP, "tp"),
        P(SP, "tp"),
    )
    return jax.shard_map(
        shards, mesh=finer, in_specs=in_specs, out_specs=out_specs, check_vma=False
    )
```

```python
import jax
import jax.numpy as jnp
from jax import lax
from jax.experimental import pallas as pl
from jax.experimental.pallas import tpu as pltpu
from jax.sharding import Mesh
from jax.sharding import PartitionSpec as P

D = 2048
HEADS = 16
STATE = 64
GROUPS = 4
SP = ("sp_0", "sp_1", "sp_2")


EPS = 1e-06
HIGHEST = lax.Precision.HIGHEST


MESH = pl.DeviceIdType.MESH
NZ, NX, NC, NY = 8, 4, 2, 4
NW = NX * NC
CHIPS = NZ * NX
CAP = 16
HALF = CHIPS * CAP
ROWS = 2 * HALF
QUARTER = 512
HID = 448
TOK = 128
CH = 256
HD = 64
LOCAL_HEADS = 4
BF16, F32 = jnp.bfloat16, jnp.float32
WIDE = QUARTER // 2
DIRECT = 512
RING = (D - DIRECT) // NY
CHUNKS = (
    (0, 0, 128, 0, QUARTER),
    (0, 128, 128, 128, QUARTER),
    (0, 256, 256, 256, QUARTER),
    (1, 0, 256, DIRECT, RING),
    (1, 256, 128, DIRECT + 256, RING),
    (1, RING, 256, 0, 0),
    (1, RING + 256, 256, 256, 0),
)
RINGED = 5
SLICE = TOK // NY
PARTS = ((0, 256), (256, 128), (384, 128))
PIECE = 16
PACK = 128
NT = (((1,), (1,)), ((), ()))
TN = (((0,), (0,)), ((), ()))
NN = (((1,), (0,)), ((), ()))


def position():
    return tuple(lax.axis_index(a) for a in ("sp_0", "sp_1", "sp_2", "tp"))


def at(z, x, c, y):
    return {"sp_0": z, "sp_1": x, "sp_2": c, "tp": y}


def remote(src, dst, send, recv, device):
    return pltpu.make_async_remote_copy(
        src_ref=src,
        dst_ref=dst,
        send_sem=send,
        recv_sem=recv,
        device_id=device,
        device_id_type=MESH,
    )


def signal(sem, device):
    pl.semaphore_signal(sem, inc=1, device_id=device, device_id_type=MESH)


def plane_peer(z, x, d):
    return lax.rem(z + d // NX, NZ), lax.rem(x + d % NX, NX)


def greet(barrier, z, x, c, y):

    def hello(d, carry):
        pz, px = plane_peer(z, x, d)
        signal(barrier, at(pz, px, c, y))
        return carry

    lax.fori_loop(1, CHIPS, hello, 0)
    for d in range(NX):
        signal(barrier, at(z, lax.rem(x + d, NX), 1 - c, y))
    signal(barrier, at(z, x, c, lax.rem(y + 1, NY)))
    signal(barrier, at(z, x, c, lax.rem(y + 3, NY)))


def times(n, body):
    def step(i, carry):
        body(i)
        return carry

    lax.fori_loop(0, n, step, 0)


def mult(i, n):
    return pl.multiple_of(i * n, n)


def dot(a, b, dims, precision=None):
    return lax.dot_general(a, b, dims, preferred_element_type=F32, precision=precision)


def layer_kernel(
    tok_hbm, cotan_hbm, gain_hbm, routes_hbm, route_weight_hbm, og_hbm, scan_in_hbm, step_hbm,
    rate_ref, keys_hbm, reads_hbm, state_hbm, gw_hbm, uw_hbm, dw_hbm, ow_hbm,
    gg_hbm, ug_hbm, dg_hbm, res_hbm, opg_hbm, scan_hbm, gog_hbm, write_hbm, read_hbm,
    sin, scot, slots, rin, rcot, gated, gz, wts, ow, accg, accu, acca, act_t, gp_t, up_t, gp, up_g,
    wg, po, pm, mate, acc, fwd, got, done, back, share_buf, res, msg, box_a, plane, box_b, fan,
    later, res_box, prod, opg_box, pairs_w, scores, heads_u, heads_silu, heads_gate, heads_sg,
    heads_in, cols_t, reads, writes, res_out, opg_out, scan_out, gog_out, write_out, read_out,
    tok_ref, cotan_ref, gain_ref, routes_ref, route_weight_ref, og_ref, scan_ref, step_ref,
    write_ref, read_ref, state_ref, tok_part, cotan_part, gain_part, li, lw, s1, r1, sy, ry, sm, rm, sgz, rgz, spm, rpm, sf, rf, sb, rb, ss, rs, sq, rq, sa, ra, sbb, rbb,
    sc, rc, sr, rr, so, ro,
):
    z, x, c, y = position()
    chip = z * NX + x
    w = x * NC + c
    up, down, far = lax.rem(y + 1, NY), lax.rem(y + 3, NY), lax.rem(y + 2, NY)
    mine, other = c * HALF, (1 - c) * HALF
    part_rows = HALF // 2
    barrier = pltpu.get_barrier_semaphore()
    own_cols = pl.ds(mult(y, QUARTER), QUARTER)
    ring_cols = pl.ds(pl.multiple_of(DIRECT + y * RING, 128), RING)
    staged_inputs = [
        (routes_hbm, routes_ref),
        (route_weight_hbm, route_weight_ref),
        (gain_hbm, gain_ref),
        (tok_hbm, tok_ref),
        (cotan_hbm, cotan_ref),
        (tok_hbm.at[:, own_cols], tok_part),
        (cotan_hbm.at[:, ring_cols], cotan_part),
        (gain_hbm.at[:, own_cols], gain_part),
        (step_hbm, step_ref),
        (keys_hbm, write_ref),
        (reads_hbm, read_ref),
        (scan_in_hbm, scan_ref),
        (og_hbm, og_ref),
        (state_hbm, state_ref),
    ]
    inputs = [
        pltpu.make_async_copy(hbm, ref, li.at[i]) for i, (hbm, ref) in enumerate(staged_inputs)
    ]
    for copy in inputs:
        copy.start()
    early_inputs, late_inputs = inputs[:8], inputs[8:]
    greet(barrier, z, x, c, y)
    for copy in early_inputs:
        copy.wait()
    loads = [
        pltpu.make_async_copy(gw_hbm, wts.at[0], lw.at[0]),
        pltpu.make_async_copy(uw_hbm, wts.at[1], lw.at[1]),
        pltpu.make_async_copy(dw_hbm, wts.at[2], lw.at[2]),
        pltpu.make_async_copy(ow_hbm, ow, lw.at[3]),
    ]
    for load in loads:
        load.start()
    sources, targets = (sin, scot), (rin, rcot)
    own_rows = pl.ds(pl.multiple_of(chip * CAP, CAP), CAP)
    kept_rows = pl.ds(pl.multiple_of(mine + chip * CAP, CAP), CAP)

    squares = jnp.zeros((TOK, 1), F32)
    for q in range(NY):
        value = tok_ref[:, q * QUARTER : (q + 1) * QUARTER].astype(F32)
        squares += jnp.sum(value * value, axis=1, keepdims=True)
    inv = lax.rsqrt(squares / D + EPS)
    earlier = (
        lax.broadcasted_iota(jnp.int32, (TOK, TOK), 0) < lax.broadcasted_iota(jnp.int32, (TOK, TOK), 1)
    ).astype(BF16)
    expert = lax.broadcasted_iota(jnp.int32, (CHIPS, TOK), 0)
    names = [routes_ref[k : k + 1, :] for k in range(2)]
    members = [(expert == name).astype(F32) for name in names]
    counts = dot((members[0] + members[1]).astype(BF16), earlier, NN)
    slot = lax.broadcasted_iota(jnp.int32, (HALF, TOK), 0).astype(F32)
    hits = [
        slot == name.astype(F32) * CAP + jnp.sum(member * counts, axis=0, keepdims=True)
        for name, member in zip(names, members)
    ]
    slots[...] = jnp.logical_or(hits[0], hits[1]).astype(BF16)
    slot_weight = jnp.sum(
        jnp.where(hits[0], route_weight_ref[0:1, :], 0.0)
        + jnp.where(hits[1], route_weight_ref[1:2, :], 0.0),
        axis=1,
        keepdims=True,
    )
    normed = (tok_part[...].astype(F32) * inv * gain_part[...]).astype(BF16)
    sin[...] = dot(slots[...], normed, NN).astype(BF16)
    scot[:, 0:RING] = (slot_weight * dot(slots[...], cotan_part[...], NN)).astype(BF16)
    scot[:, RING:] = (slot_weight * dot(slots[...], cotan_ref[:, 0:DIRECT], NN)).astype(BF16)
    rin[kept_rows, own_cols] = sin[own_rows, :]
    rcot[kept_rows, ring_cols] = scot[own_rows, 0:RING]
    rcot[kept_rows, 0:DIRECT] = scot[own_rows, RING:]
    pl.semaphore_wait(barrier, CHIPS - 1 + NX + 2)

    def block(k, row, rows, q):
        array, _, width, base, stride = CHUNKS[k]
        return targets[array].at[
            pl.ds(pl.multiple_of(row, CAP), rows),
            pl.ds(pl.multiple_of(base + q * stride, 128), width),
        ]

    short = HALF - CAP

    def staged(k, rows):
        array, column, width, _, _ = CHUNKS[k]
        return sources[array].at[rows, pl.ds(column, width)]

    def issue(k):
        def spread(d, carry):
            pz, px = plane_peer(z, x, d)
            remote(
                staged(k, pl.ds(pl.multiple_of((pz * NX + px) * CAP, CAP), CAP)),
                block(k, mine + chip * CAP, CAP, y),
                s1.at[k],
                r1.at[k],
                at(pz, px, c, y),
            ).start()
            return carry

        lax.fori_loop(1, CHIPS, spread, 0)

    def whole(k):
        return remote(
            staged(k, pl.ds(0, short)), block(k, 0, short, y), s1.at[k], r1.at[k], at(z, x, c, up)
        )

    def relay(k, row, q, slot):
        return remote(
            block(k, row, HALF, q), block(k, row, HALF, q), sm.at[k, slot], rm.at[k, slot],
            at(z, x, 1 - c, y),
        )

    def along(k, row, rows, q, slot, target):
        return remote(
            block(k, row, rows, q), block(k, row, rows, q), sy.at[k, slot], ry.at[k, slot],
            at(z, x, c, target),
        )

    def first(k):
        whole(k).wait_recv()
        along(k, mine, HALF, y, 0, up).start()
        along(k, mine, HALF, y, 1, down).start()
        relay(k, mine, y, 0).start()

    def second(k):
        along(k, mine, HALF, down, 0, up).wait_recv()
        along(k, mine, part_rows, down, 2, up).start()
        relay(k, mine, down, 1).start()
        along(k, mine, HALF, up, 1, down).wait_recv()
        along(k, mine + part_rows, part_rows, up, 3, down).start()
        relay(k, mine, up, 2).start()

    def third(k):
        along(k, mine, part_rows, far, 2, up).wait_recv()
        along(k, mine + part_rows, part_rows, far, 3, down).wait_recv()
        relay(k, mine, far, 3).start()

    def straight(k):
        whole(k).wait_recv()
        relay(k, mine, 0, 0).start()

    def gather(k):
        for slot, q in enumerate((y, down, up, far)):
            if slot == 0 or k < RINGED:
                relay(k, other, q, slot).wait_recv()

    def forward(array, columns, width, fresh):
        pairs = ((0, accg), (1, accu)) if array == 0 else ((2, acca),)
        rows_ref = targets[array]

        def body(n):
            nrows = pl.ds(mult(n, 256), 256)
            for index, total in pairs:
                value = None
                for group in columns:
                    left = [wts[index, :, column : column + width] for column in group]
                    right = [rows_ref[nrows, column : column + width] for column in group]
                    if len(group) > 1:
                        left = [jnp.concatenate(left, axis=1)]
                        right = [jnp.concatenate(right, axis=1)]
                    term = dot(left[0], right[0], NT)
                    value = term if value is None else value + term
                if fresh:
                    total[:, nrows] = value
                else:
                    total[:, nrows] += value

        times(ROWS // 256, body)

    def activate():
        def body(i):
            r = pl.ds(mult(i, 16), 16)
            g, u = accg[r, :], accu[r, :]
            s = jax.nn.sigmoid(g)
            silu = g * s
            act_t[r, :] = (silu * u).astype(BF16)
            accu[r, :] = u * s * (1.0 + g * (1.0 - s))
            accg[r, :] = silu

        times(HID // 16, body)

    def grads():
        def body(i):
            r = pl.ds(mult(i, 16), 16)
            a = acca[r, :]
            g = a * accu[r, :]
            u = a * accg[r, :]
            accu[r, :] = g
            accg[r, :] = u
            gp_t[r, :] = g.astype(BF16)
            up_t[r, :] = u.astype(BF16)

        times(HID // 16, body)

        def turn(j):
            cols = pl.ds(mult(j, 128), 128)
            gp[cols, :] = jnp.transpose(accu[:, cols]).astype(BF16)
            up_g[cols, :] = jnp.transpose(accg[:, cols]).astype(BF16)

        times(ROWS // 128, turn)

    def prepare():
        reads[...] = jnp.transpose(read_ref[...].astype(F32))
        writes[...] = jnp.transpose(write_ref[...].astype(F32))
        upto = (
            lax.broadcasted_iota(jnp.int32, (TOK, TOK), 0)
            <= lax.broadcasted_iota(jnp.int32, (TOK, TOK), 1)
        ).astype(F32)
        delta = jnp.concatenate(
            [-rate_ref[h] * step_ref[h : h + 1, :] for h in range(LOCAL_HEADS)], axis=0
        )
        logdec = dot(delta, upto, NN, HIGHEST)
        columns = jnp.transpose(jnp.concatenate([logdec, step_ref[...]], axis=0))
        cols_t[...] = columns
        causal = lax.broadcasted_iota(jnp.int32, (TOK, TOK), 0) >= lax.broadcasted_iota(
            jnp.int32, (TOK, TOK), 1
        )
        keys = dot(read_ref[...], write_ref[...], TN)
        for h in range(LOCAL_HEADS):
            spread = jnp.where(causal, columns[:, h : h + 1] - logdec[h : h + 1, :], -jnp.inf)
            weights = jnp.exp(spread)
            pairs_w[h] = weights
            scores[h] = keys * weights

    def scan_head(h):
        lanes = slice(h * HD, (h + 1) * HD)
        u = scan_ref[:, lanes].astype(F32) * cols_t[:, LOCAL_HEADS + h : LOCAL_HEADS + h + 1]
        heads_u[h] = u
        value = dot(scores[h], u, NN, HIGHEST)
        value += jnp.exp(cols_t[:, h : h + 1]) * dot(reads[...], state_ref[h], NT, HIGHEST)
        og = og_ref[:, lanes].astype(F32)
        sig = jax.nn.sigmoid(og)
        gated[:, lanes] = (value * og * sig).astype(BF16)
        heads_silu[h] = og * sig
        heads_gate[h] = value * sig * (1.0 + og * (1.0 - sig))

    def line_peer(d):
        p = lax.rem(z + d, NZ)
        return p, at(p, x, c, y)

    def plane_mate(d):
        p = lax.rem(w + d, NW)
        return p, at(z, p // NC, p % NC, y)

    own_tokens = pl.ds(mult(z, TOK), TOK)
    ring_in = [(q * QUARTER,) for q in range(NY)]
    next_in = [(q * QUARTER + 256,) for q in range(NY)]
    ring_cot = [(DIRECT + q * RING,) for q in range(NY)]
    last_cot = [tuple(DIRECT + q * RING + 256 for q in pair) for pair in ((0, 1), (2, 3))]
    issue(0)
    for copy in late_inputs:
        copy.wait()
    prepare()
    whole(0).wait_send()
    issue(1)
    scan_head(0)
    first(0)
    whole(1).wait_send()
    issue(2)
    scan_head(1)
    first(1)
    scan_head(2)
    second(0)
    whole(2).wait_send()
    issue(3)
    scan_head(3)
    gz[own_tokens, :] = gated[...]
    second(1)
    first(2)
    whole(3).wait_send()
    issue(4)
    third(0)
    third(1)
    first(3)
    whole(4).wait_send()
    issue(5)
    loads[0].wait()
    loads[1].wait()
    second(2)
    first(4)
    gather(0)
    gather(1)
    forward(0, ring_in, 256, True)
    whole(5).wait_send()
    issue(6)
    second(3)
    for d in range(1, NZ):
        remote(gated, gz.at[own_tokens, :], sgz, rgz, line_peer(d)[1]).start()
    straight(5)
    third(2)
    gather(2)
    forward(0, next_in, 256, False)
    second(4)
    activate()
    straight(6)
    third(3)
    loads[2].wait()
    gather(3)
    forward(1, ring_cot, 256, True)
    gather(5)
    gather(6)
    forward(1, [(0,)], DIRECT, False)
    third(4)
    gather(4)
    forward(1, last_cot, 128, False)
    grads()

    order = (far, up, down, y)

    def product(slot, row, target):
        cols = pl.ds(mult(order[slot], QUARTER), QUARTER)

        def body(i):
            r = pl.ds(pl.multiple_of(row + i * 256, 256), 256)
            value = dot(gp[r, :], wts[0, :, cols], NN) + dot(up_g[r, :], wts[1, :, cols], NN)
            target[slot, pl.ds(mult(i, 256), 256), :] = value.astype(target.dtype)

        times(HALF // 256, body)

    def to_mate(slot):
        return remote(po.at[slot], mate.at[slot], spm.at[slot], rpm.at[slot], at(z, x, 1 - c, y))

    def fold(slot):
        to_mate(slot).wait_recv()

        def body(i):
            r = pl.ds(mult(i, 32), 32)
            acc[slot, r, :] = (pm[slot, r, :] + mate[slot, r, :].astype(F32)).astype(BF16)

        times(HALF // 32, body)

    lo, hi = pl.ds(0, part_rows), pl.ds(part_rows, part_rows)

    def part(ch):
        return pl.ds(*PARTS[ch])

    def ring(src, dst, slot, ch, target):
        return remote(src, dst, sf.at[slot, ch], rf.at[slot, ch], at(z, x, c, target))

    def f_up(ch):
        return ring(acc.at[0, lo, part(ch)], fwd.at[0, :, part(ch)], 0, ch, up)

    def f_down(ch):
        return ring(acc.at[0, hi, part(ch)], fwd.at[1, :, part(ch)], 1, ch, down)

    def d_up(ch):
        return ring(acc.at[1, hi, part(ch)], got.at[0, hi, part(ch)], 2, ch, up)

    def d_down(ch):
        return ring(acc.at[2, lo, part(ch)], got.at[1, lo, part(ch)], 3, ch, down)

    def a_up(ch):
        return ring(acc.at[1, lo, part(ch)], got.at[0, lo, part(ch)], 4, ch, up)

    def a_down(ch):
        return ring(acc.at[2, hi, part(ch)], got.at[1, hi, part(ch)], 5, ch, down)

    def pass_on(slot, start, index, ch):
        def body(i):
            r = pl.ds(pl.multiple_of(start + i * 32, 32), 32)
            f = pl.ds(mult(i, 32), 32)
            acc[slot, r, part(ch)] = (
                acc[slot, r, part(ch)].astype(F32) + fwd[index, f, part(ch)].astype(F32)
            ).astype(BF16)

        times(part_rows // 32, body)

    def finish(ch):
        def body(i):
            r = pl.ds(mult(i, 32), 32)
            done[r, part(ch)] = (
                acc[3, r, part(ch)].astype(F32)
                + got[0, r, part(ch)].astype(F32)
                + got[1, r, part(ch)].astype(F32)
            ).astype(BF16)

        times(HALF // 32, body)

    def give_back(ch):
        def spread(d, carry):
            pz, px = plane_peer(z, x, d)
            remote(
                done.at[pl.ds(pl.multiple_of((pz * NX + px) * CAP, CAP), CAP), part(ch)],
                back.at[own_rows, part(ch)],
                sb.at[ch],
                rb.at[ch],
                at(pz, px, c, y),
            ).start()
            return carry

        lax.fori_loop(1, CHIPS, spread, 0)
        back[own_rows, part(ch)] = done[own_rows, part(ch)]

    def all_back(ch):
        piece = (pl.ds(0, short), part(ch))
        return remote(done.at[piece], back.at[piece], sb.at[ch], rb.at[ch], at(z, x, c, up))

    def weight_grads(start, stop):
        def step(i, carry):
            cols = pl.ds(mult(i, 256), 256)
            wg[0, :, cols] = dot(gp_t[...], rin[:, cols], NN).astype(BF16)
            wg[1, :, cols] = dot(up_t[...], rin[:, cols], NN).astype(BF16)
            wg[2, :, cols] = dot(act_t[...], rcot[:, cols], NN).astype(BF16)
            return carry

        lax.fori_loop(start, stop, step, 0)

    product(0, other, po)
    to_mate(0).start()
    product(0, mine, pm)
    product(1, other, po)
    to_mate(1).start()
    fold(0)
    f_up(0).start()
    f_down(0).start()
    product(1, mine, pm)
    product(2, other, po)
    to_mate(2).start()
    fold(1)
    d_up(0).start()
    product(2, mine, pm)
    product(3, other, po)
    to_mate(3).start()
    fold(2)
    d_down(0).start()

    def turn(ch):
        f_up(ch).wait_recv()
        pass_on(1, 0, 0, ch)
        a_up(ch).start()
        f_down(ch).wait_recv()
        pass_on(2, part_rows, 1, ch)
        a_down(ch).start()

    def launch(ch):
        f_up(ch).start()
        f_down(ch).start()
        d_up(ch).start()
        d_down(ch).start()

    def complete(ch):
        d_up(ch).wait_recv()
        d_down(ch).wait_recv()
        a_up(ch).wait_recv()
        a_down(ch).wait_recv()
        finish(ch)
        give_back(ch)

    turn(0)
    launch(1)
    product(3, mine, pm)
    fold(3)
    weight_grads(0, 2)
    turn(1)
    launch(2)
    weight_grads(2, 3)
    complete(0)
    turn(2)
    weight_grads(3, 5)
    complete(1)
    weight_grads(5, 6)
    complete(2)

    first_rows, second_rows = pl.ds(0, TOK // 2), pl.ds(TOK // 2, TOK // 2)
    everything = pl.ds(0, TOK)

    def share(q, piece, slot, target, ch):
        ref = share_buf.at[q, piece, part(ch)]
        return remote(ref, ref, ss.at[slot, ch], rs.at[slot, ch], at(z, x, c, target))

    def place(ch):
        all_back(ch).wait_recv()
        share_buf[y, :, part(ch)] = dot(slots[...], back[:, part(ch)], TN).astype(BF16)
        share(y, everything, 0, up, ch).start()
        share(y, everything, 1, down, ch).start()

    def pass_shares(ch):
        share(down, everything, 0, up, ch).wait_recv()
        share(down, first_rows, 2, up, ch).start()
        share(up, everything, 1, down, ch).wait_recv()
        share(up, second_rows, 3, down, ch).start()

    def sent_dispatch():
        for k in range(RINGED):
            along(k, mine, HALF, y, 0, up).wait_send()
            along(k, mine, HALF, y, 1, down).wait_send()
            along(k, mine, part_rows, down, 2, up).wait_send()
            along(k, mine + part_rows, part_rows, up, 3, down).wait_send()
            for slot, q in enumerate((y, down, up, far)):
                relay(k, mine, q, slot).wait_send()
        whole(6).wait_send()
        for k in range(RINGED, len(CHUNKS)):
            relay(k, mine, 0, 0).wait_send()

    def sent_ring():
        for slot in range(NY):
            to_mate(slot).wait_send()
        for ch in range(len(PARTS)):
            for copy in (f_up, f_down, d_up, d_down, a_up, a_down, all_back):
                copy(ch).wait_send()
            share(y, everything, 0, up, ch).wait_send()
            share(y, everything, 1, down, ch).wait_send()
            share(down, first_rows, 2, up, ch).wait_send()
            share(up, second_rows, 3, down, ch).wait_send()

    def sent_carry():
        for d in range(1, NW):
            p, device = plane_mate(d)
            remote(msg.at[p], box_a.at[w], sa.at[d], ra.at[d], device).wait_send()
            remote(plane, box_b.at[z], sbb.at[d], rbb.at[d], line_peer(d)[1]).wait_send()
            send_res(d, z).wait_send()
        ring_res(y, every, 0, up).wait_send()
        ring_res(y, every, 1, down).wait_send()

    place(0)
    weight_grads(6, 8)
    outs = [
        pltpu.make_async_copy(wg.at[i], hbm, lw.at[4 + i])
        for i, hbm in enumerate((gg_hbm, ug_hbm, dg_hbm))
    ]
    for out in outs:
        out.start()

    def put(ref, hbm):
        copy = pltpu.make_async_copy(ref, hbm, lw.at[4 + len(outs)])
        copy.start()
        outs.append(copy)

    place(1)
    pass_shares(0)
    place(2)
    pass_shares(1)
    pass_shares(2)
    dotted = jnp.zeros((TOK, 1), F32)

    def dotted_with(q):
        cols = pl.ds(mult(q, QUARTER), QUARTER)
        gained = gain_ref[:, cols] * share_buf[q].astype(F32)
        return jnp.sum(tok_ref[:, cols].astype(F32) * gained, axis=1, keepdims=True)

    loads[3].wait()
    sent_dispatch()
    dotted += dotted_with(y) + dotted_with(down) + dotted_with(up)
    for ch in range(len(PARTS)):
        share(far, first_rows, 2, up, ch).wait_recv()
        share(far, second_rows, 3, down, ch).wait_recv()

    dotted += dotted_with(far)
    coef = inv * inv * inv * dotted / D
    mix = None
    for q in range(NY):
        cols = pl.ds(q * QUARTER, QUARTER)
        gained = gain_ref[:, cols] * share_buf[q].astype(F32)
        value = (
            cotan_ref[:, cols].astype(F32) + inv * gained - tok_ref[:, cols].astype(F32) * coef
        ).astype(BF16)
        res[:, cols] = value
        term = dot(value, ow[cols, :], NN)
        mix = term if mix is None else mix + term
    res_out[...] = res[:, own_cols]
    put(res_out, res_hbm)
    slice_rows = pl.ds(mult(y, SLICE), SLICE)

    def boxed(source):
        return res_box.at[y, pl.ds(mult(source, SLICE), SLICE), :]

    res_box[y, pl.ds(mult(z, SLICE), SLICE), :] = res[slice_rows, pl.ds(mult(z, CH), CH)]

    def send_res(d, source):
        p, device = line_peer(d)
        return remote(
            res.at[slice_rows, pl.ds(mult(p, CH), CH)], boxed(source), sr.at[d], rr.at[d], device
        )

    for d in range(1, NZ):
        send_res(d, z).start()
    read, write = reads[...], writes[...]
    for h in range(LOCAL_HEADS):
        lanes = slice(h * HD, (h + 1) * HD)
        sg = mix[:, lanes] * heads_silu[h]
        heads_sg[h] = sg
        growth = jnp.exp(cols_t[:, h : h + 1])
        carried = dot(growth * sg, read, TN, HIGHEST)
        for i in range(2):
            start = 2 * i * PIECE
            msg[2 * h + i, 0:PIECE, :] = jnp.concatenate(
                [carried[start : start + PIECE, :], carried[start + PIECE : start + 2 * PIECE, :]],
                axis=1,
            )
            msg[2 * h + i, PIECE : PIECE + 8, :] = jnp.broadcast_to(
                growth[TOK - 1 :, :], (8, PACK)
            )
    for d in range(1, NW):
        p, device = plane_mate(d)
        remote(msg.at[p], box_a.at[w], sa.at[d], ra.at[d], device).start()
    box_a[w] = msg[w]
    read_grads, write_grads = [], []

    def head_back(h):
        lanes = slice(h * HD, (h + 1) * HD)
        sg = heads_sg[h]
        gog_out[:, lanes] = (mix[:, lanes] * heads_gate[h]).astype(BF16)
        heads_in[h] = dot(scores[h], sg, TN, HIGHEST)
        pair_terms = dot(sg, heads_u[h], NT, HIGHEST) * pairs_w[h]
        read_grads.append(
            dot(pair_terms, write, NN, HIGHEST)
            + jnp.exp(cols_t[:, h : h + 1]) * dot(sg, state_ref[h], NN, HIGHEST)
        )
        write_grads.append(dot(pair_terms, read, TN, HIGHEST))

    head_back(0)
    head_back(1)

    def source_of(d):
        return lax.rem(w + NW - d, NW)

    for d in range(1, NW):
        p, device = plane_mate(d)
        remote(msg.at[p], box_a.at[source_of(d)], sa.at[d], ra.at[d], device).wait_recv()
    data, scale = pl.ds(0, PIECE), pl.ds(PIECE, 8)

    def pair(ref, i):
        s = ref[i, scale, :]
        return ref[i, data, :], jnp.concatenate([s] * (PIECE // 8), axis=0)

    total = jnp.zeros((PIECE, PACK), F32)
    decay = jnp.ones((PIECE, PACK), F32)
    inside, inside_decay = [], []
    for k in reversed(range(NW)):
        inside.append(total)
        inside_decay.append(decay)
        value, factor = pair(box_a, k)
        total = value + factor * total
        decay = factor * decay
    inside, inside_decay = inside[::-1], inside_decay[::-1]
    plane[data, :] = total
    plane[scale, :] = decay[0:8, :]
    box_b[z, data, :] = total
    box_b[z, scale, :] = decay[0:8, :]
    for d in range(1, NZ):
        remote(plane, box_b.at[z], sbb.at[d], rbb.at[d], line_peer(d)[1]).start()
    for d in range(1, NZ):
        send_res(d, lax.rem(z + NZ - d, NZ)).wait_recv()

    def ring_res(q, rows, slot, target):
        ref = res_box.at[q, rows, :]
        return remote(ref, ref, sq.at[slot], rq.at[slot], at(z, x, c, target))

    every, early, late = (
        pl.ds(0, NZ * SLICE),
        pl.ds(0, NZ * SLICE // 2),
        pl.ds(NZ * SLICE // 2, NZ * SLICE // 2),
    )
    ring_res(y, every, 0, up).start()
    ring_res(y, every, 1, down).start()
    head_back(2)
    for d in range(1, NZ):
        source = lax.rem(z + NZ - d, NZ)
        remote(plane, box_b.at[source], sbb.at[d], rbb.at[d], line_peer(d)[1]).wait_recv()
    beyond = jnp.zeros((PIECE, PACK), F32)
    for k in reversed(range(1, NZ)):
        value, factor = pair(box_b, k)
        beyond = jnp.where(k > z, value + factor * beyond, beyond)
    for k in range(NW):
        fan[k] = inside[k] + inside_decay[k] * beyond

    def slot_of(p):
        return later.at[p]

    for d in range(1, NW):
        p, device = plane_mate(d)
        remote(fan.at[p], slot_of(w), sc.at[d], rc.at[d], device).start()
    later[w] = fan[w]
    head_back(3)
    put(gog_out, gog_hbm)
    sent_ring()
    ring_res(down, every, 0, up).wait_recv()
    ring_res(down, early, 2, up).start()
    ring_res(up, every, 1, down).wait_recv()
    ring_res(up, late, 3, down).start()
    seven = gz.at[pl.ds(0, (NZ - 1) * TOK), :]
    remote(seven, seven, sgz, rgz, at(z, x, c, up)).wait()
    for d in range(1, NW):
        p, device = plane_mate(d)
        remote(fan.at[p], slot_of(source_of(d)), sc.at[d], rc.at[d], device).wait_recv()

    def head_end(h):
        lanes = slice(h * HD, (h + 1) * HD)
        column = cols_t[:, h : h + 1]
        shrink = jnp.exp(column[TOK - 1 :, :] - column)
        state = jnp.concatenate(
            [later[2 * h + i, :, j * HD : (j + 1) * HD] for i in range(2) for j in range(2)], axis=0
        )
        value = heads_in[h] + shrink * dot(write, state, NT, HIGHEST)
        scan_out[:, lanes] = (value * cols_t[:, LOCAL_HEADS + h : LOCAL_HEADS + h + 1]).astype(BF16)
        write_grads[h] += shrink * dot(heads_u[h], state, NN, HIGHEST)

    for h in range(LOCAL_HEADS):
        head_end(h)
    put(scan_out, scan_hbm)
    ring_res(far, early, 2, up).wait_recv()
    ring_res(far, late, 3, down).wait_recv()
    value = None
    for q in range(NY):
        rows = jnp.concatenate(
            [gz[k * TOK + q * SLICE : k * TOK + (q + 1) * SLICE, :] for k in range(NZ)], axis=0
        )
        term = dot(res_box[q], rows, TN)
        value = term if value is None else value + term
    prod[...] = value.reshape(prod.shape).astype(BF16)
    for d in range(1, NW):
        p, device = plane_mate(d)
        remote(prod.at[p], opg_box.at[w], so.at[d], ro.at[d], device).start()
    opg_box[w] = prod[w]
    write_out[...] = jnp.transpose(sum(write_grads[1:], write_grads[0])).astype(BF16)
    read_out[...] = jnp.transpose(sum(read_grads[1:], read_grads[0])).astype(BF16)
    put(write_out, write_hbm)
    put(read_out, read_hbm)
    sent_carry()
    for d in range(1, NW):
        p, device = plane_mate(d)
        remote(prod.at[p], opg_box.at[source_of(d)], so.at[d], ro.at[d], device).wait_recv()
    opg = opg_box[0].astype(F32)
    for k in range(1, NW):
        opg = opg + opg_box[k].astype(F32)
    opg_out[...] = opg
    put(opg_out, opg_hbm)

    for d in range(1, NW):
        p, device = plane_mate(d)
        remote(fan.at[p], slot_of(w), sc.at[d], rc.at[d], device).wait_send()
        remote(prod.at[p], opg_box.at[w], so.at[d], ro.at[d], device).wait_send()
    ring_res(down, early, 2, up).wait_send()
    ring_res(up, late, 3, down).wait_send()
    for out in outs:
        out.wait()


def layer(*operands):
    dma = pltpu.SemaphoreType.DMA
    hbm = pl.BlockSpec(memory_space=pl.ANY)
    smem = pl.BlockSpec(memory_space=pltpu.SMEM)
    n = len(CHUNKS)
    shape = jax.ShapeDtypeStruct
    wide = shape((HID, D), BF16)

    def held(*dims, dtype=BF16):
        return pltpu.VMEM(dims, dtype)

    head = held(LOCAL_HEADS, TOK, HD, dtype=F32)
    return pl.pallas_call(
        layer_kernel,
        out_shape=(
            wide,
            wide,
            wide,
            shape((TOK, QUARTER), BF16),
            shape((32, CH), F32),
            shape((TOK, CH), BF16),
            shape((TOK, CH), BF16),
            shape((HD, TOK), BF16),
            shape((HD, TOK), BF16),
        ),
        in_specs=[hbm] * 8 + [smem] + [hbm] * 7,
        out_specs=(hbm,) * 9,
        scratch_shapes=[
            held(HALF, QUARTER),
            held(HALF, RING + DIRECT),
            held(HALF, TOK),
            held(ROWS, D),
            held(ROWS, D),
            held(TOK, CH),
            held(NZ * TOK, CH),
            held(3, HID, D),
            held(D, CH),
            held(HID, ROWS, dtype=F32),
            held(HID, ROWS, dtype=F32),
            held(HID, ROWS, dtype=F32),
            held(HID, ROWS),
            held(HID, ROWS),
            held(HID, ROWS),
            held(ROWS, HID),
            held(ROWS, HID),
            held(3, HID, D),
            held(NY, HALF, QUARTER),
            held(NY, HALF, QUARTER, dtype=F32),
            held(NY, HALF, QUARTER),
            held(NY, HALF, QUARTER),
            held(2, HALF // 2, QUARTER),
            held(2, HALF, QUARTER),
            held(HALF, QUARTER),
            held(HALF, QUARTER),
            held(NY, TOK, QUARTER),
            held(TOK, D),
            held(NW, PIECE + 8, PACK, dtype=F32),
            held(NW, PIECE + 8, PACK, dtype=F32),
            held(PIECE + 8, PACK, dtype=F32),
            held(NZ, PIECE + 8, PACK, dtype=F32),
            held(NW, PIECE, PACK, dtype=F32),
            held(NW, PIECE, PACK, dtype=F32),
            held(NY, NZ * SLICE, CH),
            held(NW, 32, CH),
            held(NW, 32, CH),
            held(LOCAL_HEADS, TOK, TOK, dtype=F32),
            held(LOCAL_HEADS, TOK, TOK, dtype=F32),
            head,
            head,
            head,
            head,
            head,
            held(TOK, 2 * LOCAL_HEADS, dtype=F32),
            held(TOK, HD, dtype=F32),
            held(TOK, HD, dtype=F32),
            held(TOK, QUARTER),
            held(32, CH, dtype=F32),
            held(TOK, CH),
            held(TOK, CH),
            held(HD, TOK),
            held(HD, TOK),
            held(TOK, D),
            held(TOK, D),
            held(1, D, dtype=F32),
            held(2, TOK, dtype=jnp.int32),
            held(2, TOK, dtype=F32),
            held(TOK, CH),
            held(TOK, CH),
            held(LOCAL_HEADS, TOK, dtype=F32),
            held(HD, TOK),
            held(HD, TOK),
            held(LOCAL_HEADS, HD, HD, dtype=F32),
            held(TOK, QUARTER),
            held(TOK, RING),
            held(1, QUARTER, dtype=F32),
            dma((14,)),
            dma((13,)),
            dma((n,)),
            dma((n,)),
            dma((n, 4)),
            dma((n, 4)),
            dma((n, 4)),
            dma((n, 4)),
            dma,
            dma,
            dma((NY,)),
            dma((NY,)),
            dma((6, len(PARTS))),
            dma((6, len(PARTS))),
            dma((len(PARTS),)),
            dma((len(PARTS),)),
            dma((4, len(PARTS))),
            dma((4, len(PARTS))),
            dma((4,)),
            dma((4,)),
        ]
        + [dma((8,))] * 10,
        compiler_params=pltpu.CompilerParams(
            collective_id=0, has_side_effects=True, vmem_limit_bytes=62 * 1024 * 1024
        ),
        name="layer",
    )(*operands)


def hand_over_kernel(*refs):
    n = len(refs) // 3
    sources, targets = refs[:n], refs[n : 2 * n]
    held, (fetched, written) = refs[2 * n : 3 * n], refs[3 * n :]

    def pieces(i):
        rows = sources[i].shape[0]
        parts = 4 if i < 3 else 1
        step = rows // parts
        return [(k, pl.ds(k * step, step)) for k in range(parts)]

    def fetch(i, k, rows):
        return pltpu.make_async_copy(sources[i].at[rows], held[i].at[rows], fetched.at[i, k])

    def write(i, k, rows):
        return pltpu.make_async_copy(held[i].at[rows], targets[i].at[rows], written.at[i, k])

    every = [(i, k, rows) for i in range(n) for k, rows in pieces(i)]
    for piece in every:
        fetch(*piece).start()
    for piece in every:
        fetch(*piece).wait()
        write(*piece).start()
    for piece in every:
        write(*piece).wait()


def hand_over(arrays):
    hbm = pl.BlockSpec(memory_space=pl.ANY)
    n = len(arrays)
    return pl.pallas_call(
        hand_over_kernel,
        out_shape=tuple(jax.ShapeDtypeStruct(a.shape, a.dtype) for a in arrays),
        in_specs=[hbm] * n,
        out_specs=(hbm,) * n,
        scratch_shapes=[pltpu.VMEM(a.shape, a.dtype) for a in arrays]
        + [pltpu.SemaphoreType.DMA((n, 4))] * 2,
        compiler_params=pltpu.CompilerParams(vmem_limit_bytes=62 * 1024 * 1024),
        name="hand_over",
    )(*arrays)


def shards(
    tokens,
    norm_gain,
    cotangent,
    routes,
    route_weight,
    gate_weight,
    up_weight,
    down_weight,
    scan_input,
    out_gate,
    step_size,
    decay_rate,
    write_keys,
    read_keys,
    start_state,
    out_proj,
):
    (
        gate_grad,
        up_grad,
        down_grad,
        residual_part,
        out_proj_grad,
        scan_grad,
        gate_out_grad,
        write_grad,
        read_grad,
    ) = hand_over(
        layer(
        tokens,
        cotangent,
        norm_gain[None, :],
        jnp.transpose(routes),
        jnp.transpose(route_weight),
        out_gate,
        scan_input,
        step_size,
        decay_rate,
        jnp.transpose(write_keys),
        jnp.transpose(read_keys),
        start_state[0],
        jnp.transpose(gate_weight[0]),
        jnp.transpose(up_weight[0]),
        down_weight[0],
        out_proj,
        )
    )
    return (
        residual_part,
        jnp.transpose(gate_grad)[None],
        jnp.transpose(up_grad)[None],
        down_grad[None],
        out_proj_grad,
        scan_grad,
        gate_out_grad,
        jnp.transpose(write_grad),
        jnp.transpose(read_grad),
    )


def solution(mesh):
    finer = Mesh(mesh.devices.reshape(8, 4, 2, mesh.shape["tp"]), ("sp_0", "sp_1", "sp_2", "tp"))
    in_specs = (
        P(SP, None),
        P(),
        P(SP, None),
        P(SP, None),
        P(SP, None),
        P(SP, None, "tp"),
        P(SP, None, "tp"),
        P(SP, "tp", None),
        P(SP, "tp"),
        P(SP, "tp"),
        P("tp", SP),
        P("tp"),
        P(SP, "tp"),
        P(SP, "tp"),
        P(SP, "tp", None, None),
        P(None, "tp"),
    )
    out_specs = (
        P(SP, "tp"),
        P(SP, None, "tp"),
        P(SP, None, "tp"),
        P(SP, "tp", None),
        P(SP, "tp"),
        P(SP, "tp"),
        P(SP, "tp"),
        P(SP, "tp"),
        P(SP, "tp"),
    )
    return jax.shard_map(
        shards, mesh=finer, in_specs=in_specs, out_specs=out_specs, check_vma=False
    )
```

```python
import jax
import jax.numpy as jnp
from jax import lax
from jax.experimental import pallas as pl
from jax.experimental.pallas import tpu as pltpu
from jax.sharding import Mesh
from jax.sharding import PartitionSpec as P

D = 2048
HEADS = 16
STATE = 64
GROUPS = 4
SP = ("sp_0", "sp_1", "sp_2")


EPS = 1e-06
HIGHEST = lax.Precision.HIGHEST


MESH = pl.DeviceIdType.MESH
NZ, NX, NC, NY = 8, 4, 2, 4
NW = NX * NC
CHIPS = NZ * NX
CAP = 16
HALF = CHIPS * CAP
ROWS = 2 * HALF
QUARTER = 512
HID = 448
TOK = 128
CH = 256
HD = 64
LOCAL_HEADS = 4
BF16, F32 = jnp.bfloat16, jnp.float32
WIDE = QUARTER // 2
DIRECT = 512
RING = (D - DIRECT) // NY
CHUNKS = (
    (0, 0, 128, 0, QUARTER),
    (0, 128, 128, 128, QUARTER),
    (0, 256, 256, 256, QUARTER),
    (1, 0, 256, DIRECT, RING),
    (1, 256, 128, DIRECT + 256, RING),
    (1, RING, 256, 0, 0),
    (1, RING + 256, 256, 256, 0),
)
RINGED = 5
SLICE = TOK // NY
PARTS = tuple((128 * i, 128) for i in range(4))
PIECE = 16
PACK = 128
NT = (((1,), (1,)), ((), ()))
TN = (((0,), (0,)), ((), ()))
NN = (((1,), (0,)), ((), ()))


def position():
    return tuple(lax.axis_index(a) for a in ("sp_0", "sp_1", "sp_2", "tp"))


def at(z, x, c, y):
    return {"sp_0": z, "sp_1": x, "sp_2": c, "tp": y}


def remote(src, dst, send, recv, device):
    return pltpu.make_async_remote_copy(
        src_ref=src,
        dst_ref=dst,
        send_sem=send,
        recv_sem=recv,
        device_id=device,
        device_id_type=MESH,
    )


def signal(sem, device):
    pl.semaphore_signal(sem, inc=1, device_id=device, device_id_type=MESH)


def plane_peer(z, x, d):
    return lax.rem(z + d // NX, NZ), lax.rem(x + d % NX, NX)


def greet(barrier, z, x, c, y):

    def hello(d, carry):
        pz, px = plane_peer(z, x, d)
        signal(barrier, at(pz, px, c, y))
        return carry

    lax.fori_loop(1, CHIPS, hello, 0)
    for d in range(NX):
        signal(barrier, at(z, lax.rem(x + d, NX), 1 - c, y))
    signal(barrier, at(z, x, c, lax.rem(y + 1, NY)))
    signal(barrier, at(z, x, c, lax.rem(y + 3, NY)))


def times(n, body):
    def step(i, carry):
        body(i)
        return carry

    lax.fori_loop(0, n, step, 0)


def mult(i, n):
    return pl.multiple_of(i * n, n)


def dot(a, b, dims, precision=None):
    return lax.dot_general(a, b, dims, preferred_element_type=F32, precision=precision)


def layer_kernel(
    tok_hbm, cotan_hbm, gain_hbm, routes_hbm, route_weight_hbm, og_hbm, scan_in_hbm, step_hbm,
    rate_ref, keys_hbm, reads_hbm, state_hbm, gw_hbm, uw_hbm, dw_hbm, ow_hbm,
    gg_hbm, ug_hbm, dg_hbm, res_hbm, opg_hbm, scan_hbm, gog_hbm, write_hbm, read_hbm,
    sin, scot, slots, rin, rcot, gated, gz, wts, ow, accg, accu, acca, act_t, gp_t, up_t, gp, up_g,
    wg, po, pm, mate, acc, fwd, got, done, back, share_buf, res, msg, box_a, plane, box_b, fan,
    later, res_box, prod, opg_box, pairs_w, scores, heads_u, heads_silu, heads_gate, heads_sg,
    heads_in, cols_t, reads, writes, res_out, opg_out, scan_out, gog_out, write_out, read_out,
    tok_ref, cotan_ref, gain_ref, routes_ref, route_weight_ref, og_ref, scan_ref, step_ref,
    write_ref, read_ref, state_ref, tok_part, cotan_part, gain_part, credit, li, lw, s1, r1, sy, ry, sm, rm, sgz, rgz, spm, rpm, sf, rf, sb, rb, ss, rs, sq, rq, sa, ra, sbb, rbb,
    sc, rc, sr, rr, so, ro,
):
    z, x, c, y = position()
    chip = z * NX + x
    w = x * NC + c
    up, down, far = lax.rem(y + 1, NY), lax.rem(y + 3, NY), lax.rem(y + 2, NY)
    mine, other = c * HALF, (1 - c) * HALF
    part_rows = HALF // 2
    barrier = pltpu.get_barrier_semaphore()
    own_cols = pl.ds(mult(y, QUARTER), QUARTER)
    ring_cols = pl.ds(pl.multiple_of(DIRECT + y * RING, 128), RING)
    staged_inputs = [
        (routes_hbm, routes_ref),
        (route_weight_hbm, route_weight_ref),
        (gain_hbm, gain_ref),
        (tok_hbm, tok_ref),
        (cotan_hbm, cotan_ref),
        (tok_hbm.at[:, own_cols], tok_part),
        (cotan_hbm.at[:, ring_cols], cotan_part),
        (gain_hbm.at[:, own_cols], gain_part),
        (step_hbm, step_ref),
        (keys_hbm, write_ref),
        (reads_hbm, read_ref),
        (scan_in_hbm, scan_ref),
        (og_hbm, og_ref),
        (state_hbm, state_ref),
    ]
    inputs = [
        pltpu.make_async_copy(hbm, ref, li.at[i]) for i, (hbm, ref) in enumerate(staged_inputs)
    ]
    for copy in inputs:
        copy.start()
    early_inputs, late_inputs = inputs[:8], inputs[8:]
    greet(barrier, z, x, c, y)
    for copy in early_inputs:
        copy.wait()
    loads = [
        pltpu.make_async_copy(gw_hbm, wts.at[0], lw.at[0]),
        pltpu.make_async_copy(uw_hbm, wts.at[1], lw.at[1]),
        pltpu.make_async_copy(dw_hbm, wts.at[2], lw.at[2]),
        pltpu.make_async_copy(ow_hbm, ow, lw.at[3]),
    ]
    for load in loads:
        load.start()
    sources, targets = (sin, scot), (rin, rcot)
    own_rows = pl.ds(pl.multiple_of(chip * CAP, CAP), CAP)
    kept_rows = pl.ds(pl.multiple_of(mine + chip * CAP, CAP), CAP)

    squares = jnp.zeros((TOK, 1), F32)
    for q in range(NY):
        value = tok_ref[:, q * QUARTER : (q + 1) * QUARTER].astype(F32)
        squares += jnp.sum(value * value, axis=1, keepdims=True)
    inv = lax.rsqrt(squares / D + EPS)
    earlier = (
        lax.broadcasted_iota(jnp.int32, (TOK, TOK), 0) < lax.broadcasted_iota(jnp.int32, (TOK, TOK), 1)
    ).astype(BF16)
    expert = lax.broadcasted_iota(jnp.int32, (CHIPS, TOK), 0)
    names = [routes_ref[k : k + 1, :] for k in range(2)]
    members = [(expert == name).astype(F32) for name in names]
    counts = dot((members[0] + members[1]).astype(BF16), earlier, NN)
    slot = lax.broadcasted_iota(jnp.int32, (HALF, TOK), 0).astype(F32)
    hits = [
        slot == name.astype(F32) * CAP + jnp.sum(member * counts, axis=0, keepdims=True)
        for name, member in zip(names, members)
    ]
    slots[...] = jnp.logical_or(hits[0], hits[1]).astype(BF16)
    slot_weight = jnp.sum(
        jnp.where(hits[0], route_weight_ref[0:1, :], 0.0)
        + jnp.where(hits[1], route_weight_ref[1:2, :], 0.0),
        axis=1,
        keepdims=True,
    )
    normed = (tok_part[...].astype(F32) * inv * gain_part[...]).astype(BF16)
    sin[...] = dot(slots[...], normed, NN).astype(BF16)
    scot[:, 0:RING] = (slot_weight * dot(slots[...], cotan_part[...], NN)).astype(BF16)
    scot[:, RING:] = (slot_weight * dot(slots[...], cotan_ref[:, 0:DIRECT], NN)).astype(BF16)
    rin[kept_rows, own_cols] = sin[own_rows, :]
    rcot[kept_rows, ring_cols] = scot[own_rows, 0:RING]
    rcot[kept_rows, 0:DIRECT] = scot[own_rows, RING:]
    pl.semaphore_wait(barrier, CHIPS - 1 + NX + 2)

    def block(k, row, rows, q):
        array, _, width, base, stride = CHUNKS[k]
        return targets[array].at[
            pl.ds(pl.multiple_of(row, CAP), rows),
            pl.ds(pl.multiple_of(base + q * stride, 128), width),
        ]

    short = HALF - CAP

    def staged(k, rows):
        array, column, width, _, _ = CHUNKS[k]
        return sources[array].at[rows, pl.ds(column, width)]

    def issue(k):
        def spread(d, carry):
            pz, px = plane_peer(z, x, d)
            remote(
                staged(k, pl.ds(pl.multiple_of((pz * NX + px) * CAP, CAP), CAP)),
                block(k, mine + chip * CAP, CAP, y),
                s1.at[k],
                r1.at[k],
                at(pz, px, c, y),
            ).start()
            return carry

        lax.fori_loop(1, CHIPS, spread, 0)

    def whole(k):
        return remote(
            staged(k, pl.ds(0, short)), block(k, 0, short, y), s1.at[k], r1.at[k], at(z, x, c, up)
        )

    def relay(k, row, q):
        return remote(
            block(k, row, HALF, q), block(k, row, HALF, q), sm.at[k], rm.at[k], at(z, x, 1 - c, y)
        )

    def relayed(k):
        array, _, width, _, _ = CHUNKS[k]
        view = targets[array].at[pl.ds(0, ROWS if k < RINGED else HALF)]
        view = view.at[:, pl.ds(0, 2 * width if k < RINGED else width)]
        return remote(view, view, sm.at[k], rm.at[k], at(z, x, 1 - c, y))

    def along(k, row, rows, q, slot, target):
        return remote(
            block(k, row, rows, q), block(k, row, rows, q), sy.at[CHUNKS[k][0]], ry.at[k, slot],
            at(z, x, c, target),
        )

    def first(k):
        whole(k).wait_recv()
        along(k, mine, HALF, y, 0, up).start()
        along(k, mine, HALF, y, 1, down).start()
        relay(k, mine, y).start()

    def second(k):
        along(k, mine, HALF, down, 0, up).wait_recv()
        along(k, mine, part_rows, down, 2, up).start()
        relay(k, mine, down).start()
        along(k, mine, HALF, up, 1, down).wait_recv()
        along(k, mine + part_rows, part_rows, up, 3, down).start()
        relay(k, mine, up).start()

    def third(k):
        along(k, mine, part_rows, far, 2, up).wait_recv()
        along(k, mine + part_rows, part_rows, far, 3, down).wait_recv()
        relay(k, mine, far).start()

    def straight(k):
        whole(k).wait_recv()
        relay(k, mine, 0).start()

    def gather(k):
        relayed(k).wait_recv()

    def forward(array, columns, width, fresh):
        pairs = ((0, accg), (1, accu)) if array == 0 else ((2, acca),)
        rows_ref = targets[array]

        def body(n):
            nrows = pl.ds(mult(n, 256), 256)
            for index, total in pairs:
                value = None
                for group in columns:
                    left = [wts[index, :, column : column + width] for column in group]
                    right = [rows_ref[nrows, column : column + width] for column in group]
                    if len(group) > 1:
                        left = [jnp.concatenate(left, axis=1)]
                        right = [jnp.concatenate(right, axis=1)]
                    term = dot(left[0], right[0], NT)
                    value = term if value is None else value + term
                if fresh:
                    total[:, nrows] = value
                else:
                    total[:, nrows] += value

        times(ROWS // 256, body)

    def activate():
        def body(i):
            r = pl.ds(mult(i, 16), 16)
            g, u = accg[r, :], accu[r, :]
            s = jax.nn.sigmoid(g)
            silu = g * s
            act_t[r, :] = (silu * u).astype(BF16)
            accu[r, :] = u * s * (1.0 + g * (1.0 - s))
            accg[r, :] = silu

        times(HID // 16, body)

    def grads():
        def body(i):
            r = pl.ds(mult(i, 16), 16)
            a = acca[r, :]
            g = a * accu[r, :]
            u = a * accg[r, :]
            accu[r, :] = g
            accg[r, :] = u
            gp_t[r, :] = g.astype(BF16)
            up_t[r, :] = u.astype(BF16)

        times(HID // 16, body)

        def turn(j):
            cols = pl.ds(mult(j, 128), 128)
            gp[cols, :] = jnp.transpose(accu[:, cols]).astype(BF16)
            up_g[cols, :] = jnp.transpose(accg[:, cols]).astype(BF16)

        times(ROWS // 128, turn)

    def prepare():
        reads[...] = jnp.transpose(read_ref[...].astype(F32))
        writes[...] = jnp.transpose(write_ref[...].astype(F32))
        upto = (
            lax.broadcasted_iota(jnp.int32, (TOK, TOK), 0)
            <= lax.broadcasted_iota(jnp.int32, (TOK, TOK), 1)
        ).astype(F32)
        delta = jnp.concatenate(
            [-rate_ref[h] * step_ref[h : h + 1, :] for h in range(LOCAL_HEADS)], axis=0
        )
        logdec = dot(delta, upto, NN, HIGHEST)
        columns = jnp.transpose(jnp.concatenate([logdec, step_ref[...]], axis=0))
        cols_t[...] = columns
        causal = lax.broadcasted_iota(jnp.int32, (TOK, TOK), 0) >= lax.broadcasted_iota(
            jnp.int32, (TOK, TOK), 1
        )
        keys = dot(read_ref[...], write_ref[...], TN)
        for h in range(LOCAL_HEADS):
            spread = jnp.where(causal, columns[:, h : h + 1] - logdec[h : h + 1, :], -jnp.inf)
            weights = jnp.exp(spread)
            pairs_w[h] = weights
            scores[h] = keys * weights

    def scan_head(h):
        lanes = slice(h * HD, (h + 1) * HD)
        u = scan_ref[:, lanes].astype(F32) * cols_t[:, LOCAL_HEADS + h : LOCAL_HEADS + h + 1]
        heads_u[h] = u
        value = dot(scores[h], u, NN, HIGHEST)
        value += jnp.exp(cols_t[:, h : h + 1]) * dot(reads[...], state_ref[h], NT, HIGHEST)
        og = og_ref[:, lanes].astype(F32)
        sig = jax.nn.sigmoid(og)
        gated[:, lanes] = (value * og * sig).astype(BF16)
        heads_silu[h] = og * sig
        heads_gate[h] = value * sig * (1.0 + og * (1.0 - sig))

    def line_peer(d):
        p = lax.rem(z + d, NZ)
        return p, at(p, x, c, y)

    def plane_mate(d):
        p = lax.rem(w + d, NW)
        return p, at(z, p // NC, p % NC, y)

    own_tokens = pl.ds(mult(z, TOK), TOK)
    ring_in = [(q * QUARTER,) for q in range(NY)]
    next_in = [(q * QUARTER + 256,) for q in range(NY)]
    ring_cot = [(DIRECT + q * RING,) for q in range(NY)]
    last_cot = [tuple(DIRECT + q * RING + 256 for q in pair) for pair in ((0, 1), (2, 3))]
    issue(0)
    for copy in late_inputs:
        copy.wait()
    prepare()
    whole(0).wait_send()
    issue(1)
    scan_head(0)
    first(0)
    whole(1).wait_send()
    issue(2)
    scan_head(1)
    first(1)
    scan_head(2)
    second(0)
    whole(2).wait_send()
    issue(3)
    scan_head(3)
    gz[own_tokens, :] = gated[...]
    second(1)
    first(2)
    whole(3).wait_send()
    issue(4)
    third(0)
    third(1)
    first(3)
    signal(credit, at(z, x, 1 - c, y))
    whole(4).wait_send()
    pl.semaphore_wait(credit, 1)
    issue(5)
    loads[0].wait()
    loads[1].wait()
    second(2)
    first(4)
    signal(credit, at(z, x, 1 - c, y))
    gather(0)
    gather(1)
    forward(0, ring_in, 256, True)
    whole(5).wait_send()
    pl.semaphore_wait(credit, 1)
    issue(6)
    second(3)
    for d in range(1, NZ):
        remote(gated, gz.at[own_tokens, :], sgz, rgz, line_peer(d)[1]).start()
    straight(5)
    third(2)
    gather(2)
    forward(0, next_in, 256, False)
    second(4)
    activate()
    straight(6)
    third(3)
    loads[2].wait()
    gather(3)
    forward(1, ring_cot, 256, True)
    gather(5)
    gather(6)
    forward(1, [(0,)], DIRECT, False)
    third(4)
    gather(4)
    forward(1, last_cot, 128, False)
    grads()

    order = (far, up, down, y)

    def product(slot, row, target):
        cols = pl.ds(mult(order[slot], QUARTER), QUARTER)

        def body(i):
            r = pl.ds(pl.multiple_of(row + i * 256, 256), 256)
            value = dot(gp[r, :], wts[0, :, cols], NN) + dot(up_g[r, :], wts[1, :, cols], NN)
            target[slot, pl.ds(mult(i, 256), 256), :] = value.astype(target.dtype)

        times(HALF // 256, body)

    def to_mate(slot):
        return remote(po.at[slot], mate.at[slot], spm, rpm.at[slot], at(z, x, 1 - c, y))

    def fold(slot):
        to_mate(slot).wait_recv()

        def body(i):
            r = pl.ds(mult(i, 32), 32)
            acc[slot, r, :] = (pm[slot, r, :] + mate[slot, r, :].astype(F32)).astype(BF16)

        times(HALF // 32, body)

    lo, hi = pl.ds(0, part_rows), pl.ds(part_rows, part_rows)

    def part(ch):
        return pl.ds(*PARTS[ch])

    def ring(src, dst, slot, ch, target):
        return remote(src, dst, sf, rf.at[slot, ch], at(z, x, c, target))

    def f_up(ch):
        return ring(acc.at[0, lo, part(ch)], fwd.at[0, :, part(ch)], 0, ch, up)

    def f_down(ch):
        return ring(acc.at[0, hi, part(ch)], fwd.at[1, :, part(ch)], 1, ch, down)

    def d_up(ch):
        return ring(acc.at[1, hi, part(ch)], got.at[0, hi, part(ch)], 2, ch, up)

    def d_down(ch):
        return ring(acc.at[2, lo, part(ch)], got.at[1, lo, part(ch)], 3, ch, down)

    def a_up(ch):
        return ring(acc.at[1, lo, part(ch)], got.at[0, lo, part(ch)], 4, ch, up)

    def a_down(ch):
        return ring(acc.at[2, hi, part(ch)], got.at[1, hi, part(ch)], 5, ch, down)

    def pass_on(slot, start, index, ch):
        def body(i):
            r = pl.ds(pl.multiple_of(start + i * 32, 32), 32)
            f = pl.ds(mult(i, 32), 32)
            acc[slot, r, part(ch)] = (
                acc[slot, r, part(ch)].astype(F32) + fwd[index, f, part(ch)].astype(F32)
            ).astype(BF16)

        times(part_rows // 32, body)

    def finish(ch):
        def body(i):
            r = pl.ds(mult(i, 32), 32)
            done[r, part(ch)] = (
                acc[3, r, part(ch)].astype(F32)
                + got[0, r, part(ch)].astype(F32)
                + got[1, r, part(ch)].astype(F32)
            ).astype(BF16)

        times(HALF // 32, body)

    def give_back(ch):
        def spread(d, carry):
            pz, px = plane_peer(z, x, d)
            remote(
                done.at[pl.ds(pl.multiple_of((pz * NX + px) * CAP, CAP), CAP), part(ch)],
                back.at[own_rows, part(ch)],
                sb,
                rb.at[ch],
                at(pz, px, c, y),
            ).start()
            return carry

        lax.fori_loop(1, CHIPS, spread, 0)
        back[own_rows, part(ch)] = done[own_rows, part(ch)]

    def all_back(ch):
        piece = (pl.ds(0, short), part(ch))
        return remote(done.at[piece], back.at[piece], sb, rb.at[ch], at(z, x, c, up))

    def weight_grads(start, stop):
        def step(i, carry):
            cols = pl.ds(mult(i, 256), 256)
            wg[0, :, cols] = dot(gp_t[...], rin[:, cols], NN).astype(BF16)
            wg[1, :, cols] = dot(up_t[...], rin[:, cols], NN).astype(BF16)
            wg[2, :, cols] = dot(act_t[...], rcot[:, cols], NN).astype(BF16)
            return carry

        lax.fori_loop(start, stop, step, 0)

    product(0, other, po)
    to_mate(0).start()
    product(0, mine, pm)
    product(1, other, po)
    to_mate(1).start()
    fold(0)
    f_up(0).start()
    f_down(0).start()
    product(1, mine, pm)
    product(2, other, po)
    to_mate(2).start()
    fold(1)
    d_up(0).start()
    product(2, mine, pm)
    product(3, other, po)
    to_mate(3).start()
    fold(2)
    d_down(0).start()

    def turn(ch):
        f_up(ch).wait_recv()
        pass_on(1, 0, 0, ch)
        a_up(ch).start()
        f_down(ch).wait_recv()
        pass_on(2, part_rows, 1, ch)
        a_down(ch).start()

    def launch(ch):
        f_up(ch).start()
        f_down(ch).start()
        d_up(ch).start()
        d_down(ch).start()

    def complete(ch):
        d_up(ch).wait_recv()
        d_down(ch).wait_recv()
        a_up(ch).wait_recv()
        a_down(ch).wait_recv()
        finish(ch)
        give_back(ch)

    launch(1)
    turn(0)
    launch(2)
    product(3, mine, pm)
    fold(3)
    turn(1)
    launch(3)
    weight_grads(0, 1)
    complete(0)
    turn(2)
    weight_grads(1, 2)
    complete(1)
    turn(3)
    weight_grads(2, 4)
    complete(2)
    weight_grads(4, 5)
    complete(3)

    first_rows, second_rows = pl.ds(0, TOK // 2), pl.ds(TOK // 2, TOK // 2)
    everything = pl.ds(0, TOK)

    def share(q, piece, slot, target, ch):
        ref = share_buf.at[q, piece, part(ch)]
        return remote(ref, ref, ss, rs.at[slot, ch], at(z, x, c, target))

    def place(ch):
        all_back(ch).wait_recv()
        share_buf[y, :, part(ch)] = dot(slots[...], back[:, part(ch)], TN).astype(BF16)
        share(y, everything, 0, up, ch).start()
        share(y, everything, 1, down, ch).start()

    def pass_shares(ch):
        share(down, everything, 0, up, ch).wait_recv()
        share(down, first_rows, 2, up, ch).start()
        share(up, everything, 1, down, ch).wait_recv()
        share(up, second_rows, 3, down, ch).start()

    def sent(view, sem):
        remote(view, view, sem, sem, at(z, x, c, up)).wait_send()

    def sent_dispatch():
        sent(rin.at[pl.ds(0, HALF), pl.ds(0, 3 * QUARTER)], sy.at[0])
        sent(rcot.at[pl.ds(0, HALF), pl.ds(0, 3 * RING)], sy.at[1])
        whole(6).wait_send()
        for k in range(len(CHUNKS)):
            relayed(k).wait_send()

    def sent_ring():
        sent(po, spm)
        sent(acc.at[pl.ds(0, 3)], sf)
        sent(done.at[pl.ds(0, short)], sb)
        sent(share_buf.at[pl.ds(0, 3)], ss)

    def sent_carry():
        sent(msg.at[pl.ds(0, NW - 1)], sa)
        sent(box_b.at[pl.ds(0, NZ - 1)], sbb)
        sent(res_box.at[0, pl.ds(0, (NZ - 1) * SLICE)], sr)

    place(0)
    outs = []

    def put(ref, hbm):
        copy = pltpu.make_async_copy(ref, hbm, lw.at[7 + len(outs)])
        copy.start()
        outs.append(copy)

    place(1)
    pass_shares(0)
    place(2)
    pass_shares(1)
    place(3)
    pass_shares(2)
    pass_shares(3)
    dotted = jnp.zeros((TOK, 1), F32)

    def dotted_with(q):
        cols = pl.ds(mult(q, QUARTER), QUARTER)
        gained = gain_ref[:, cols] * share_buf[q].astype(F32)
        return jnp.sum(tok_ref[:, cols].astype(F32) * gained, axis=1, keepdims=True)

    loads[3].wait()
    sent_dispatch()
    dotted += dotted_with(y) + dotted_with(down) + dotted_with(up)
    for ch in range(len(PARTS)):
        share(far, first_rows, 2, up, ch).wait_recv()
        share(far, second_rows, 3, down, ch).wait_recv()

    dotted += dotted_with(far)
    coef = inv * inv * inv * dotted / D
    mix = None
    for q in range(NY):
        cols = pl.ds(q * QUARTER, QUARTER)
        gained = gain_ref[:, cols] * share_buf[q].astype(F32)
        value = (
            cotan_ref[:, cols].astype(F32) + inv * gained - tok_ref[:, cols].astype(F32) * coef
        ).astype(BF16)
        res[:, cols] = value
        term = dot(value, ow[cols, :], NN)
        mix = term if mix is None else mix + term
    res_out[...] = res[:, own_cols]
    put(res_out, res_hbm)
    slice_rows = pl.ds(mult(y, SLICE), SLICE)

    def boxed(source):
        return res_box.at[y, pl.ds(mult(source, SLICE), SLICE), :]

    res_box[y, pl.ds(mult(z, SLICE), SLICE), :] = res[slice_rows, pl.ds(mult(z, CH), CH)]

    def send_res(d, source):
        p, device = line_peer(d)
        return remote(
            res.at[slice_rows, pl.ds(mult(p, CH), CH)], boxed(source), sr, rr, device
        )

    for d in range(1, NZ):
        send_res(d, z).start()
    read, write = reads[...], writes[...]
    for h in range(LOCAL_HEADS):
        lanes = slice(h * HD, (h + 1) * HD)
        sg = mix[:, lanes] * heads_silu[h]
        heads_sg[h] = sg
        growth = jnp.exp(cols_t[:, h : h + 1])
        carried = dot(growth * sg, read, TN, HIGHEST)
        for i in range(2):
            start = 2 * i * PIECE
            msg[2 * h + i, 0:PIECE, :] = jnp.concatenate(
                [carried[start : start + PIECE, :], carried[start + PIECE : start + 2 * PIECE, :]],
                axis=1,
            )
            msg[2 * h + i, PIECE : PIECE + 8, :] = jnp.broadcast_to(
                growth[TOK - 1 :, :], (8, PACK)
            )
    for d in range(1, NW):
        p, device = plane_mate(d)
        remote(msg.at[p], box_a.at[w], sa, ra, device).start()
    box_a[w] = msg[w]
    read_grads, write_grads = [], []

    def head_back(h):
        lanes = slice(h * HD, (h + 1) * HD)
        sg = heads_sg[h]
        gog_out[:, lanes] = (mix[:, lanes] * heads_gate[h]).astype(BF16)
        heads_in[h] = dot(scores[h], sg, TN, HIGHEST)
        pair_terms = dot(sg, heads_u[h], NT, HIGHEST) * pairs_w[h]
        read_grads.append(
            dot(pair_terms, write, NN, HIGHEST)
            + jnp.exp(cols_t[:, h : h + 1]) * dot(sg, state_ref[h], NN, HIGHEST)
        )
        write_grads.append(dot(pair_terms, read, TN, HIGHEST))

    head_back(0)
    weight_grads(5, 6)
    head_back(1)

    seven_a = box_a.at[pl.ds(0, NW - 1)]
    remote(seven_a, seven_a, sa, ra, at(z, x, c, up)).wait_recv()
    data, scale = pl.ds(0, PIECE), pl.ds(PIECE, 8)

    def pair(ref, i):
        s = ref[i, scale, :]
        return ref[i, data, :], jnp.concatenate([s] * (PIECE // 8), axis=0)

    total = jnp.zeros((PIECE, PACK), F32)
    decay = jnp.ones((PIECE, PACK), F32)
    inside, inside_decay = [], []
    for k in reversed(range(NW)):
        inside.append(total)
        inside_decay.append(decay)
        value, factor = pair(box_a, k)
        total = value + factor * total
        decay = factor * decay
    inside, inside_decay = inside[::-1], inside_decay[::-1]
    plane[data, :] = total
    plane[scale, :] = decay[0:8, :]
    box_b[z, data, :] = total
    box_b[z, scale, :] = decay[0:8, :]
    for d in range(1, NZ):
        remote(plane, box_b.at[z], sbb, rbb, line_peer(d)[1]).start()
    seven_res = res_box.at[y, pl.ds(0, (NZ - 1) * SLICE)]
    remote(seven_res, seven_res, sr, rr, at(z, x, c, up)).wait_recv()

    def ring_res(q, rows, slot, target):
        ref = res_box.at[q, rows, :]
        return remote(ref, ref, sq, rq.at[slot], at(z, x, c, target))

    every, early, late = (
        pl.ds(0, NZ * SLICE),
        pl.ds(0, NZ * SLICE // 2),
        pl.ds(NZ * SLICE // 2, NZ * SLICE // 2),
    )
    ring_res(y, every, 0, up).start()
    ring_res(y, every, 1, down).start()
    head_back(2)
    weight_grads(6, 8)
    wide_outs = [
        pltpu.make_async_copy(wg.at[i], hbm, lw.at[4 + i])
        for i, hbm in enumerate((gg_hbm, ug_hbm, dg_hbm))
    ]
    for out in wide_outs:
        out.start()
    seven_b = box_b.at[pl.ds(0, NZ - 1)]
    remote(seven_b, seven_b, sbb, rbb, at(z, x, c, up)).wait_recv()
    beyond = jnp.zeros((PIECE, PACK), F32)
    for k in reversed(range(1, NZ)):
        value, factor = pair(box_b, k)
        beyond = jnp.where(k > z, value + factor * beyond, beyond)
    for k in range(NW):
        fan[k] = inside[k] + inside_decay[k] * beyond

    def slot_of(p):
        return later.at[p]

    for d in range(1, NW):
        p, device = plane_mate(d)
        remote(fan.at[p], slot_of(w), sc, rc, device).start()
    later[w] = fan[w]
    head_back(3)
    put(gog_out, gog_hbm)
    sent_ring()
    ring_res(down, every, 0, up).wait_recv()
    ring_res(down, early, 2, up).start()
    ring_res(up, every, 1, down).wait_recv()
    ring_res(up, late, 3, down).start()
    seven = gz.at[pl.ds(0, (NZ - 1) * TOK), :]
    remote(seven, seven, sgz, rgz, at(z, x, c, up)).wait()
    seven_c = later.at[pl.ds(0, NW - 1)]
    remote(seven_c, seven_c, sc, rc, at(z, x, c, up)).wait_recv()

    def head_end(h):
        lanes = slice(h * HD, (h + 1) * HD)
        column = cols_t[:, h : h + 1]
        shrink = jnp.exp(column[TOK - 1 :, :] - column)
        state = jnp.concatenate(
            [later[2 * h + i, :, j * HD : (j + 1) * HD] for i in range(2) for j in range(2)], axis=0
        )
        value = heads_in[h] + shrink * dot(write, state, NT, HIGHEST)
        scan_out[:, lanes] = (value * cols_t[:, LOCAL_HEADS + h : LOCAL_HEADS + h + 1]).astype(BF16)
        write_grads[h] += shrink * dot(heads_u[h], state, NN, HIGHEST)

    for h in range(LOCAL_HEADS):
        head_end(h)
    put(scan_out, scan_hbm)
    ring_res(far, early, 2, up).wait_recv()
    ring_res(far, late, 3, down).wait_recv()
    value = None
    for q in range(NY):
        rows = jnp.concatenate(
            [gz[k * TOK + q * SLICE : k * TOK + (q + 1) * SLICE, :] for k in range(NZ)], axis=0
        )
        term = dot(res_box[q], rows, TN)
        value = term if value is None else value + term
    prod[...] = value.reshape(prod.shape).astype(BF16)
    for d in range(1, NW):
        p, device = plane_mate(d)
        remote(prod.at[p], opg_box.at[w], so, ro, device).start()
    opg_box[w] = prod[w]
    write_out[...] = jnp.transpose(sum(write_grads[1:], write_grads[0])).astype(BF16)
    read_out[...] = jnp.transpose(sum(read_grads[1:], read_grads[0])).astype(BF16)
    put(write_out, write_hbm)
    put(read_out, read_hbm)
    sent_carry()
    seven_o = opg_box.at[pl.ds(0, NW - 1)]
    remote(seven_o, seven_o, so, ro, at(z, x, c, up)).wait_recv()
    opg = opg_box[0].astype(F32)
    for k in range(1, NW):
        opg = opg + opg_box[k].astype(F32)
    opg_out[...] = opg
    put(opg_out, opg_hbm)

    sent(fan.at[pl.ds(0, NW - 1)], sc)
    sent(prod.at[pl.ds(0, NW - 1)], so)
    sent(res_box.at[pl.ds(0, 3)], sq)
    for out in wide_outs + outs:
        out.wait()


def layer(*operands):
    dma = pltpu.SemaphoreType.DMA
    hbm = pl.BlockSpec(memory_space=pl.ANY)
    smem = pl.BlockSpec(memory_space=pltpu.SMEM)
    n = len(CHUNKS)
    shape = jax.ShapeDtypeStruct
    wide = shape((HID, D), BF16)

    def held(*dims, dtype=BF16):
        return pltpu.VMEM(dims, dtype)

    head = held(LOCAL_HEADS, TOK, HD, dtype=F32)
    return pl.pallas_call(
        layer_kernel,
        out_shape=(
            wide,
            wide,
            wide,
            shape((TOK, QUARTER), BF16),
            shape((32, CH), F32),
            shape((TOK, CH), BF16),
            shape((TOK, CH), BF16),
            shape((HD, TOK), BF16),
            shape((HD, TOK), BF16),
        ),
        in_specs=[hbm] * 8 + [smem] + [hbm] * 7,
        out_specs=(hbm,) * 9,
        scratch_shapes=[
            held(HALF, QUARTER),
            held(HALF, RING + DIRECT),
            held(HALF, TOK),
            held(ROWS, D),
            held(ROWS, D),
            held(TOK, CH),
            held(NZ * TOK, CH),
            held(3, HID, D),
            held(D, CH),
            held(HID, ROWS, dtype=F32),
            held(HID, ROWS, dtype=F32),
            held(HID, ROWS, dtype=F32),
            held(HID, ROWS),
            held(HID, ROWS),
            held(HID, ROWS),
            held(ROWS, HID),
            held(ROWS, HID),
            held(3, HID, D),
            held(NY, HALF, QUARTER),
            held(NY, HALF, QUARTER, dtype=F32),
            held(NY, HALF, QUARTER),
            held(NY, HALF, QUARTER),
            held(2, HALF // 2, QUARTER),
            held(2, HALF, QUARTER),
            held(HALF, QUARTER),
            held(HALF, QUARTER),
            held(NY, TOK, QUARTER),
            held(TOK, D),
            held(NW, PIECE + 8, PACK, dtype=F32),
            held(NW, PIECE + 8, PACK, dtype=F32),
            held(PIECE + 8, PACK, dtype=F32),
            held(NZ, PIECE + 8, PACK, dtype=F32),
            held(NW, PIECE, PACK, dtype=F32),
            held(NW, PIECE, PACK, dtype=F32),
            held(NY, NZ * SLICE, CH),
            held(NW, 32, CH),
            held(NW, 32, CH),
            held(LOCAL_HEADS, TOK, TOK, dtype=F32),
            held(LOCAL_HEADS, TOK, TOK, dtype=F32),
            head,
            head,
            head,
            head,
            head,
            held(TOK, 2 * LOCAL_HEADS, dtype=F32),
            held(TOK, HD, dtype=F32),
            held(TOK, HD, dtype=F32),
            held(TOK, QUARTER),
            held(32, CH, dtype=F32),
            held(TOK, CH),
            held(TOK, CH),
            held(HD, TOK),
            held(HD, TOK),
            held(TOK, D),
            held(TOK, D),
            held(1, D, dtype=F32),
            held(2, TOK, dtype=jnp.int32),
            held(2, TOK, dtype=F32),
            held(TOK, CH),
            held(TOK, CH),
            held(LOCAL_HEADS, TOK, dtype=F32),
            held(HD, TOK),
            held(HD, TOK),
            held(LOCAL_HEADS, HD, HD, dtype=F32),
            held(TOK, QUARTER),
            held(TOK, RING),
            held(1, QUARTER, dtype=F32),
            pltpu.SemaphoreType.REGULAR,
            dma((14,)),
            dma((13,)),
            dma((n,)),
            dma((n,)),
            dma((2,)),
            dma((RINGED, 4)),
            dma((n,)),
            dma((n,)),
            dma,
            dma,
            dma,
            dma((NY,)),
            dma,
            dma((6, len(PARTS))),
            dma,
            dma((len(PARTS),)),
            dma,
            dma((4, len(PARTS))),
            dma,
            dma((4,)),
        ]
        + [dma] * 10,
        compiler_params=pltpu.CompilerParams(
            collective_id=0, has_side_effects=True, vmem_limit_bytes=62 * 1024 * 1024
        ),
        name="layer",
    )(*operands)


def hand_over_kernel(*refs):
    n = len(refs) // 3
    sources, targets = refs[:n], refs[n : 2 * n]
    held, (fetched, written) = refs[2 * n : 3 * n], refs[3 * n :]

    def pieces(i):
        rows = sources[i].shape[0]
        parts = 4 if i < 3 else 1
        step = rows // parts
        return [(k, pl.ds(k * step, step)) for k in range(parts)]

    def fetch(i, k, rows):
        return pltpu.make_async_copy(sources[i].at[rows], held[i].at[rows], fetched.at[i, k])

    def write(i, k, rows):
        return pltpu.make_async_copy(held[i].at[rows], targets[i].at[rows], written.at[i, k])

    every = [(i, k, rows) for i in range(n) for k, rows in pieces(i)]
    for piece in every:
        fetch(*piece).start()
    for piece in every:
        fetch(*piece).wait()
        write(*piece).start()
    for piece in every:
        write(*piece).wait()


def hand_over(arrays):
    hbm = pl.BlockSpec(memory_space=pl.ANY)
    n = len(arrays)
    return pl.pallas_call(
        hand_over_kernel,
        out_shape=tuple(jax.ShapeDtypeStruct(a.shape, a.dtype) for a in arrays),
        in_specs=[hbm] * n,
        out_specs=(hbm,) * n,
        scratch_shapes=[pltpu.VMEM(a.shape, a.dtype) for a in arrays]
        + [pltpu.SemaphoreType.DMA((n, 4))] * 2,
        compiler_params=pltpu.CompilerParams(vmem_limit_bytes=62 * 1024 * 1024),
        name="hand_over",
    )(*arrays)


def shards(
    tokens,
    norm_gain,
    cotangent,
    routes,
    route_weight,
    gate_weight,
    up_weight,
    down_weight,
    scan_input,
    out_gate,
    step_size,
    decay_rate,
    write_keys,
    read_keys,
    start_state,
    out_proj,
):
    (
        gate_grad,
        up_grad,
        down_grad,
        residual_part,
        out_proj_grad,
        scan_grad,
        gate_out_grad,
        write_grad,
        read_grad,
    ) = hand_over(
        layer(
        tokens,
        cotangent,
        norm_gain[None, :],
        jnp.transpose(routes),
        jnp.transpose(route_weight),
        out_gate,
        scan_input,
        step_size,
        decay_rate,
        jnp.transpose(write_keys),
        jnp.transpose(read_keys),
        start_state[0],
        jnp.transpose(gate_weight[0]),
        jnp.transpose(up_weight[0]),
        down_weight[0],
        out_proj,
        )
    )
    return (
        residual_part,
        jnp.transpose(gate_grad)[None],
        jnp.transpose(up_grad)[None],
        down_grad[None],
        out_proj_grad,
        scan_grad,
        gate_out_grad,
        jnp.transpose(write_grad),
        jnp.transpose(read_grad),
    )


def solution(mesh):
    finer = Mesh(mesh.devices.reshape(8, 4, 2, mesh.shape["tp"]), ("sp_0", "sp_1", "sp_2", "tp"))
    in_specs = (
        P(SP, None),
        P(),
        P(SP, None),
        P(SP, None),
        P(SP, None),
        P(SP, None, "tp"),
        P(SP, None, "tp"),
        P(SP, "tp", None),
        P(SP, "tp"),
        P(SP, "tp"),
        P("tp", SP),
        P("tp"),
        P(SP, "tp"),
        P(SP, "tp"),
        P(SP, "tp", None, None),
        P(None, "tp"),
    )
    out_specs = (
        P(SP, "tp"),
        P(SP, None, "tp"),
        P(SP, None, "tp"),
        P(SP, "tp", None),
        P(SP, "tp"),
        P(SP, "tp"),
        P(SP, "tp"),
        P(SP, "tp"),
        P(SP, "tp"),
    )
    return jax.shard_map(
        shards, mesh=finer, in_specs=in_specs, out_specs=out_specs, check_vma=False
    )
```

```python
import jax
import jax.numpy as jnp
from jax import lax
from jax.experimental import pallas as pl
from jax.experimental.pallas import tpu as pltpu
from jax.sharding import Mesh
from jax.sharding import PartitionSpec as P

D = 2048
HEADS = 16
STATE = 64
GROUPS = 4
SP = ("sp_0", "sp_1", "sp_2")


EPS = 1e-06
HIGHEST = lax.Precision.HIGHEST


MESH = pl.DeviceIdType.MESH
NZ, NX, NC, NY = 8, 4, 2, 4
NW = NX * NC
CHIPS = NZ * NX
CAP = 16
HALF = CHIPS * CAP
ROWS = 2 * HALF
QUARTER = 512
HID = 448
TOK = 128
CH = 256
HD = 64
LOCAL_HEADS = 4
BF16, F32 = jnp.bfloat16, jnp.float32
WIDE = QUARTER // 2
DIRECT = 512
RING = (D - DIRECT) // NY
CHUNKS = (
    (0, 0, 128, 0, QUARTER),
    (0, 128, 128, 128, QUARTER),
    (0, 256, 256, 256, QUARTER),
    (1, 0, 256, DIRECT, RING),
    (1, 256, 128, DIRECT + 256, RING),
    (1, RING, 256, 0, 0),
    (1, RING + 256, 256, 256, 0),
)
RINGED = 5
SLICE = TOK // NY
PARTS = tuple((128 * i, 128) for i in range(4))
PIECE = 16
PACK = 128
NT = (((1,), (1,)), ((), ()))
TN = (((0,), (0,)), ((), ()))
NN = (((1,), (0,)), ((), ()))


def position():
    return tuple(lax.axis_index(a) for a in ("sp_0", "sp_1", "sp_2", "tp"))


def at(z, x, c, y):
    return {"sp_0": z, "sp_1": x, "sp_2": c, "tp": y}


def remote(src, dst, send, recv, device):
    return pltpu.make_async_remote_copy(
        src_ref=src,
        dst_ref=dst,
        send_sem=send,
        recv_sem=recv,
        device_id=device,
        device_id_type=MESH,
    )


def signal(sem, device):
    pl.semaphore_signal(sem, inc=1, device_id=device, device_id_type=MESH)


def plane_peer(z, x, d):
    return lax.rem(z + d // NX, NZ), lax.rem(x + d % NX, NX)


def greet(barrier, z, x, c, y):

    def hello(d, carry):
        pz, px = plane_peer(z, x, d)
        signal(barrier, at(pz, px, c, y))
        return carry

    lax.fori_loop(1, CHIPS, hello, 0)
    for d in range(NX):
        signal(barrier, at(z, lax.rem(x + d, NX), 1 - c, y))
    signal(barrier, at(z, x, c, lax.rem(y + 1, NY)))
    signal(barrier, at(z, x, c, lax.rem(y + 2, NY)))
    signal(barrier, at(z, x, c, lax.rem(y + 3, NY)))


def times(n, body):
    def step(i, carry):
        body(i)
        return carry

    lax.fori_loop(0, n, step, 0)


def mult(i, n):
    return pl.multiple_of(i * n, n)


def dot(a, b, dims, precision=None):
    return lax.dot_general(a, b, dims, preferred_element_type=F32, precision=precision)


def layer_kernel(
    tok_hbm, cotan_hbm, gain_hbm, routes_hbm, route_weight_hbm, og_hbm, scan_in_hbm, step_hbm,
    rate_ref, keys_hbm, reads_hbm, state_hbm, gw_hbm, uw_hbm, dw_hbm, ow_hbm,
    gg_hbm, ug_hbm, dg_hbm, res_hbm, opg_hbm, scan_hbm, gog_hbm, write_hbm, read_hbm,
    sin, scot, slots, rin, rcot, gated, gz, wts, ow, accg, accu, acca, act_t, gp_t, up_t, gp, up_g,
    wg, po, pm, mate, acc, fwd, got, done, back, share_buf, res, msg, box_a, plane, box_b, fan,
    later, res_box, prod, opg_box, pairs_w, scores, heads_u, heads_silu, heads_gate, heads_sg,
    heads_in, cols_t, reads, writes, res_out, opg_out, scan_out, gog_out, write_out, read_out,
    tok_ref, cotan_ref, gain_ref, routes_ref, route_weight_ref, og_ref, scan_ref, step_ref,
    write_ref, read_ref, state_ref, tok_part, cotan_part, gain_part, credit, li, lw, s1, r1, sy, ry, sm, rm, sgz, rgz, spm, rpm, sf, rf, sb, rb, ss, rs, sq, rq, sa, ra, sbb, rbb,
    sc, rc, sr, rr, so, ro,
):
    z, x, c, y = position()
    chip = z * NX + x
    w = x * NC + c
    up, down, far = lax.rem(y + 1, NY), lax.rem(y + 3, NY), lax.rem(y + 2, NY)
    mine, other = c * HALF, (1 - c) * HALF
    part_rows = HALF // 2
    barrier = pltpu.get_barrier_semaphore()
    own_cols = pl.ds(mult(y, QUARTER), QUARTER)
    ring_cols = pl.ds(pl.multiple_of(DIRECT + y * RING, 128), RING)
    staged_inputs = [
        (routes_hbm, routes_ref),
        (route_weight_hbm, route_weight_ref),
        (gain_hbm, gain_ref),
        (tok_hbm, tok_ref),
        (cotan_hbm, cotan_ref),
        (tok_hbm.at[:, own_cols], tok_part),
        (cotan_hbm.at[:, ring_cols], cotan_part),
        (gain_hbm.at[:, own_cols], gain_part),
        (step_hbm, step_ref),
        (keys_hbm, write_ref),
        (reads_hbm, read_ref),
        (scan_in_hbm, scan_ref),
        (og_hbm, og_ref),
        (state_hbm, state_ref),
    ]
    inputs = [
        pltpu.make_async_copy(hbm, ref, li.at[i]) for i, (hbm, ref) in enumerate(staged_inputs)
    ]
    for copy in inputs:
        copy.start()
    early_inputs, late_inputs = inputs[:8], inputs[8:]
    greet(barrier, z, x, c, y)
    for copy in early_inputs:
        copy.wait()
    loads = [
        pltpu.make_async_copy(gw_hbm, wts.at[0], lw.at[0]),
        pltpu.make_async_copy(uw_hbm, wts.at[1], lw.at[1]),
        pltpu.make_async_copy(dw_hbm, wts.at[2], lw.at[2]),
        pltpu.make_async_copy(ow_hbm, ow, lw.at[3]),
    ]
    for load in loads:
        load.start()
    sources, targets = (sin, scot), (rin, rcot)
    own_rows = pl.ds(pl.multiple_of(chip * CAP, CAP), CAP)
    kept_rows = pl.ds(pl.multiple_of(mine + chip * CAP, CAP), CAP)

    squares = jnp.zeros((TOK, 1), F32)
    for q in range(NY):
        value = tok_ref[:, q * QUARTER : (q + 1) * QUARTER].astype(F32)
        squares += jnp.sum(value * value, axis=1, keepdims=True)
    inv = lax.rsqrt(squares / D + EPS)
    earlier = (
        lax.broadcasted_iota(jnp.int32, (TOK, TOK), 0) < lax.broadcasted_iota(jnp.int32, (TOK, TOK), 1)
    ).astype(BF16)
    expert = lax.broadcasted_iota(jnp.int32, (CHIPS, TOK), 0)
    names = [routes_ref[k : k + 1, :] for k in range(2)]
    members = [(expert == name).astype(F32) for name in names]
    counts = dot((members[0] + members[1]).astype(BF16), earlier, NN)
    slot = lax.broadcasted_iota(jnp.int32, (HALF, TOK), 0).astype(F32)
    hits = [
        slot == name.astype(F32) * CAP + jnp.sum(member * counts, axis=0, keepdims=True)
        for name, member in zip(names, members)
    ]
    slots[...] = jnp.logical_or(hits[0], hits[1]).astype(BF16)
    slot_weight = jnp.sum(
        jnp.where(hits[0], route_weight_ref[0:1, :], 0.0)
        + jnp.where(hits[1], route_weight_ref[1:2, :], 0.0),
        axis=1,
        keepdims=True,
    )
    normed = (tok_part[...].astype(F32) * inv * gain_part[...]).astype(BF16)
    sin[...] = dot(slots[...], normed, NN).astype(BF16)
    scot[:, 0:RING] = (slot_weight * dot(slots[...], cotan_part[...], NN)).astype(BF16)
    scot[:, RING:] = (slot_weight * dot(slots[...], cotan_ref[:, 0:DIRECT], NN)).astype(BF16)
    rin[kept_rows, own_cols] = sin[own_rows, :]
    rcot[kept_rows, ring_cols] = scot[own_rows, 0:RING]
    rcot[kept_rows, 0:DIRECT] = scot[own_rows, RING:]
    pl.semaphore_wait(barrier, CHIPS - 1 + NX + 3)

    def block(k, row, rows, q):
        array, _, width, base, stride = CHUNKS[k]
        return targets[array].at[
            pl.ds(pl.multiple_of(row, CAP), rows),
            pl.ds(pl.multiple_of(base + q * stride, 128), width),
        ]

    short = HALF - CAP

    def staged(k, rows):
        array, column, width, _, _ = CHUNKS[k]
        return sources[array].at[rows, pl.ds(column, width)]

    def issue(k):
        def spread(d, carry):
            pz, px = plane_peer(z, x, d)
            remote(
                staged(k, pl.ds(pl.multiple_of((pz * NX + px) * CAP, CAP), CAP)),
                block(k, mine + chip * CAP, CAP, y),
                s1.at[k],
                r1.at[k],
                at(pz, px, c, y),
            ).start()
            return carry

        lax.fori_loop(1, CHIPS, spread, 0)

    def whole(k):
        return remote(
            staged(k, pl.ds(0, short)), block(k, 0, short, y), s1.at[k], r1.at[k], at(z, x, c, up)
        )

    def relay(k, row, q):
        return remote(
            block(k, row, HALF, q), block(k, row, HALF, q), sm.at[k], rm.at[k], at(z, x, 1 - c, y)
        )

    def relayed(k):
        array, _, width, _, _ = CHUNKS[k]
        view = targets[array].at[pl.ds(0, ROWS if k < RINGED else HALF)]
        view = view.at[:, pl.ds(0, 2 * width if k < RINGED else width)]
        return remote(view, view, sm.at[k], rm.at[k], at(z, x, 1 - c, y))

    def along(k, row, rows, q, slot, target):
        return remote(
            block(k, row, rows, q), block(k, row, rows, q), sy.at[CHUNKS[k][0]], ry.at[k, slot],
            at(z, x, c, target),
        )

    def first(k):
        whole(k).wait_recv()
        along(k, mine, HALF, y, 0, up).start()
        along(k, mine, HALF, y, 1, down).start()
        relay(k, mine, y).start()

    def second(k):
        along(k, mine, HALF, down, 0, up).wait_recv()
        along(k, mine, part_rows, down, 2, up).start()
        relay(k, mine, down).start()
        along(k, mine, HALF, up, 1, down).wait_recv()
        along(k, mine + part_rows, part_rows, up, 3, down).start()
        relay(k, mine, up).start()

    def third(k):
        along(k, mine, part_rows, far, 2, up).wait_recv()
        along(k, mine + part_rows, part_rows, far, 3, down).wait_recv()
        relay(k, mine, far).start()

    def straight(k):
        whole(k).wait_recv()
        relay(k, mine, 0).start()

    def gather(k):
        relayed(k).wait_recv()

    def forward(array, columns, width, fresh):
        pairs = ((0, accg), (1, accu)) if array == 0 else ((2, acca),)
        rows_ref = targets[array]

        def body(n):
            nrows = pl.ds(mult(n, 256), 256)
            for index, total in pairs:
                value = None
                for group in columns:
                    left = [wts[index, :, column : column + width] for column in group]
                    right = [rows_ref[nrows, column : column + width] for column in group]
                    if len(group) > 1:
                        left = [jnp.concatenate(left, axis=1)]
                        right = [jnp.concatenate(right, axis=1)]
                    term = dot(left[0], right[0], NT)
                    value = term if value is None else value + term
                if fresh:
                    total[:, nrows] = value
                else:
                    total[:, nrows] += value

        times(ROWS // 256, body)

    def activate():
        def body(i):
            r = pl.ds(mult(i, 16), 16)
            g, u = accg[r, :], accu[r, :]
            s = jax.nn.sigmoid(g)
            silu = g * s
            act_t[r, :] = (silu * u).astype(BF16)
            accu[r, :] = u * s * (1.0 + g * (1.0 - s))
            accg[r, :] = silu

        times(HID // 16, body)

    def grads():
        def body(i):
            r = pl.ds(mult(i, 16), 16)
            a = acca[r, :]
            g = a * accu[r, :]
            u = a * accg[r, :]
            accu[r, :] = g
            accg[r, :] = u
            gp_t[r, :] = g.astype(BF16)
            up_t[r, :] = u.astype(BF16)

        times(HID // 16, body)

        def turn(j):
            cols = pl.ds(mult(j, 128), 128)
            gp[cols, :] = jnp.transpose(accu[:, cols]).astype(BF16)
            up_g[cols, :] = jnp.transpose(accg[:, cols]).astype(BF16)

        times(ROWS // 128, turn)

    def prepare():
        reads[...] = jnp.transpose(read_ref[...].astype(F32))
        writes[...] = jnp.transpose(write_ref[...].astype(F32))
        upto = (
            lax.broadcasted_iota(jnp.int32, (TOK, TOK), 0)
            <= lax.broadcasted_iota(jnp.int32, (TOK, TOK), 1)
        ).astype(F32)
        delta = jnp.concatenate(
            [-rate_ref[h] * step_ref[h : h + 1, :] for h in range(LOCAL_HEADS)], axis=0
        )
        logdec = dot(delta, upto, NN, HIGHEST)
        columns = jnp.transpose(jnp.concatenate([logdec, step_ref[...]], axis=0))
        cols_t[...] = columns
        causal = lax.broadcasted_iota(jnp.int32, (TOK, TOK), 0) >= lax.broadcasted_iota(
            jnp.int32, (TOK, TOK), 1
        )
        keys = dot(read_ref[...], write_ref[...], TN)
        for h in range(LOCAL_HEADS):
            spread = jnp.where(causal, columns[:, h : h + 1] - logdec[h : h + 1, :], -jnp.inf)
            weights = jnp.exp(spread)
            pairs_w[h] = weights
            scores[h] = keys * weights

    def scan_head(h):
        lanes = slice(h * HD, (h + 1) * HD)
        u = scan_ref[:, lanes].astype(F32) * cols_t[:, LOCAL_HEADS + h : LOCAL_HEADS + h + 1]
        heads_u[h] = u
        value = dot(scores[h], u, NN, HIGHEST)
        value += jnp.exp(cols_t[:, h : h + 1]) * dot(reads[...], state_ref[h], NT, HIGHEST)
        og = og_ref[:, lanes].astype(F32)
        sig = jax.nn.sigmoid(og)
        gated[:, lanes] = (value * og * sig).astype(BF16)
        heads_silu[h] = og * sig
        heads_gate[h] = value * sig * (1.0 + og * (1.0 - sig))

    def line_peer(d):
        p = lax.rem(z + d, NZ)
        return p, at(p, x, c, y)

    def plane_mate(d):
        p = lax.rem(w + d, NW)
        return p, at(z, p // NC, p % NC, y)

    own_tokens = pl.ds(mult(z, TOK), TOK)
    ring_in = [(q * QUARTER,) for q in range(NY)]
    next_in = [(q * QUARTER + 256,) for q in range(NY)]
    ring_cot = [(DIRECT + q * RING,) for q in range(NY)]
    last_cot = [tuple(DIRECT + q * RING + 256 for q in pair) for pair in ((0, 1), (2, 3))]
    issue(0)
    for copy in late_inputs:
        copy.wait()
    prepare()
    whole(0).wait_send()
    issue(1)
    scan_head(0)
    first(0)
    whole(1).wait_send()
    issue(2)
    scan_head(1)
    first(1)
    scan_head(2)
    second(0)
    whole(2).wait_send()
    issue(3)
    scan_head(3)
    gz[own_tokens, :] = gated[...]
    second(1)
    first(2)
    whole(3).wait_send()
    issue(4)
    third(0)
    third(1)
    first(3)
    signal(credit, at(z, x, 1 - c, y))
    whole(4).wait_send()
    pl.semaphore_wait(credit, 1)
    issue(5)
    loads[0].wait()
    loads[1].wait()
    second(2)
    first(4)
    signal(credit, at(z, x, 1 - c, y))
    gather(0)
    gather(1)
    forward(0, ring_in, 256, True)
    whole(5).wait_send()
    pl.semaphore_wait(credit, 1)
    issue(6)
    second(3)
    for d in range(1, NZ):
        remote(gated, gz.at[own_tokens, :], sgz, rgz, line_peer(d)[1]).start()
    straight(5)
    third(2)
    gather(2)
    forward(0, next_in, 256, False)
    second(4)
    activate()
    straight(6)
    third(3)
    loads[2].wait()
    gather(3)
    forward(1, ring_cot, 256, True)
    gather(5)
    gather(6)
    forward(1, [(0,)], DIRECT, False)
    third(4)
    gather(4)
    forward(1, last_cot, 128, False)
    grads()

    order = (far, up, down, y)

    def product(slot, row, target):
        cols = pl.ds(mult(order[slot], QUARTER), QUARTER)

        def body(i):
            r = pl.ds(pl.multiple_of(row + i * 256, 256), 256)
            value = dot(gp[r, :], wts[0, :, cols], NN) + dot(up_g[r, :], wts[1, :, cols], NN)
            target[slot, pl.ds(mult(i, 256), 256), :] = value.astype(target.dtype)

        times(HALF // 256, body)

    def to_mate(slot):
        return remote(po.at[slot], mate.at[slot], spm, rpm.at[slot], at(z, x, 1 - c, y))

    def fold(slot):
        to_mate(slot).wait_recv()

        def body(i):
            r = pl.ds(mult(i, 32), 32)
            acc[slot, r, :] = (pm[slot, r, :] + mate[slot, r, :].astype(F32)).astype(BF16)

        times(HALF // 32, body)

    lo, hi = pl.ds(0, part_rows), pl.ds(part_rows, part_rows)

    def part(ch):
        return pl.ds(*PARTS[ch])

    def ring(src, dst, slot, ch, target):
        return remote(src, dst, sf, rf.at[slot, ch], at(z, x, c, target))

    def f_up(ch):
        return ring(acc.at[0, lo, part(ch)], fwd.at[0, :, part(ch)], 0, ch, up)

    def f_down(ch):
        return ring(acc.at[0, hi, part(ch)], fwd.at[1, :, part(ch)], 1, ch, down)

    def d_up(ch):
        return ring(acc.at[1, hi, part(ch)], got.at[0, hi, part(ch)], 2, ch, up)

    def d_down(ch):
        return ring(acc.at[2, lo, part(ch)], got.at[1, lo, part(ch)], 3, ch, down)

    def a_up(ch):
        return ring(acc.at[1, lo, part(ch)], got.at[0, lo, part(ch)], 4, ch, up)

    def a_down(ch):
        return ring(acc.at[2, hi, part(ch)], got.at[1, hi, part(ch)], 5, ch, down)

    def pass_on(slot, start, index, ch):
        def body(i):
            r = pl.ds(pl.multiple_of(start + i * 32, 32), 32)
            f = pl.ds(mult(i, 32), 32)
            acc[slot, r, part(ch)] = (
                acc[slot, r, part(ch)].astype(F32) + fwd[index, f, part(ch)].astype(F32)
            ).astype(BF16)

        times(part_rows // 32, body)

    def finish(ch):
        def body(i):
            r = pl.ds(mult(i, 32), 32)
            done[r, part(ch)] = (
                acc[3, r, part(ch)].astype(F32)
                + got[0, r, part(ch)].astype(F32)
                + got[1, r, part(ch)].astype(F32)
            ).astype(BF16)

        times(HALF // 32, body)

    def give_back(ch):
        def spread(d, carry):
            pz, px = plane_peer(z, x, d)
            remote(
                done.at[pl.ds(pl.multiple_of((pz * NX + px) * CAP, CAP), CAP), part(ch)],
                back.at[own_rows, part(ch)],
                sb,
                rb.at[ch],
                at(pz, px, c, y),
            ).start()
            return carry

        lax.fori_loop(1, CHIPS, spread, 0)
        back[own_rows, part(ch)] = done[own_rows, part(ch)]

    def all_back(ch):
        piece = (pl.ds(0, short), part(ch))
        return remote(done.at[piece], back.at[piece], sb, rb.at[ch], at(z, x, c, up))

    def weight_grads(start, stop):
        def step(i, carry):
            cols = pl.ds(mult(i, 256), 256)
            wg[0, :, cols] = dot(gp_t[...], rin[:, cols], NN).astype(BF16)
            wg[1, :, cols] = dot(up_t[...], rin[:, cols], NN).astype(BF16)
            wg[2, :, cols] = dot(act_t[...], rcot[:, cols], NN).astype(BF16)
            return carry

        lax.fori_loop(start, stop, step, 0)

    product(0, other, po)
    to_mate(0).start()
    product(0, mine, pm)
    product(1, other, po)
    to_mate(1).start()
    fold(0)
    f_up(0).start()
    f_down(0).start()
    product(1, mine, pm)
    product(2, other, po)
    to_mate(2).start()
    fold(1)
    d_up(0).start()
    product(2, mine, pm)
    product(3, other, po)
    to_mate(3).start()
    fold(2)
    d_down(0).start()

    def turn(ch):
        f_up(ch).wait_recv()
        pass_on(1, 0, 0, ch)
        a_up(ch).start()
        f_down(ch).wait_recv()
        pass_on(2, part_rows, 1, ch)
        a_down(ch).start()

    def launch(ch):
        f_up(ch).start()
        f_down(ch).start()
        d_up(ch).start()
        d_down(ch).start()

    def complete(ch):
        d_up(ch).wait_recv()
        d_down(ch).wait_recv()
        a_up(ch).wait_recv()
        a_down(ch).wait_recv()
        finish(ch)
        give_back(ch)

    launch(1)
    turn(0)
    launch(2)
    product(3, mine, pm)
    fold(3)
    turn(1)
    launch(3)
    weight_grads(0, 1)
    complete(0)
    turn(2)
    weight_grads(1, 2)
    complete(1)
    turn(3)
    weight_grads(2, 4)
    complete(2)
    weight_grads(4, 5)
    complete(3)

    everything = pl.ds(0, TOK)

    def share(q, piece, slot, target, ch):
        ref = share_buf.at[q, piece, part(ch)]
        return remote(ref, ref, ss, rs.at[slot, ch], at(z, x, c, target))

    def place(ch):
        all_back(ch).wait_recv()
        share_buf[y, :, part(ch)] = dot(slots[...], back[:, part(ch)], TN).astype(BF16)
        share(y, everything, 0, up, ch).start()
        share(y, everything, 1, down, ch).start()
        share(y, everything, 2, far, ch).start()

    def sent(view, sem):
        remote(view, view, sem, sem, at(z, x, c, up)).wait_send()

    def sent_dispatch():
        sent(rin.at[pl.ds(0, HALF), pl.ds(0, 3 * QUARTER)], sy.at[0])
        sent(rcot.at[pl.ds(0, HALF), pl.ds(0, 3 * RING)], sy.at[1])
        whole(6).wait_send()
        for k in range(len(CHUNKS)):
            relayed(k).wait_send()

    def sent_ring():
        sent(po, spm)
        sent(acc.at[pl.ds(0, 3)], sf)
        sent(done.at[pl.ds(0, short)], sb)
        sent(share_buf.at[pl.ds(0, 3)], ss)

    def sent_carry():
        sent(msg.at[pl.ds(0, NW - 1)], sa)
        sent(box_b.at[pl.ds(0, NZ - 1)], sbb)
        sent(res_box.at[0, pl.ds(0, (NZ - 1) * SLICE)], sr)

    place(0)
    outs = []

    def put(ref, hbm):
        copy = pltpu.make_async_copy(ref, hbm, lw.at[7 + len(outs)])
        copy.start()
        outs.append(copy)

    for ch in range(1, len(PARTS)):
        place(ch)
    for ch in range(len(PARTS)):
        share(down, everything, 0, up, ch).wait_recv()
        share(up, everything, 1, down, ch).wait_recv()
    dotted = jnp.zeros((TOK, 1), F32)

    def dotted_with(q):
        cols = pl.ds(mult(q, QUARTER), QUARTER)
        gained = gain_ref[:, cols] * share_buf[q].astype(F32)
        return jnp.sum(tok_ref[:, cols].astype(F32) * gained, axis=1, keepdims=True)

    loads[3].wait()
    sent_dispatch()
    dotted += dotted_with(y) + dotted_with(down) + dotted_with(up)
    for ch in range(len(PARTS)):
        share(far, everything, 2, far, ch).wait_recv()

    dotted += dotted_with(far)
    coef = inv * inv * inv * dotted / D
    mix = None
    for q in range(NY):
        cols = pl.ds(q * QUARTER, QUARTER)
        gained = gain_ref[:, cols] * share_buf[q].astype(F32)
        value = (
            cotan_ref[:, cols].astype(F32) + inv * gained - tok_ref[:, cols].astype(F32) * coef
        ).astype(BF16)
        res[:, cols] = value
        term = dot(value, ow[cols, :], NN)
        mix = term if mix is None else mix + term
    res_out[...] = res[:, own_cols]
    put(res_out, res_hbm)
    slice_rows = pl.ds(mult(y, SLICE), SLICE)

    def boxed(source):
        return res_box.at[y, pl.ds(mult(source, SLICE), SLICE), :]

    res_box[y, pl.ds(mult(z, SLICE), SLICE), :] = res[slice_rows, pl.ds(mult(z, CH), CH)]

    def send_res(d, source):
        p, device = line_peer(d)
        return remote(
            res.at[slice_rows, pl.ds(mult(p, CH), CH)], boxed(source), sr, rr, device
        )

    for d in range(1, NZ):
        send_res(d, z).start()
    read, write = reads[...], writes[...]
    for h in range(LOCAL_HEADS):
        lanes = slice(h * HD, (h + 1) * HD)
        sg = mix[:, lanes] * heads_silu[h]
        heads_sg[h] = sg
        growth = jnp.exp(cols_t[:, h : h + 1])
        carried = dot(growth * sg, read, TN, HIGHEST)
        for i in range(2):
            start = 2 * i * PIECE
            msg[2 * h + i, 0:PIECE, :] = jnp.concatenate(
                [carried[start : start + PIECE, :], carried[start + PIECE : start + 2 * PIECE, :]],
                axis=1,
            )
            msg[2 * h + i, PIECE : PIECE + 8, :] = jnp.broadcast_to(
                growth[TOK - 1 :, :], (8, PACK)
            )
    for d in range(1, NW):
        p, device = plane_mate(d)
        remote(msg.at[p], box_a.at[w], sa, ra, device).start()
    box_a[w] = msg[w]
    read_grads, write_grads = [], []

    def head_back(h):
        lanes = slice(h * HD, (h + 1) * HD)
        sg = heads_sg[h]
        gog_out[:, lanes] = (mix[:, lanes] * heads_gate[h]).astype(BF16)
        heads_in[h] = dot(scores[h], sg, TN, HIGHEST)
        pair_terms = dot(sg, heads_u[h], NT, HIGHEST) * pairs_w[h]
        read_grads.append(
            dot(pair_terms, write, NN, HIGHEST)
            + jnp.exp(cols_t[:, h : h + 1]) * dot(sg, state_ref[h], NN, HIGHEST)
        )
        write_grads.append(dot(pair_terms, read, TN, HIGHEST))

    head_back(0)
    weight_grads(5, 6)
    head_back(1)

    seven_a = box_a.at[pl.ds(0, NW - 1)]
    remote(seven_a, seven_a, sa, ra, at(z, x, c, up)).wait_recv()
    data, scale = pl.ds(0, PIECE), pl.ds(PIECE, 8)

    def pair(ref, i):
        s = ref[i, scale, :]
        return ref[i, data, :], jnp.concatenate([s] * (PIECE // 8), axis=0)

    total = jnp.zeros((PIECE, PACK), F32)
    decay = jnp.ones((PIECE, PACK), F32)
    inside, inside_decay = [], []
    for k in reversed(range(NW)):
        inside.append(total)
        inside_decay.append(decay)
        value, factor = pair(box_a, k)
        total = value + factor * total
        decay = factor * decay
    inside, inside_decay = inside[::-1], inside_decay[::-1]
    plane[data, :] = total
    plane[scale, :] = decay[0:8, :]
    box_b[z, data, :] = total
    box_b[z, scale, :] = decay[0:8, :]
    for d in range(1, NZ):
        remote(plane, box_b.at[z], sbb, rbb, line_peer(d)[1]).start()
    seven_res = res_box.at[y, pl.ds(0, (NZ - 1) * SLICE)]
    remote(seven_res, seven_res, sr, rr, at(z, x, c, up)).wait_recv()

    def ring_res(q, rows, slot, target):
        ref = res_box.at[q, rows, :]
        return remote(ref, ref, sq, rq.at[slot], at(z, x, c, target))

    every, early, late = (
        pl.ds(0, NZ * SLICE),
        pl.ds(0, NZ * SLICE // 2),
        pl.ds(NZ * SLICE // 2, NZ * SLICE // 2),
    )
    ring_res(y, every, 0, up).start()
    ring_res(y, every, 1, down).start()
    head_back(2)
    weight_grads(6, 8)
    wide_outs = [
        pltpu.make_async_copy(wg.at[i], hbm, lw.at[4 + i])
        for i, hbm in enumerate((gg_hbm, ug_hbm, dg_hbm))
    ]
    for out in wide_outs:
        out.start()
    seven_b = box_b.at[pl.ds(0, NZ - 1)]
    remote(seven_b, seven_b, sbb, rbb, at(z, x, c, up)).wait_recv()
    beyond = jnp.zeros((PIECE, PACK), F32)
    for k in reversed(range(1, NZ)):
        value, factor = pair(box_b, k)
        beyond = jnp.where(k > z, value + factor * beyond, beyond)
    for k in range(NW):
        fan[k] = inside[k] + inside_decay[k] * beyond

    def slot_of(p):
        return later.at[p]

    for d in range(1, NW):
        p, device = plane_mate(d)
        remote(fan.at[p], slot_of(w), sc, rc, device).start()
    later[w] = fan[w]
    head_back(3)
    put(gog_out, gog_hbm)
    sent_ring()
    ring_res(down, every, 0, up).wait_recv()
    ring_res(down, early, 2, up).start()
    ring_res(up, every, 1, down).wait_recv()
    ring_res(up, late, 3, down).start()
    seven = gz.at[pl.ds(0, (NZ - 1) * TOK), :]
    remote(seven, seven, sgz, rgz, at(z, x, c, up)).wait()
    seven_c = later.at[pl.ds(0, NW - 1)]
    remote(seven_c, seven_c, sc, rc, at(z, x, c, up)).wait_recv()

    def head_end(h):
        lanes = slice(h * HD, (h + 1) * HD)
        column = cols_t[:, h : h + 1]
        shrink = jnp.exp(column[TOK - 1 :, :] - column)
        state = jnp.concatenate(
            [later[2 * h + i, :, j * HD : (j + 1) * HD] for i in range(2) for j in range(2)], axis=0
        )
        value = heads_in[h] + shrink * dot(write, state, NT, HIGHEST)
        scan_out[:, lanes] = (value * cols_t[:, LOCAL_HEADS + h : LOCAL_HEADS + h + 1]).astype(BF16)
        write_grads[h] += shrink * dot(heads_u[h], state, NN, HIGHEST)

    for h in range(LOCAL_HEADS):
        head_end(h)
    put(scan_out, scan_hbm)
    ring_res(far, early, 2, up).wait_recv()
    ring_res(far, late, 3, down).wait_recv()
    value = None
    for q in range(NY):
        rows = jnp.concatenate(
            [gz[k * TOK + q * SLICE : k * TOK + (q + 1) * SLICE, :] for k in range(NZ)], axis=0
        )
        term = dot(res_box[q], rows, TN)
        value = term if value is None else value + term
    prod[...] = value.reshape(prod.shape).astype(BF16)
    for d in range(1, NW):
        p, device = plane_mate(d)
        remote(prod.at[p], opg_box.at[w], so, ro, device).start()
    opg_box[w] = prod[w]
    write_out[...] = jnp.transpose(sum(write_grads[1:], write_grads[0])).astype(BF16)
    read_out[...] = jnp.transpose(sum(read_grads[1:], read_grads[0])).astype(BF16)
    put(write_out, write_hbm)
    put(read_out, read_hbm)
    sent_carry()
    seven_o = opg_box.at[pl.ds(0, NW - 1)]
    remote(seven_o, seven_o, so, ro, at(z, x, c, up)).wait_recv()
    opg = opg_box[0].astype(F32)
    for k in range(1, NW):
        opg = opg + opg_box[k].astype(F32)
    opg_out[...] = opg
    put(opg_out, opg_hbm)

    sent(fan.at[pl.ds(0, NW - 1)], sc)
    sent(prod.at[pl.ds(0, NW - 1)], so)
    sent(res_box.at[pl.ds(0, 3)], sq)
    for out in wide_outs + outs:
        out.wait()


def layer(*operands):
    dma = pltpu.SemaphoreType.DMA
    hbm = pl.BlockSpec(memory_space=pl.ANY)
    smem = pl.BlockSpec(memory_space=pltpu.SMEM)
    n = len(CHUNKS)
    shape = jax.ShapeDtypeStruct
    wide = shape((HID, D), BF16)

    def held(*dims, dtype=BF16):
        return pltpu.VMEM(dims, dtype)

    head = held(LOCAL_HEADS, TOK, HD, dtype=F32)
    return pl.pallas_call(
        layer_kernel,
        out_shape=(
            wide,
            wide,
            wide,
            shape((TOK, QUARTER), BF16),
            shape((32, CH), F32),
            shape((TOK, CH), BF16),
            shape((TOK, CH), BF16),
            shape((HD, TOK), BF16),
            shape((HD, TOK), BF16),
        ),
        in_specs=[hbm] * 8 + [smem] + [hbm] * 7,
        out_specs=(hbm,) * 9,
        scratch_shapes=[
            held(HALF, QUARTER),
            held(HALF, RING + DIRECT),
            held(HALF, TOK),
            held(ROWS, D),
            held(ROWS, D),
            held(TOK, CH),
            held(NZ * TOK, CH),
            held(3, HID, D),
            held(D, CH),
            held(HID, ROWS, dtype=F32),
            held(HID, ROWS, dtype=F32),
            held(HID, ROWS, dtype=F32),
            held(HID, ROWS),
            held(HID, ROWS),
            held(HID, ROWS),
            held(ROWS, HID),
            held(ROWS, HID),
            held(3, HID, D),
            held(NY, HALF, QUARTER),
            held(NY, HALF, QUARTER, dtype=F32),
            held(NY, HALF, QUARTER),
            held(NY, HALF, QUARTER),
            held(2, HALF // 2, QUARTER),
            held(2, HALF, QUARTER),
            held(HALF, QUARTER),
            held(HALF, QUARTER),
            held(NY, TOK, QUARTER),
            held(TOK, D),
            held(NW, PIECE + 8, PACK, dtype=F32),
            held(NW, PIECE + 8, PACK, dtype=F32),
            held(PIECE + 8, PACK, dtype=F32),
            held(NZ, PIECE + 8, PACK, dtype=F32),
            held(NW, PIECE, PACK, dtype=F32),
            held(NW, PIECE, PACK, dtype=F32),
            held(NY, NZ * SLICE, CH),
            held(NW, 32, CH),
            held(NW, 32, CH),
            held(LOCAL_HEADS, TOK, TOK, dtype=F32),
            held(LOCAL_HEADS, TOK, TOK, dtype=F32),
            head,
            head,
            head,
            head,
            head,
            held(TOK, 2 * LOCAL_HEADS, dtype=F32),
            held(TOK, HD, dtype=F32),
            held(TOK, HD, dtype=F32),
            held(TOK, QUARTER),
            held(32, CH, dtype=F32),
            held(TOK, CH),
            held(TOK, CH),
            held(HD, TOK),
            held(HD, TOK),
            held(TOK, D),
            held(TOK, D),
            held(1, D, dtype=F32),
            held(2, TOK, dtype=jnp.int32),
            held(2, TOK, dtype=F32),
            held(TOK, CH),
            held(TOK, CH),
            held(LOCAL_HEADS, TOK, dtype=F32),
            held(HD, TOK),
            held(HD, TOK),
            held(LOCAL_HEADS, HD, HD, dtype=F32),
            held(TOK, QUARTER),
            held(TOK, RING),
            held(1, QUARTER, dtype=F32),
            pltpu.SemaphoreType.REGULAR,
            dma((14,)),
            dma((13,)),
            dma((n,)),
            dma((n,)),
            dma((2,)),
            dma((RINGED, 4)),
            dma((n,)),
            dma((n,)),
            dma,
            dma,
            dma,
            dma((NY,)),
            dma,
            dma((6, len(PARTS))),
            dma,
            dma((len(PARTS),)),
            dma,
            dma((3, len(PARTS))),
            dma,
            dma((4,)),
        ]
        + [dma] * 10,
        compiler_params=pltpu.CompilerParams(
            collective_id=0, has_side_effects=True, vmem_limit_bytes=62 * 1024 * 1024
        ),
        name="layer",
    )(*operands)


def hand_over_kernel(*refs):
    n = len(refs) // 3
    sources, targets = refs[:n], refs[n : 2 * n]
    held, (fetched, written) = refs[2 * n : 3 * n], refs[3 * n :]

    def pieces(i):
        rows = sources[i].shape[0]
        parts = 4 if i < 3 else 1
        step = rows // parts
        return [(k, pl.ds(k * step, step)) for k in range(parts)]

    def fetch(i, k, rows):
        return pltpu.make_async_copy(sources[i].at[rows], held[i].at[rows], fetched.at[i, k])

    def write(i, k, rows):
        return pltpu.make_async_copy(held[i].at[rows], targets[i].at[rows], written.at[i, k])

    every = [(i, k, rows) for i in range(n) for k, rows in pieces(i)]
    for piece in every:
        fetch(*piece).start()
    for piece in every:
        fetch(*piece).wait()
        write(*piece).start()
    for piece in every:
        write(*piece).wait()


def hand_over(arrays):
    hbm = pl.BlockSpec(memory_space=pl.ANY)
    n = len(arrays)
    return pl.pallas_call(
        hand_over_kernel,
        out_shape=tuple(jax.ShapeDtypeStruct(a.shape, a.dtype) for a in arrays),
        in_specs=[hbm] * n,
        out_specs=(hbm,) * n,
        scratch_shapes=[pltpu.VMEM(a.shape, a.dtype) for a in arrays]
        + [pltpu.SemaphoreType.DMA((n, 4))] * 2,
        compiler_params=pltpu.CompilerParams(vmem_limit_bytes=62 * 1024 * 1024),
        name="hand_over",
    )(*arrays)


def shards(
    tokens,
    norm_gain,
    cotangent,
    routes,
    route_weight,
    gate_weight,
    up_weight,
    down_weight,
    scan_input,
    out_gate,
    step_size,
    decay_rate,
    write_keys,
    read_keys,
    start_state,
    out_proj,
):
    (
        gate_grad,
        up_grad,
        down_grad,
        residual_part,
        out_proj_grad,
        scan_grad,
        gate_out_grad,
        write_grad,
        read_grad,
    ) = hand_over(
        layer(
        tokens,
        cotangent,
        norm_gain[None, :],
        jnp.transpose(routes),
        jnp.transpose(route_weight),
        out_gate,
        scan_input,
        step_size,
        decay_rate,
        jnp.transpose(write_keys),
        jnp.transpose(read_keys),
        start_state[0],
        jnp.transpose(gate_weight[0]),
        jnp.transpose(up_weight[0]),
        down_weight[0],
        out_proj,
        )
    )
    return (
        residual_part,
        jnp.transpose(gate_grad)[None],
        jnp.transpose(up_grad)[None],
        down_grad[None],
        out_proj_grad,
        scan_grad,
        gate_out_grad,
        jnp.transpose(write_grad),
        jnp.transpose(read_grad),
    )


def solution(mesh):
    finer = Mesh(mesh.devices.reshape(8, 4, 2, mesh.shape["tp"]), ("sp_0", "sp_1", "sp_2", "tp"))
    in_specs = (
        P(SP, None),
        P(),
        P(SP, None),
        P(SP, None),
        P(SP, None),
        P(SP, None, "tp"),
        P(SP, None, "tp"),
        P(SP, "tp", None),
        P(SP, "tp"),
        P(SP, "tp"),
        P("tp", SP),
        P("tp"),
        P(SP, "tp"),
        P(SP, "tp"),
        P(SP, "tp", None, None),
        P(None, "tp"),
    )
    out_specs = (
        P(SP, "tp"),
        P(SP, None, "tp"),
        P(SP, None, "tp"),
        P(SP, "tp", None),
        P(SP, "tp"),
        P(SP, "tp"),
        P(SP, "tp"),
        P(SP, "tp"),
        P(SP, "tp"),
    )
    return jax.shard_map(
        shards, mesh=finer, in_specs=in_specs, out_specs=out_specs, check_vma=False
    )
```
